128 devices in a mesh: ra: 16 (over z, x), cb: 8 (over y, core).
Axes of the slice: x: 4, y: 4, z: 4, core: 2. Of those that a mesh axis runs over, the one named last changes fastest.
Arguments:
- inputs: bfloat16 [1536, 4096], P(None, 'ra'), may hold values from -12 to 12
- gate_weight: bfloat16 [2, 4096, 11264], P(None, 'ra', 'cb'), may hold values from -0.09375 to 0.09375
- up_weight: bfloat16 [2, 4096, 11264], P(None, 'ra', 'cb'), may hold values from -0.09375 to 0.09375
- down_weight: bfloat16 [2, 11264, 4096], P(None, 'cb', 'ra'), may hold values from -0.0546875 to 0.0546875
- norm_gain: float32 [2, 4096], P(None, 'ra'), may hold values from 0.05 to 8
- norm_shift: float32 [2, 4096], P(None, 'ra'), may hold values from -1.5 to 1.5
Outputs:
- outputs: bfloat16 [1536, 4096], P(None, 'ra')
The draws below stay inside these ranges and needn't reach their ends.
All inputs are finite; a program needn't handle non-finite values.
Results may differ from the reference program's by a relative error of at most 0.04.
Values may be sent and summed in bfloat16 or wider, within the bound.
A program may use at most 64 MiB of HBM per device.

```python
import jax
import jax.numpy as jnp
from jax import lax

D = 4096
FF = 11264
TOKENS = 1536
LAYERS = 2
N_RA = 16


def draw_inputs(key, part):
    key = jax.random.fold_in(key, 11)
    keys = jax.random.split(key, 3)
    groups = 32
    factor = jnp.exp(jax.random.uniform(keys[0], (1, groups), jnp.float32, jnp.log(0.3), jnp.log(3.0)))
    offset = jax.random.uniform(keys[1], (1, groups), jnp.float32, -1.0, 1.0)
    factor = jnp.repeat(factor, D // groups, axis=1)
    offset = jnp.repeat(offset, D // groups, axis=1)
    base = jax.random.normal(keys[2], (TOKENS, D), jnp.float32)
    return jnp.clip(base * factor + offset, -12.0, 12.0).astype(jnp.bfloat16)


def draw_norm_gain(key, part):
    key = jax.random.fold_in(key, 23)
    keys = jax.random.split(key, 2)
    groups = 32
    factor = jnp.exp(jax.random.uniform(keys[0], (LAYERS, groups), jnp.float32, jnp.log(0.35), jnp.log(3.0)))
    factor = jnp.repeat(factor, D // groups, axis=1)
    noise = jnp.clip(jax.random.normal(keys[1], (LAYERS, D), jnp.float32), -3.0, 3.0)
    return (factor * (1.0 + 0.18 * noise)).astype(jnp.float32)


def block_levels(stream_key, dims, pieces, low, high):
    level, own = 1.0, jax.random.fold_in(stream_key, 6)
    for axis_at, blocks in pieces:
        draws = jnp.exp(jax.random.uniform(jax.random.fold_in(own, axis_at), (blocks,), jnp.float32, low / len(pieces), high / len(pieces)))
        level = level * jnp.repeat(draws, dims[axis_at] // blocks).reshape([-1 if axis == axis_at else 1 for axis in range(len(dims))])
    return level


def scatter_about(key, shape, spread, most, pieces=(), dtype=jnp.bfloat16):
    loudness = block_levels(key, shape, pieces, -0.22, 0.18) if pieces else 1.0
    entries = jax.random.normal(key, shape, jnp.float32) * spread * loudness
    return jnp.minimum(jnp.maximum(entries, -most), most).astype(dtype)


def setup_inputs(seed: int = 0) -> dict:
    seeds = jax.random.split(jax.random.key(seed), 7)
    inputs = draw_inputs(jax.random.fold_in(seeds[6], 71), 0)
    gate_weight = scatter_about(seeds[1], (LAYERS, D, FF), D ** -0.5, 0.09375, ((1, 16), (2, 8)))
    up_weight = scatter_about(seeds[2], (LAYERS, D, FF), D ** -0.5, 0.09375, ((1, 16), (2, 8)))
    down_weight = scatter_about(seeds[3], (LAYERS, FF, D), FF ** -0.5, 0.0546875, ((1, 8), (2, 16)))
    norm_gain = draw_norm_gain(jax.random.fold_in(seeds[6], 71), 0)
    norm_shift = scatter_about(seeds[5], (LAYERS, D), 0.3, 1.5, ((1, 16),), jnp.float32)
    return {"inputs": inputs, "gate_weight": gate_weight, "up_weight": up_weight, "down_weight": down_weight, "norm_gain": norm_gain, "norm_shift": norm_shift}


RESIDUAL = 0.5
EPSILON = 1e-05

def block_products(stream, paired):
    width = D // N_RA
    total = jnp.zeros((stream.shape[0], paired.shape[1]), jnp.float32)
    for block_index in range(N_RA):
        start = block_index * width
        piece = jnp.dot(stream[:, start:start + width], paired[start:start + width], preferred_element_type=jnp.float32)
        rounded = lax.optimization_barrier(piece.astype(jnp.bfloat16))
        total = total + rounded.astype(jnp.float32)
    return total

def sublayer(stream, w_gate, w_up, w_down, gain_row, shift_row):
    columns = w_gate.shape[1]
    paired = jnp.concatenate((w_gate, w_up), axis=1)
    summed = block_products(stream, paired)
    hidden = (jax.nn.silu(summed[:, :columns]) * summed[:, columns:]).astype(jnp.bfloat16)
    branch = jnp.dot(hidden, w_down, preferred_element_type=jnp.float32)
    mixed_rows = RESIDUAL * stream.astype(jnp.float32) + branch
    mean_rows = lax.optimization_barrier(jnp.sum(mixed_rows, axis=1)) / D
    var_rows = lax.optimization_barrier(jnp.sum(mixed_rows * mixed_rows, axis=1)) / D - mean_rows * mean_rows
    normed = (mixed_rows - mean_rows[:, None]) * lax.rsqrt(var_rows + EPSILON)[:, None]
    return (normed * gain_row + shift_row).astype(jnp.bfloat16)

def reference(inputs, gate_weight, up_weight, down_weight, norm_gain, norm_shift):
    stream = inputs
    for layer_index in range(LAYERS):
        stream = sublayer(stream, gate_weight[layer_index], up_weight[layer_index], down_weight[layer_index], norm_gain[layer_index], norm_shift[layer_index])
    return stream
```

```python
import functools

import jax
import jax.numpy as jnp
from jax import lax
from jax.experimental import pallas as pl
from jax.experimental.pallas import tpu as pltpu
from jax.sharding import PartitionSpec as P

MESH = pl.DeviceIdType.MESH
BF = jnp.bfloat16
F32 = jnp.float32
RESIDUAL = 0.5
EPSILON = 1e-05

T, D, FF, LAYERS = 1536, 4096, 11264, 2
NC = 3
TC = T // NC
ZB = TC // 4
ZH = ZB // 2
CB_ROWS = TC // 2
YB = TC // 8
YH = YB // 2
R = TC // 32
DB = D // 16
DQ = D // 4
FB = FF // 8
FS = 384
F_LAST = FB - FS

ZA0, ZA1, ZB0, ZB1, ZC0, ZC1 = range(6)
HF0, HF1, HB1, HB0, HG0, HG1 = range(6, 12)
CX = 12
YA0, YA1, YB0, YB1, YC0, YC1 = range(13, 19)
XR = 19
ST = 22
N_RS = 25
XG = 0
YF0, YF1, YK1, YK0, YG0, YG1 = range(3, 9)
DD = 9
N_AG = 13

PERIOD, LAYER_TIME, START = 9.5, 42.0, 18.0
OFFSETS = dict(A=0, B=4.3, C=8.5, D=11.6, E=13.7, F=16.2, G=19.5, H=22.3, I=26.5, J=29.2, K=33.5, L=36.6, M=39.4)


def order():
    timed = []
    for k in range(NC):
        for stage in "KLM":
            timed.append((START - LAYER_TIME + OFFSETS[stage] + 4.0 * k, (stage, -1, k)))
        for layer in range(LAYERS):
            for stage, offset in OFFSETS.items():
                timed.append((START + layer * LAYER_TIME + k * PERIOD + offset, (stage, layer, k)))
    timed.sort(key=lambda item: item[0])
    return [task for _, task in timed]


def kernel(
    x_hbm, wg_hbm, wu_hbm, wd_hbm, gain_hbm, shift_hbm, out_hbm,
    xs, wgu, wd, part, ra, rb, rc, hid, down, core_in, ya, yb, yc, ys, xr, mixed, st, st_in, nb, ov, ga, sh,
    rs_recv, rs_send, ag_recv, ag_send, w_recv, w_send, g_recv, g_send, local,
):
    ra_at, cb_at = lax.axis_index("ra"), lax.axis_index("cb")
    z, x = ra_at // 4, lax.rem(ra_at, 4)
    y, c = cb_at // 2, lax.rem(cb_at, 2)

    def turn(v, d):
        return lax.rem(v + d, 4)

    zp, zo, zm = turn(z, 1), turn(z, 2), turn(z, 3)
    yp, yo, ym = turn(y, 1), turn(y, 2), turn(y, 3)

    def at_z(v):
        return (v * 4 + x, cb_at)

    def at_x(v):
        return (z * 4 + v, cb_at)

    def at_y(v):
        return (ra_at, v * 2 + c)

    other = (ra_at, y * 2 + (1 - c))

    peers = [at_z(zp), at_z(zo), at_z(zm)] + [at_x(turn(x, d)) for d in (1, 2, 3)] + [at_y(yp), at_y(ym), other]
    barrier = pltpu.get_barrier_semaphore()
    for peer in peers:
        pl.semaphore_signal(barrier, inc=1, device_id=peer, device_id_type=MESH)
    pl.semaphore_wait(barrier, len(peers))

    sent = []

    def send(src, dst, send_sem, recv_sem, dev):
        copy = pltpu.make_async_remote_copy(
            src_ref=src, dst_ref=dst, send_sem=send_sem, recv_sem=recv_sem, device_id=dev, device_id_type=MESH
        )
        copy.start()
        sent.append(copy)

    def arrived(dst, recv_sem):
        pltpu.make_async_remote_copy(
            src_ref=dst, dst_ref=dst, send_sem=recv_sem, recv_sem=recv_sem, device_id=other, device_id_type=MESH
        ).wait_recv()

    def f_start(v):
        return pl.multiple_of(jnp.minimum(v * FS, F_LAST), 128)

    def d_cols(v):
        return pl.ds(pl.multiple_of(v * DB, DB), DB)

    def weight_views(l, what, dst, owner):
        units = pl.ds(f_start(dst), FS)
        if what == 0:
            return wg_hbm.at[l, :, units], wgu.at[l, d_cols(owner), pl.ds(0, FS)]
        if what == 1:
            return wu_hbm.at[l, :, units], wgu.at[l, d_cols(owner), pl.ds(FS, FS)]
        return wd_hbm.at[l, units, :], wd.at[l, :, d_cols(owner)]

    own_copies = {}

    def weights_send(l, what):
        for d in (1, 3, 2):
            src, dst = weight_views(l, what, turn(x, d), x)
            send(src, dst, w_send.at[l, what, d - 1], w_recv.at[l, what, d - 1], at_x(turn(x, d)))
        src, dst = weight_views(l, what, x, x)
        own_copies[l, what] = pltpu.make_async_copy(src, dst, local.at[l * 3 + what])
        own_copies[l, what].start()

    def weights_wait(l, what):
        for d in (1, 3, 2):
            _, dst = weight_views(l, what, x, turn(x, 4 - d))
            arrived(dst, w_recv.at[l, what, d - 1])
        own_copies[l, what].wait()

    def gathered(p, k, rows):
        if p < 2:
            return xs.at[p, k, rows, :]
        return ov.at[k, rows, :]

    def y_rows(cc, yy):
        return pl.ds(pl.multiple_of(cc * CB_ROWS + yy * YB, YB), YB)

    def y_half(cc, yy, h):
        return pl.ds(pl.multiple_of(cc * CB_ROWS + yy * YB + h * YH, YH), YH)

    def x_rows(xx):
        return pl.ds(pl.multiple_of(c * CB_ROWS + y * YB + xx * R, R), R)

    in_copies = []
    for k in range(NC):
        rows = pl.ds(pl.multiple_of(k * TC + c * CB_ROWS + y * YB, YB), YB)
        for d in (1, 3, 2):
            send(
                x_hbm.at[rows, :], xs.at[0, k, y_rows(c, y), d_cols(x)],
                ag_send.at[0, k, XG + d - 1], ag_recv.at[0, k, XG + d - 1], at_x(turn(x, d)),
            )
        copy = pltpu.make_async_copy(x_hbm.at[rows, :], xs.at[0, k, y_rows(c, y), d_cols(x)], local.at[6 + k])
        copy.start()
        in_copies.append(copy)
    weights_send(0, 0)
    weights_send(0, 1)
    for i, (src, dst) in enumerate(((gain_hbm, ga), (shift_hbm, sh))):
        for d in (1, 3, 2):
            send(src, dst.at[x], g_send.at[i, d - 1], g_recv.at[i, d - 1], at_x(turn(x, d)))
        copy = pltpu.make_async_copy(src, dst.at[x], local.at[6 + NC + i])
        copy.start()
        own_copies["g", i] = copy
    weights_send(0, 2)

    def stage_a(l, k):
        for j, (cc, yy) in enumerate(((1 - c, y), (1 - c, ym), (1 - c, yp), (1 - c, yo))):
            arrived(gathered(l, k, y_rows(cc, yy)), ag_recv.at[l, k, DD + j])
        if k == 0:
            weights_wait(l, 0)
            weights_wait(l, 1)

        def block(o):
            rows = pl.ds(pl.multiple_of(o * ZB, ZB), ZB)

            def columns(n, carry):
                cols = pl.ds(pl.multiple_of(n * 256, 256), 256)
                value = jnp.dot(xs[l, k, rows, :], wgu[l, :, cols], preferred_element_type=F32).astype(BF)
                part[l, k, o, 0, :, cols] = value[:ZH]
                part[l, k, o, 1, :, cols] = value[ZH:]
                return carry

            lax.fori_loop(0, 2 * FS // 256, columns, 0)

        sems = rs_send.at[l, k], rs_recv.at[l, k]
        block(zo)
        send(part.at[l, k, zo, 0], ra.at[l, k, 0], sems[0].at[ZA0], sems[1].at[ZA0], at_z(zp))
        send(part.at[l, k, zo, 1], ra.at[l, k, 1], sems[0].at[ZA1], sems[1].at[ZA1], at_z(zm))

        def rest(j, carry):
            block(lax.rem(z + 1 + j * 2, 4))
            return carry

        lax.fori_loop(0, 2, rest, 0)
        send(part.at[l, k, zp, 1], rb.at[l, k, 0], sems[0].at[ZB0], sems[1].at[ZB0], at_z(zp))
        send(part.at[l, k, zm, 0], rb.at[l, k, 1], sems[0].at[ZB1], sems[1].at[ZB1], at_z(zm))
        block(z)

    def stage_b(l, k):
        sems = rs_send.at[l, k], rs_recv.at[l, k]
        arrived(ra.at[l, k, 0], sems[1].at[ZA0])
        part[l, k, zp, 0] = (part[l, k, zp, 0].astype(F32) + ra[l, k, 0].astype(F32)).astype(BF)
        send(part.at[l, k, zp, 0], rc.at[l, k, 0], sems[0].at[ZC0], sems[1].at[ZC0], at_z(zp))
        arrived(ra.at[l, k, 1], sems[1].at[ZA1])
        part[l, k, zm, 1] = (part[l, k, zm, 1].astype(F32) + ra[l, k, 1].astype(F32)).astype(BF)
        send(part.at[l, k, zm, 1], rc.at[l, k, 1], sems[0].at[ZC1], sems[1].at[ZC1], at_z(zm))

    def stage_c(l, k):
        sems = rs_send.at[l, k], rs_recv.at[l, k]
        for h in (0, 1):
            arrived(rb.at[l, k, 1 - h], sems[1].at[(ZB1, ZB0)[h]])
            arrived(rc.at[l, k, h], sems[1].at[(ZC0, ZC1)[h]])
            total = part[l, k, z, h].astype(F32) + rc[l, k, h].astype(F32) + rb[l, k, 1 - h].astype(F32)
            gate, up = total[:, :FS], total[:, FS:]
            value = gate * jax.nn.sigmoid(gate) * up
            column = lax.broadcasted_iota(jnp.int32, (ZH, FS), 1)
            value = jnp.where(jnp.logical_and(x == 3, column < 4 * FS - FB), 0.0, value)
            hid[l, k, z, h] = value.astype(BF)
        for h in (0, 1):
            send(hid.at[l, k, z, h], hid.at[l, k, z, h], sems[0].at[(HF0, HF1)[h]], sems[1].at[(HF0, HF1)[h]], at_z(zp))
            g = 1 - h
            send(hid.at[l, k, z, g], hid.at[l, k, z, g], sems[0].at[(HB0, HB1)[g]], sems[1].at[(HB0, HB1)[g]], at_z(zm))

    def stage_d(l, k):
        sems = rs_send.at[l, k], rs_recv.at[l, k]
        arrived(hid.at[l, k, zm, 0], sems[1].at[HF0])
        send(hid.at[l, k, zm, 0], hid.at[l, k, zm, 0], sems[0].at[HG0], sems[1].at[HG0], at_z(zp))
        arrived(hid.at[l, k, zp, 1], sems[1].at[HB1])
        send(hid.at[l, k, zp, 1], hid.at[l, k, zp, 1], sems[0].at[HG1], sems[1].at[HG1], at_z(zm))

    def stage_e(l, k):
        sems = rs_send.at[l, k], rs_recv.at[l, k]
        arrived(hid.at[l, k, zm, 1], sems[1].at[HF1])
        arrived(hid.at[l, k, zp, 0], sems[1].at[HB0])
        arrived(hid.at[l, k, zo, 0], sems[1].at[HG0])
        arrived(hid.at[l, k, zo, 1], sems[1].at[HG1])
        if k == 0:
            weights_wait(l, 2)

        def half(cc):
            def columns(n, carry):
                cols = pl.ds(pl.multiple_of(n * 256, 256), 256)
                lhs = hid[l, k, pl.ds(cc * 2, 2)].reshape(CB_ROWS, FS)
                value = jnp.dot(lhs, wd[l, :, cols], preferred_element_type=F32).astype(BF)
                for yy in range(4):
                    for h in (0, 1):
                        at = yy * YB + h * YH
                        down[l, k, cc, yy, h, :, cols] = value[at:at + YH]
                return carry

            lax.fori_loop(0, DQ // 256, columns, 0)

        half(1 - c)
        send(down.at[l, k, 1 - c], core_in.at[l, k], sems[0].at[CX], sems[1].at[CX], other)
        half(c)

    def stage_f(l, k):
        sems = rs_send.at[l, k], rs_recv.at[l, k]
        arrived(core_in.at[l, k], sems[1].at[CX])

        def add(yy):
            for h in (0, 1):
                down[l, k, c, yy, h] = (
                    down[l, k, c, yy, h].astype(F32) + core_in[l, k, yy, h].astype(F32)
                ).astype(BF)

        add(yo)
        send(down.at[l, k, c, yo, 0], ya.at[l, k, 0], sems[0].at[YA0], sems[1].at[YA0], at_y(yp))
        send(down.at[l, k, c, yo, 1], ya.at[l, k, 1], sems[0].at[YA1], sems[1].at[YA1], at_y(ym))
        add(yp)
        send(down.at[l, k, c, yp, 1], yb.at[l, k, 0], sems[0].at[YB0], sems[1].at[YB0], at_y(yp))
        add(ym)
        send(down.at[l, k, c, ym, 0], yb.at[l, k, 1], sems[0].at[YB1], sems[1].at[YB1], at_y(ym))
        add(y)

    def stage_g(l, k):
        sems = rs_send.at[l, k], rs_recv.at[l, k]
        arrived(ya.at[l, k, 0], sems[1].at[YA0])
        down[l, k, c, yp, 0] = (down[l, k, c, yp, 0].astype(F32) + ya[l, k, 0].astype(F32)).astype(BF)
        send(down.at[l, k, c, yp, 0], yc.at[l, k, 0], sems[0].at[YC0], sems[1].at[YC0], at_y(yp))
        arrived(ya.at[l, k, 1], sems[1].at[YA1])
        down[l, k, c, ym, 1] = (down[l, k, c, ym, 1].astype(F32) + ya[l, k, 1].astype(F32)).astype(BF)
        send(down.at[l, k, c, ym, 1], yc.at[l, k, 1], sems[0].at[YC1], sems[1].at[YC1], at_y(ym))

    def stage_h(l, k):
        sems = rs_send.at[l, k], rs_recv.at[l, k]
        for h in (0, 1):
            arrived(yb.at[l, k, 1 - h], sems[1].at[(YB1, YB0)[h]])
            arrived(yc.at[l, k, h], sems[1].at[(YC0, YC1)[h]])
            total = down[l, k, c, y, h].astype(F32) + yc[l, k, h].astype(F32) + yb[l, k, 1 - h].astype(F32)
            ys[l, k, 2 * h] = total[:R].astype(BF)
            ys[l, k, 2 * h + 1] = total[R:].astype(BF)
        for d in (2, 1, 3):
            send(
                ys.at[l, k, turn(x, d)], xr.at[l, k, d - 1], sems[0].at[XR + d - 1], sems[1].at[XR + d - 1],
                at_x(turn(x, d)),
            )

    def stage_i(l, k):
        sems = rs_send.at[l, k], rs_recv.at[l, k]
        value = RESIDUAL * xs[l, k, x_rows(x), :].astype(F32) + ys[l, k, x].astype(F32)
        for d in (1, 3, 2):
            arrived(xr.at[l, k, d - 1], sems[1].at[XR + d - 1])
            value = value + xr[l, k, d - 1].astype(F32)
        mixed[l, k] = value
        row_sum = jnp.sum(value, axis=1, keepdims=True)
        row_squares = jnp.sum(value * value, axis=1, keepdims=True)
        lane = lax.broadcasted_iota(jnp.int32, (R, 128), 1)
        st[l, k] = jnp.where(lane == 0, row_sum, jnp.where(lane == 1, row_squares, 0.0))
        for d in (2, 1, 3):
            send(
                st.at[l, k], st_in.at[l, k, d - 1], sems[0].at[ST + d - 1], sems[1].at[ST + d - 1],
                at_z(turn(z, d)),
            )

    def stage_j(l, k):
        sems = rs_recv.at[l, k]
        if l == 0 and k == 0:
            for i, dst in enumerate((ga, sh)):
                for d in (1, 3, 2):
                    arrived(dst.at[turn(x, 4 - d)], g_recv.at[i, d - 1])
                own_copies["g", i].wait()
        stats = st[l, k]
        for d in (1, 3, 2):
            arrived(st_in.at[l, k, d - 1], sems.at[ST + d - 1])
            stats = stats + st_in[l, k, d - 1]
        mean = stats[:, 0:1] / D
        var = stats[:, 1:2] / D - mean * mean
        scale = lax.rsqrt(var + EPSILON)
        for q in range(4):
            cols = slice(q * DB, (q + 1) * DB)
            normed = (mixed[l, k, :, cols] - mean) * scale
            value = (normed * ga[q, l:l + 1, :] + sh[q, l:l + 1, :]).astype(BF)
            if l + 1 < LAYERS:
                xs[l + 1, k, x_rows(x), cols] = value
            else:
                nb[k, q] = value
        if l + 1 == LAYERS:
            ov[k, x_rows(x), :] = nb[k, x]
        for d in (2, 1, 3):
            src = xs.at[l + 1, k, x_rows(x), :] if l + 1 < LAYERS else nb.at[k, turn(x, d)]
            send(
                src, gathered(l + 1, k, x_rows(x)), ag_send.at[l + 1, k, XG + d - 1],
                ag_recv.at[l + 1, k, XG + d - 1], at_x(turn(x, d)),
            )

    def stage_k(l, k):
        p = l + 1
        sems = ag_send.at[p, k], ag_recv.at[p, k]
        for d in (1, 3, 2):
            owner = turn(x, 4 - d)
            if p == 0:
                arrived(xs.at[0, k, y_rows(c, y), d_cols(owner)], sems[1].at[XG + d - 1])
            else:
                arrived(gathered(p, k, x_rows(owner)), sems[1].at[XG + d - 1])
        if p == 0:
            in_copies[k].wait()
        for h in (0, 1):
            ref = gathered(p, k, y_half(c, y, h))
            send(ref, ref, sems[0].at[(YF0, YF1)[h]], sems[1].at[(YF0, YF1)[h]], at_y(yp))
            g = 1 - h
            ref = gathered(p, k, y_half(c, y, g))
            send(ref, ref, sems[0].at[(YK0, YK1)[g]], sems[1].at[(YK0, YK1)[g]], at_y(ym))
        ref = gathered(p, k, y_rows(c, y))
        send(ref, ref, sems[0].at[DD], sems[1].at[DD], other)

    def stage_l(l, k):
        p = l + 1
        sems = ag_send.at[p, k], ag_recv.at[p, k]
        ref = gathered(p, k, y_half(c, ym, 0))
        arrived(ref, sems[1].at[YF0])
        send(ref, ref, sems[0].at[YG0], sems[1].at[YG0], at_y(yp))
        ref = gathered(p, k, y_half(c, yp, 1))
        arrived(ref, sems[1].at[YK1])
        send(ref, ref, sems[0].at[YG1], sems[1].at[YG1], at_y(ym))

    def stage_m(l, k):
        p = l + 1
        sems = ag_send.at[p, k], ag_recv.at[p, k]
        for j, (yy, last, slot) in enumerate(((ym, 1, YF1), (yp, 0, YK0))):
            arrived(gathered(p, k, y_half(c, yy, last)), sems[1].at[slot])
            ref = gathered(p, k, y_rows(c, yy))
            send(ref, ref, sems[0].at[DD + 1 + j], sems[1].at[DD + 1 + j], other)
        arrived(gathered(p, k, y_half(c, yo, 0)), sems[1].at[YG0])
        arrived(gathered(p, k, y_half(c, yo, 1)), sems[1].at[YG1])
        ref = gathered(p, k, y_rows(c, yo))
        send(ref, ref, sems[0].at[DD + 3], sems[1].at[DD + 3], other)

    stages = dict(
        A=stage_a, B=stage_b, C=stage_c, D=stage_d, E=stage_e, F=stage_f, G=stage_g, H=stage_h, I=stage_i,
        J=stage_j, K=stage_k, L=stage_l, M=stage_m,
    )
    later_weights = {("A", 0, 0): 0, ("A", 0, 1): 1, ("A", 0, 2): 2}
    for stage, l, k in order():
        stages[stage](l, k)
        if (stage, l, k) in later_weights:
            weights_send(1, later_weights[stage, l, k])

    out_copies = []
    for k in range(NC):
        for j, (cc, yy) in enumerate(((1 - c, y), (1 - c, ym), (1 - c, yp), (1 - c, yo))):
            arrived(gathered(2, k, y_rows(cc, yy)), ag_recv.at[2, k, DD + j])
        copy = pltpu.make_async_copy(ov.at[k], out_hbm.at[pl.ds(k * TC, TC), :], local.at[8 + NC + k])
        copy.start()
        out_copies.append(copy)
    for copy in sent:
        copy.wait_send()
    for copy in out_copies:
        copy.wait()


def solution(mesh):
    dma = pltpu.SemaphoreType.DMA

    def per_device(inputs, gate_weight, up_weight, down_weight, norm_gain, norm_shift):
        any_space = pl.BlockSpec(memory_space=pl.ANY)
        return pl.pallas_call(
            kernel,
            out_shape=jax.ShapeDtypeStruct((T, DB), BF),
            in_specs=[any_space] * 6,
            out_specs=any_space,
            scratch_shapes=[
                pltpu.VMEM((2, NC, TC, DQ), BF),
                pltpu.VMEM((2, DQ, 2 * FS), BF),
                pltpu.VMEM((2, FS, DQ), BF),
                pltpu.VMEM((2, NC, 4, 2, ZH, 2 * FS), BF),
                pltpu.VMEM((2, NC, 2, ZH, 2 * FS), BF),
                pltpu.VMEM((2, NC, 2, ZH, 2 * FS), BF),
                pltpu.VMEM((2, NC, 2, ZH, 2 * FS), BF),
                pltpu.VMEM((2, NC, 4, 2, ZH, FS), BF),
                pltpu.VMEM((2, NC, 2, 4, 2, YH, DQ), BF),
                pltpu.VMEM((2, NC, 4, 2, YH, DQ), BF),
                pltpu.VMEM((2, NC, 2, YH, DQ), BF),
                pltpu.VMEM((2, NC, 2, YH, DQ), BF),
                pltpu.VMEM((2, NC, 2, YH, DQ), BF),
                pltpu.VMEM((2, NC, 4, R, DQ), BF),
                pltpu.VMEM((2, NC, 3, R, DQ), BF),
                pltpu.VMEM((2, NC, R, DQ), F32),
                pltpu.VMEM((2, NC, R, 128), F32),
                pltpu.VMEM((2, NC, 3, R, 128), F32),
                pltpu.VMEM((NC, 4, R, DB), BF),
                pltpu.VMEM((NC, TC, DB), BF),
                pltpu.VMEM((4, 2, DB), F32),
                pltpu.VMEM((4, 2, DB), F32),
                dma((2, NC, N_RS)),
                dma((2, NC, N_RS)),
                dma((3, NC, N_AG)),
                dma((3, NC, N_AG)),
                dma((2, 3, 3)),
                dma((2, 3, 3)),
                dma((2, 3)),
                dma((2, 3)),
                dma((8 + 2 * NC,)),
            ],
            compiler_params=pltpu.CompilerParams(
                collective_id=0, has_side_effects=True, vmem_limit_bytes=62 * 1024 * 1024
            ),
        )(inputs, gate_weight, up_weight, down_weight, norm_gain, norm_shift)

    return jax.shard_map(
        per_device,
        mesh=mesh,
        in_specs=(P(None, "ra"), P(None, "ra", "cb"), P(None, "ra", "cb"), P(None, "cb", "ra"), P(None, "ra"), P(None, "ra")),
        out_specs=P(None, "ra"),
        check_vma=False,
    )
```

```python
import jax
import jax.numpy as jnp
from jax import lax
from jax.experimental import pallas as pl
from jax.experimental.pallas import tpu as pltpu
from jax.sharding import PartitionSpec as P

MESH = pl.DeviceIdType.MESH
BF = jnp.bfloat16
F32 = jnp.float32
RESIDUAL = 0.5
EPSILON = 1e-05

T, D, FF, LAYERS = 1536, 4096, 11264, 2
TCORE = T // 2
NC = 3
TC = TCORE // NC
ZB = TC // 4
ZH = ZB // 2
YB = TC // 4
YH = YB // 2
R = TC // 16
DB = D // 16
DQ = D // 4
UT = 128
NJ = 3
NT = 2 * NJ
TILES = FF // 8 // UT
SHARED = 4 * NJ - TILES

ZA0, ZA1, ZB0, ZB1, ZC0, ZC1, HF0, HF1, HB1, HB0, HG0, HG1 = range(12)
N_Z = 12
YA0, YA1, YB0, YB1, YC0, YC1 = range(6)
XR = 6
ST = 9
N_Y = 12
XG = 0
YF0, YF1, YK1, YK0, YG0, YG1 = range(3, 9)
DD = 9
N_AG = 13
WM, WP, WRM, WRP, WOM, WOP, WD = range(7)
N_W = 10

HOP = {1: 1.8, 2: 2.6}
CORE_HOP = 1.0
FROM_HBM = 1.1
LINK = 46.6e3
CORE_LINK = 500e3
TIMES = dict(A=0.5, B=0.1, C=0.2, D=0.05, E=0.9, G=0.12, H=0.15, I=0.25, J=0.3, K=0.06, L=0.06, M=0.03, W=0.1, V=0.05, U=0.08)


SLACK = dict(A=0.5, E=0.5, W=0.7)


def plan():
    tasks = {}
    gu, dn = DB * UT * 2, NJ * UT * DB * 2
    for l in range(LAYERS):
        for j in range(NJ + 1):
            size = 2 * gu if j < NJ else dn
            tasks["W", l, j] = ([], [
                (("wrm", l, j), "x+", size // 2, 1), (("wrp", l, j), "x-", size // 2, 1),
                (("wm", l, j), "x+", size, 1), (("wp", l, j), "x-", size, 1), (("wd", l, j), "c", size, 0),
            ])
            tasks["V", l, j] = ([("wrm", l, j), ("wrp", l, j)], [
                (("wom", l, j), "x+", size // 2, 1), (("wop", l, j), "x-", size // 2, 1)])
            tasks["U", l, j] = ([("wm", l, j), ("wp", l, j), ("wom", l, j), ("wop", l, j)], [(("wu", l, j), "c", 3 * size, 0)])
    zs, hs = ZH * 4 * UT * 2, ZH * 2 * UT * 2
    for k in range(NC):
        for p in range(LAYERS + 1):
            ys = YH * (DQ if p < LAYERS else DB) * 2
            sends = [(("yf", p, k), "y+", ys, 1), (("yk", p, k), "y-", ys, 1), (("yf1", p, k), "y+", ys, 1), (("yk1", p, k), "y-", ys, 1)]
            tasks["K", p - 1, k] = ([("xg", p, k)], sends)
            tasks["L", p - 1, k] = ([("yf", p, k), ("yk", p, k)], [(("yg", p, k), "y+", ys, 1), (("yg1", p, k), "y-", ys, 1)])
        for l in range(LAYERS):
            for j in range(NJ):
                need = [("yg", l, k), ("yg1", l, k), ("yf1", l, k), ("yk1", l, k)] + [("wd", l, j), ("wu", l, j)]
                tasks["A", l, k, j] = (need, [
                    (("za", l, k, j), "z+", zs, 1), (("za1", l, k, j), "z-", zs, 1),
                    (("zb", l, k, j), "z+", zs, 1), (("zb1", l, k, j), "z-", zs, 1)])
                tasks["B", l, k, j] = ([("za", l, k, j), ("za1", l, k, j)], [
                    (("zc", l, k, j), "z+", zs, 1), (("zc1", l, k, j), "z-", zs, 1)])
                tasks["C", l, k, j] = ([(m, l, k, j) for m in ("zb", "zb1", "zc", "zc1")], [
                    (("hf", l, k, j), "z+", hs, 1), (("hk", l, k, j), "z-", hs, 1),
                    (("hf1", l, k, j), "z+", hs, 1), (("hk1", l, k, j), "z-", hs, 1)])
                tasks["D", l, k, j] = ([("hf", l, k, j), ("hk", l, k, j)], [
                    (("hg", l, k, j), "z+", hs, 1), (("hg1", l, k, j), "z-", hs, 1)])
            ys, xsz = YH * DQ * 2, R * DQ * 2
            tasks["E", l, k] = ([(m, l, k, j) for m in ("hf1", "hk1", "hg", "hg1") for j in range(NJ)] + [("wd", l, NJ), ("wu", l, NJ)], [
                (("ya", l, k), "y+", ys, 1), (("ya1", l, k), "y-", ys, 1), (("yb", l, k), "y+", ys, 1), (("yb1", l, k), "y-", ys, 1)])
            tasks["G", l, k] = ([("ya", l, k), ("ya1", l, k)], [(("yc", l, k), "y+", ys, 1), (("yc1", l, k), "y-", ys, 1)])
            three = lambda m, size, axis: [((m, l, k, 2), axis + "+", size, 2), ((m, l, k, 1), axis + "+", size, 1), ((m, l, k, 3), axis + "-", size, 1)]
            tasks["H", l, k] = ([(m, l, k) for m in ("yb", "yb1", "yc", "yc1")], three("xr", xsz, "x"))
            tasks["I", l, k] = ([("xr", l, k, d) for d in (1, 2, 3)], three("st", R * 512, "z"))
            tasks["J", l, k] = ([("st", l, k, d) for d in (1, 2, 3)], [
                (("xg2", l + 1, k), "x+", xsz if l + 1 < LAYERS else xsz // 4, 2),
                (("xg", l + 1, k), "x+", xsz if l + 1 < LAYERS else xsz // 4, 1),
                (("xg3", l + 1, k), "x-", xsz if l + 1 < LAYERS else xsz // 4, 1)])
            tasks["K", l, k][0].extend([("xg2", l + 1, k), ("xg3", l + 1, k)])
    return tasks


def order(report=None):
    tasks = plan()
    maker = {m[0]: t for t, (_, sends) in tasks.items() for m in sends}
    rank = {}

    def rest(task):
        if task not in rank:
            rank[task] = TIMES[task[0]] + max((rest(u) + 2.0 for u in users.get(task, ())), default=0.0)
        return rank[task]

    users = {}
    for t, (needs, _) in tasks.items():
        for m in needs:
            if m in maker:
                users.setdefault(maker[m], set()).add(t)
    arrive, free = {}, {}

    def transmit(sends, now, hbm=0.0):
        for m, link, size, hops in sends:
            if link == "c":
                done = max(now, free.get(link, 0.0)) + size / CORE_LINK
                arrive[m] = done + CORE_HOP + hbm
            else:
                done = max(now, free.get(link, 0.0)) + size * hops / LINK
                arrive[m] = done + HOP[hops] + hbm
            free[link] = done

    now = 3.5
    done, out = set(), []
    x_in = YB * DB * 2
    for k in range(NC):
        transmit([(("xg2", 0, k), "x+", x_in, 2), (("xg", 0, k), "x+", x_in, 1), (("xg3", 0, k), "x-", x_in, 1)], now, FROM_HBM)
        tasks["K", -1, k][0].extend([("xg2", 0, k), ("xg3", 0, k)])
        if k == 0:
            transmit(tasks["W", 0, 0][1], now, FROM_HBM)
            done.add(("W", 0, 0))
    left = [t for t in tasks if t not in done]
    after = {}
    while left:
        ready = []
        for t in left:
            needs = tasks[t][0]
            at = None
            if t[0] == "W":
                before = ("W", t[1], t[2] - 1) if t[2] else ("W", t[1] - 1, NJ)
                if before in done:
                    at = max(free["x+"], free["x-"]) - SLACK["W"]
            elif all(m in arrive for m in needs):
                at = max((arrive[m] for m in needs), default=0.0)
                if t[0] in SLACK:
                    at = max(at, max(free.get(m[1], 0.0) for m in tasks[t][1]) - SLACK[t[0]])
            if at is not None:
                ready.append((at, t))
        at, t = min(ready, key=lambda r: (max(r[0], now), -rest(r[1]), r[1][1:]))
        begin = max(now, at)
        now = begin + TIMES[t[0]]
        transmit(tasks[t][1], now, FROM_HBM if t[0] == "W" else 0.0)
        left.remove(t)
        done.add(t)
        out.append(t)
        if report is not None:
            report.append((begin, now, t))
    return out


def kernel(
    x_hbm, wg_hbm, wu_hbm, wd_hbm, gain_hbm, shift_hbm, out_hbm,
    xs, wgu, wd, rel, rel_d, part, ra, rb, rc, hid, down, ya, yb, yc, ys, xr, mixed, st, st_in, nb, ov, ga, sh,
    z_recv, z_send, y_recv, y_send, ag_recv, ag_send, w_recv, w_send, g_recv, g_send, local,
):
    ra_at, cb_at = lax.axis_index("ra"), lax.axis_index("cb")
    z, x = ra_at // 4, lax.rem(ra_at, 4)
    y, c = cb_at // 2, lax.rem(cb_at, 2)

    def turn(v, d):
        return lax.rem(v + d, 4)

    zp, zo, zm = turn(z, 1), turn(z, 2), turn(z, 3)
    yp, yo, ym = turn(y, 1), turn(y, 2), turn(y, 3)
    xp, xo, xm = turn(x, 1), turn(x, 2), turn(x, 3)

    def at_z(v):
        return (v * 4 + x, cb_at)

    def at_x(v):
        return (z * 4 + v, cb_at)

    def at_y(v):
        return (ra_at, v * 2 + c)

    other = (ra_at, y * 2 + (1 - c))

    peers = [at_z(zp), at_z(zo), at_z(zm), at_x(xp), at_x(xo), at_x(xm), at_y(yp), at_y(ym), other]
    barrier = pltpu.get_barrier_semaphore()
    for peer in peers:
        pl.semaphore_signal(barrier, inc=1, device_id=peer, device_id_type=MESH)
    pl.semaphore_wait(barrier, len(peers))

    waits = []

    def start(src, dst, send_sem, recv_sem, dev):
        copy = pltpu.make_async_remote_copy(
            src_ref=src, dst_ref=dst, send_sem=send_sem, recv_sem=recv_sem, device_id=dev, device_id_type=MESH
        )
        copy.start()
        return copy

    def send(src, dst, sems, slot, dev):
        waits.append(start(src, dst, sems[0].at[slot], sems[1].at[slot], dev).wait_send)

    def described(ref, sem):
        return pltpu.make_async_remote_copy(
            src_ref=ref, dst_ref=ref, send_sem=sem, recv_sem=sem, device_id=other, device_id_type=MESH
        )

    def arrived(dst, recv_sem):
        described(dst, recv_sem).wait_recv()

    def d_cols(v):
        return pl.ds(pl.multiple_of(v * DB, DB), DB)

    def tile_of(v):
        return jnp.minimum(v * NJ, TILES - NJ)

    def units(v, j):
        return pl.ds(pl.multiple_of((tile_of(v) + j) * UT, UT), UT)

    def gu_dst(l, j, cc, owner):
        return wgu.at[l, 2 * j + cc, d_cols(owner), :]

    def gu_half(l, j, cc, owner, what):
        return wgu.at[l, 2 * j + cc, d_cols(owner), pl.ds(what * UT, UT)]

    def d_dst(l, cc, owner):
        return wd.at[l, :, cc, :, d_cols(owner)]

    def d_half(l, cc, owner, h):
        return wd.at[l, :, cc, pl.ds(h * 64, 64), d_cols(owner)]

    local_waits = {}

    def w_sems(l, j):
        return w_send.at[l, j], w_recv.at[l, j]

    def stage_w(l, j):
        sems = w_sems(l, j)
        if j < NJ:
            send(wg_hbm.at[l, :, units(xo, j)], rel.at[l, j, 0], sems, WRM, at_x(xp))
            send(wu_hbm.at[l, :, units(xo, j)], rel.at[l, j, 1], sems, WRP, at_x(xm))
            for dev, dst_x, slot in ((at_x(xp), xp, WM), (at_x(xm), xm, WP)):
                for what, src in enumerate((wg_hbm, wu_hbm)):
                    start(src.at[l, :, units(dst_x, j)], gu_half(l, j, c, x, what), sems[0].at[slot], sems[1].at[slot], dev)
                waits.append(described(gu_dst(l, j, c, x), sems[0].at[slot]).wait_send)
            for what, src in enumerate((wg_hbm, wu_hbm)):
                start(src.at[l, :, units(x, j)], gu_half(l, j, c, x, what), sems[0].at[WD], sems[1].at[WD], other)
            waits.append(described(gu_dst(l, j, c, x), sems[0].at[WD]).wait_send)
            mine = []
            for what, src in enumerate((wg_hbm, wu_hbm)):
                copy = pltpu.make_async_copy(
                    src.at[l, :, units(x, j)], gu_half(l, j, c, x, what), local.at[l * 7 + j * 2 + what]
                )
                copy.start()
                mine.append(copy.wait)
            local_waits[l, j] = mine
        else:
            def src(v, h=None):
                if h is None:
                    return wd_hbm.at[l, pl.ds(tile_of(v), NJ)]
                return wd_hbm.at[l, pl.ds(tile_of(v), NJ), pl.ds(h * 64, 64)]

            send(src(xo, 0), rel_d.at[l, 0], sems, WRM, at_x(xp))
            send(src(xo, 1), rel_d.at[l, 1], sems, WRP, at_x(xm))
            send(src(xp), d_dst(l, c, x), sems, WM, at_x(xp))
            send(src(xm), d_dst(l, c, x), sems, WP, at_x(xm))
            send(src(x), d_dst(l, c, x), sems, WD, other)
            copy = pltpu.make_async_copy(src(x), d_dst(l, c, x), local.at[l * 7 + 6])
            copy.start()
            local_waits[l, j] = [copy.wait]

    def relay_ref(l, j, h):
        return rel.at[l, j, h] if j < NJ else rel_d.at[l, h]

    def w_half(l, j, cc, owner, h):
        return gu_half(l, j, cc, owner, h) if j < NJ else d_half(l, cc, owner, h)

    def w_whole(l, j, cc, owner):
        return gu_dst(l, j, cc, owner) if j < NJ else d_dst(l, cc, owner)

    def stage_v(l, j):
        sems = w_sems(l, j)
        arrived(relay_ref(l, j, 0), sems[1].at[WRM])
        send(relay_ref(l, j, 0), w_half(l, j, c, xm, 0), sems, WOM, at_x(xp))
        arrived(relay_ref(l, j, 1), sems[1].at[WRP])
        send(relay_ref(l, j, 1), w_half(l, j, c, xp, 1), sems, WOP, at_x(xm))

    def stage_u(l, j):
        sems = w_sems(l, j)
        for n, (owner, slot) in enumerate(((xm, WM), (xp, WP))):
            ref = w_whole(l, j, c, owner)
            arrived(ref, sems[1].at[slot])
            send(ref, ref, sems, WD + 1 + n, other)
        arrived(w_half(l, j, c, xo, 0), sems[1].at[WOM])
        arrived(w_half(l, j, c, xo, 1), sems[1].at[WOP])
        ref = w_whole(l, j, c, xo)
        send(ref, ref, sems, WD + 3, other)

    def weights_ready(l, j):
        for wait in local_waits[l, j]:
            wait()
        for n, owner in enumerate((x, xm, xp)):
            arrived(w_whole(l, j, 1 - c, owner), w_recv.at[l, j, WD + n])
        arrived(w_whole(l, j, 1 - c, xo), w_recv.at[l, j, WD + 3])

    def gathered(p, k, at, rows, cc=None):
        if p < 2:
            return xs.at[p, k, pl.ds(pl.multiple_of(at, rows), rows), :]
        base = (c if cc is None else cc) * TCORE + k * TC
        return ov.at[pl.ds(pl.multiple_of(base + at, rows), rows), :]

    def x_rows(v):
        return y * YB + v * R

    in_copies = []

    def input_send(k):
        rows = pl.ds(pl.multiple_of(c * TCORE + k * TC + y * YB, YB), YB)
        dst = xs.at[0, k, pl.ds(pl.multiple_of(y * YB, YB), YB), d_cols(x)]
        for d in (2, 1, 3):
            send(x_hbm.at[rows, :], dst, (ag_send.at[0, k], ag_recv.at[0, k]), XG + d - 1, at_x(turn(x, d)))
        copy = pltpu.make_async_copy(x_hbm.at[rows, :], dst, local.at[14 + k])
        copy.start()
        in_copies.append(copy)

    for k in range(NC):
        input_send(k)
        if k == 0:
            stage_w(0, 0)
    gain_copies = []
    for i, (src, dst) in enumerate(((gain_hbm, ga), (shift_hbm, sh))):
        for d in (1, 3, 2):
            send(src, dst.at[x], (g_send.at[i], g_recv.at[i]), d - 1, at_x(turn(x, d)))
        copy = pltpu.make_async_copy(src, dst.at[x], local.at[14 + NC + i])
        copy.start()
        gain_copies.append(copy)

    def z_sems(l, k, j):
        return z_send.at[l, k, j], z_recv.at[l, k, j]

    def y_sems(l, k):
        return y_send.at[l, k], y_recv.at[l, k]

    def ag_sems(p, k):
        return ag_send.at[p, k], ag_recv.at[p, k]

    def stage_a(l, k, j):
        if j == 0:
            sems = ag_sems(l, k)
            arrived(gathered(l, k, ym * YB + YH, YH), sems[1].at[YF1])
            arrived(gathered(l, k, yp * YB, YH), sems[1].at[YK0])
            arrived(gathered(l, k, yo * YB, YH), sems[1].at[YG0])
            arrived(gathered(l, k, yo * YB + YH, YH), sems[1].at[YG1])
        if k == 0:
            weights_ready(l, j)

        def columns(n, carry):
            cols = pl.ds(pl.multiple_of(n * 256, 256), 256)
            value = jnp.dot(xs[l, k], wgu[l, 2 * j + n], preferred_element_type=F32).astype(BF)
            for o in range(4):
                for h in (0, 1):
                    at = o * ZB + h * ZH
                    part[l, k, j, o, h, :, cols] = value[at:at + ZH]
            return carry

        lax.fori_loop(0, 2, columns, 0)
        sems = z_sems(l, k, j)
        send(part.at[l, k, j, zo, 0], ra.at[l, k, j, 0], sems, ZA0, at_z(zp))
        send(part.at[l, k, j, zo, 1], ra.at[l, k, j, 1], sems, ZA1, at_z(zm))
        send(part.at[l, k, j, zp, 1], rb.at[l, k, j, 0], sems, ZB0, at_z(zp))
        send(part.at[l, k, j, zm, 0], rb.at[l, k, j, 1], sems, ZB1, at_z(zm))

    def stage_b(l, k, j):
        sems = z_sems(l, k, j)
        for h, (to, slot, out) in enumerate(((zp, ZA0, ZC0), (zm, ZA1, ZC1))):
            arrived(ra.at[l, k, j, h], sems[1].at[slot])
            part[l, k, j, to, h] = (part[l, k, j, to, h].astype(F32) + ra[l, k, j, h].astype(F32)).astype(BF)
            send(part.at[l, k, j, to, h], rc.at[l, k, j, h], sems, out, at_z(to))

    def hid_ref(l, k, j, o, h):
        return hid.at[l, k, pl.ds(2 * j, 2), pl.ds(pl.multiple_of(o * ZB + h * ZH, ZH), ZH), :]

    def stage_c(l, k, j):
        sems = z_sems(l, k, j)
        for h in (0, 1):
            arrived(rb.at[l, k, j, 1 - h], sems[1].at[(ZB1, ZB0)[h]])
            arrived(rc.at[l, k, j, h], sems[1].at[(ZC0, ZC1)[h]])
            total = (
                part[l, k, j, z, h].astype(F32) + rc[l, k, j, h].astype(F32) + rb[l, k, j, 1 - h].astype(F32)
            )
            for n in (0, 1):
                gate, up = total[:, n * 256:n * 256 + UT], total[:, n * 256 + UT:(n + 1) * 256]
                value = gate * jax.nn.sigmoid(gate) * up
                if j < SHARED:
                    value = jnp.where(x == 3, jnp.zeros_like(value), value)
                hid[l, k, 2 * j + n, pl.ds(pl.multiple_of(z * ZB + h * ZH, ZH), ZH), :] = value.astype(BF)
        for h in (0, 1):
            ref = hid_ref(l, k, j, z, h)
            send(ref, ref, sems, (HF0, HF1)[h], at_z(zp))
            ref = hid_ref(l, k, j, z, 1 - h)
            send(ref, ref, sems, (HB1, HB0)[h], at_z(zm))

    def stage_d(l, k, j):
        sems = z_sems(l, k, j)
        ref = hid_ref(l, k, j, zm, 0)
        arrived(ref, sems[1].at[HF0])
        send(ref, ref, sems, HG0, at_z(zp))
        ref = hid_ref(l, k, j, zp, 1)
        arrived(ref, sems[1].at[HB1])
        send(ref, ref, sems, HG1, at_z(zm))

    def stage_e(l, k):
        for j in range(NJ):
            sems = z_sems(l, k, j)
            arrived(hid_ref(l, k, j, zm, 1), sems[1].at[HF1])
            arrived(hid_ref(l, k, j, zp, 0), sems[1].at[HB0])
            arrived(hid_ref(l, k, j, zo, 0), sems[1].at[HG0])
            arrived(hid_ref(l, k, j, zo, 1), sems[1].at[HG1])
        if k == 0:
            weights_ready(l, NJ)

        def columns(n, carry):
            cols = pl.ds(pl.multiple_of(n * 256, 256), 256)
            lhs = jnp.concatenate([hid[l, k, t] for t in range(NT)], axis=1)
            rhs = wd[l, :, :, :, cols].reshape(NT * UT, 256)
            value = jnp.dot(lhs, rhs, preferred_element_type=F32).astype(BF)
            for yy in range(4):
                for h in (0, 1):
                    at = yy * YB + h * YH
                    down[l, k, yy, h, :, cols] = value[at:at + YH]
            return carry

        lax.fori_loop(0, DQ // 256, columns, 0)
        sems = y_sems(l, k)
        send(down.at[l, k, yo, 0], ya.at[l, k, 0], sems, YA0, at_y(yp))
        send(down.at[l, k, yo, 1], ya.at[l, k, 1], sems, YA1, at_y(ym))
        send(down.at[l, k, yp, 1], yb.at[l, k, 0], sems, YB0, at_y(yp))
        send(down.at[l, k, ym, 0], yb.at[l, k, 1], sems, YB1, at_y(ym))

    def stage_g(l, k):
        sems = y_sems(l, k)
        for h, (to, slot, out) in enumerate(((yp, YA0, YC0), (ym, YA1, YC1))):
            arrived(ya.at[l, k, h], sems[1].at[slot])
            down[l, k, to, h] = (down[l, k, to, h].astype(F32) + ya[l, k, h].astype(F32)).astype(BF)
            send(down.at[l, k, to, h], yc.at[l, k, h], sems, out, at_y(to))

    def stage_h(l, k):
        sems = y_sems(l, k)
        for h in (0, 1):
            arrived(yb.at[l, k, 1 - h], sems[1].at[(YB1, YB0)[h]])
            arrived(yc.at[l, k, h], sems[1].at[(YC0, YC1)[h]])
            total = down[l, k, y, h].astype(F32) + yc[l, k, h].astype(F32) + yb[l, k, 1 - h].astype(F32)
            ys[l, k, 2 * h] = total[:R].astype(BF)
            ys[l, k, 2 * h + 1] = total[R:].astype(BF)
        for d in (2, 1, 3):
            send(ys.at[l, k, turn(x, d)], xr.at[l, k, d - 1], sems, XR + d - 1, at_x(turn(x, d)))

    def stage_i(l, k):
        sems = y_sems(l, k)
        rows = pl.ds(pl.multiple_of(x_rows(x), R), R)
        value = RESIDUAL * xs[l, k, rows, :].astype(F32) + ys[l, k, x].astype(F32)
        for d in (1, 3, 2):
            arrived(xr.at[l, k, d - 1], sems[1].at[XR + d - 1])
            value = value + xr[l, k, d - 1].astype(F32)
        mixed[l, k] = value
        row_sum = jnp.sum(value, axis=1, keepdims=True)
        row_squares = jnp.sum(value * value, axis=1, keepdims=True)
        lane = lax.broadcasted_iota(jnp.int32, (R, 128), 1)
        st[l, k] = jnp.where(lane == 0, row_sum, jnp.where(lane == 1, row_squares, 0.0))
        for d in (2, 1, 3):
            send(st.at[l, k], st_in.at[l, k, d - 1], sems, ST + d - 1, at_z(turn(z, d)))

    def stage_j(l, k):
        if l == 0 and k == 0:
            for i, dst in enumerate((ga, sh)):
                for d in (1, 3, 2):
                    arrived(dst.at[turn(x, 4 - d)], g_recv.at[i, d - 1])
                gain_copies[i].wait()
        stats = st[l, k]
        for d in (1, 3, 2):
            arrived(st_in.at[l, k, d - 1], y_recv.at[l, k, ST + d - 1])
            stats = stats + st_in[l, k, d - 1]
        mean = stats[:, 0:1] / D
        var = stats[:, 1:2] / D - mean * mean
        scale = lax.rsqrt(var + EPSILON)
        rows = pl.ds(pl.multiple_of(x_rows(x), R), R)
        for q in range(4):
            cols = slice(q * DB, (q + 1) * DB)
            normed = (mixed[l, k, :, cols] - mean) * scale
            value = (normed * ga[q, l:l + 1, :] + sh[q, l:l + 1, :]).astype(BF)
            if l + 1 < LAYERS:
                xs[l + 1, k, rows, cols] = value
            else:
                nb[k, q] = value
        if l + 1 == LAYERS:
            ov[pl.ds(pl.multiple_of(c * TCORE + k * TC + x_rows(x), R), R), :] = nb[k, x]
        dst = gathered(l + 1, k, x_rows(x), R)
        for d in (2, 1, 3):
            src = dst if l + 1 < LAYERS else nb.at[k, turn(x, d)]
            send(src, dst, ag_sems(l + 1, k), XG + d - 1, at_x(turn(x, d)))

    def stage_k(l, k):
        p = l + 1
        sems = ag_sems(p, k)
        for d in (1, 3, 2):
            owner = turn(x, 4 - d)
            if p == 0:
                ref = xs.at[0, k, pl.ds(pl.multiple_of(y * YB, YB), YB), d_cols(owner)]
            else:
                ref = gathered(p, k, x_rows(owner), R)
            arrived(ref, sems[1].at[XG + d - 1])
        if p == 0:
            in_copies[k].wait()
        for h in (0, 1):
            ref = gathered(p, k, y * YB + h * YH, YH)
            send(ref, ref, sems, (YF0, YF1)[h], at_y(yp))
            ref = gathered(p, k, y * YB + (1 - h) * YH, YH)
            send(ref, ref, sems, (YK1, YK0)[h], at_y(ym))
        if p == 2:
            ref = gathered(p, k, y * YB, YB)
            send(ref, ref, sems, DD, other)

    def stage_l(l, k):
        p = l + 1
        sems = ag_sems(p, k)
        ref = gathered(p, k, ym * YB, YH)
        arrived(ref, sems[1].at[YF0])
        send(ref, ref, sems, YG0, at_y(yp))
        ref = gathered(p, k, yp * YB + YH, YH)
        arrived(ref, sems[1].at[YK1])
        send(ref, ref, sems, YG1, at_y(ym))
        if p == 2:
            for n, (at, half, slot) in enumerate(((ym, 1, YF1), (yp, 0, YK0))):
                arrived(gathered(p, k, at * YB + half * YH, YH), sems[1].at[slot])
                ref = gathered(p, k, at * YB, YB)
                send(ref, ref, sems, DD + 1 + n, other)

    def stage_m(l, k):
        p = l + 1
        sems = ag_sems(p, k)
        arrived(gathered(p, k, yo * YB, YH), sems[1].at[YG0])
        arrived(gathered(p, k, yo * YB + YH, YH), sems[1].at[YG1])
        ref = gathered(p, k, yo * YB, YB)
        send(ref, ref, sems, DD + 3, other)

    stages = dict(
        A=stage_a, B=stage_b, C=stage_c, D=stage_d, E=stage_e, G=stage_g, H=stage_h, I=stage_i, J=stage_j,
        K=stage_k, L=stage_l, W=stage_w, V=stage_v, U=stage_u,
    )
    for stage, *key in order():
        stages[stage](*key)

    for k in range(NC):
        stage_m(1, k)
    out_waits = []
    for k in range(NC):
        for n, yy in enumerate((y, ym, yp, yo)):
            arrived(gathered(2, k, yy * YB, YB, 1 - c), ag_recv.at[2, k, DD + n])
    for cc in range(2):
        rows = pl.ds(cc * TCORE, TCORE)
        copy = pltpu.make_async_copy(ov.at[rows, :], out_hbm.at[rows, :], local.at[16 + NC + cc])
        copy.start()
        out_waits.append(copy.wait)
    for wait in waits:
        wait()
    for wait in out_waits:
        wait()


def solution(mesh):
    dma = pltpu.SemaphoreType.DMA

    def per_device(inputs, gate_weight, up_weight, down_weight, norm_gain, norm_shift):
        any_space = pl.BlockSpec(memory_space=pl.ANY)
        return pl.pallas_call(
            kernel,
            out_shape=jax.ShapeDtypeStruct((T, DB), BF),
            in_specs=[any_space] * 6,
            out_specs=any_space,
            scratch_shapes=[
                pltpu.VMEM((2, NC, TC, DQ), BF),
                pltpu.VMEM((2, NT, DQ, 2 * UT), BF),
                pltpu.VMEM((2, NJ, 2, UT, DQ), BF),
                pltpu.VMEM((2, NJ, 2, DB, UT), BF),
                pltpu.VMEM((2, 2, NJ, UT // 2, DB), BF),
                pltpu.VMEM((2, NC, NJ, 4, 2, ZH, 4 * UT), BF),
                pltpu.VMEM((2, NC, NJ, 2, ZH, 4 * UT), BF),
                pltpu.VMEM((2, NC, NJ, 2, ZH, 4 * UT), BF),
                pltpu.VMEM((2, NC, NJ, 2, ZH, 4 * UT), BF),
                pltpu.VMEM((2, NC, NT, TC, UT), BF),
                pltpu.VMEM((2, NC, 4, 2, YH, DQ), BF),
                pltpu.VMEM((2, NC, 2, YH, DQ), BF),
                pltpu.VMEM((2, NC, 2, YH, DQ), BF),
                pltpu.VMEM((2, NC, 2, YH, DQ), BF),
                pltpu.VMEM((2, NC, 4, R, DQ), BF),
                pltpu.VMEM((2, NC, 3, R, DQ), BF),
                pltpu.VMEM((2, NC, R, DQ), F32),
                pltpu.VMEM((2, NC, R, 128), F32),
                pltpu.VMEM((2, NC, 3, R, 128), F32),
                pltpu.VMEM((NC, 4, R, DB), BF),
                pltpu.VMEM((T, DB), BF),
                pltpu.VMEM((4, 2, DB), F32),
                pltpu.VMEM((4, 2, DB), F32),
                dma((2, NC, NJ, N_Z)),
                dma((2, NC, NJ, N_Z)),
                dma((2, NC, N_Y)),
                dma((2, NC, N_Y)),
                dma((3, NC, N_AG)),
                dma((3, NC, N_AG)),
                dma((2, NJ + 1, N_W)),
                dma((2, NJ + 1, N_W)),
                dma((2, 3)),
                dma((2, 3)),
                dma((18 + NC,)),
            ],
            compiler_params=pltpu.CompilerParams(
                collective_id=0, has_side_effects=True, vmem_limit_bytes=62 * 1024 * 1024
            ),
        )(inputs, gate_weight, up_weight, down_weight.reshape(LAYERS, TILES, UT, DB), norm_gain, norm_shift)

    return jax.shard_map(
        per_device,
        mesh=mesh,
        in_specs=(P(None, "ra"), P(None, "ra", "cb"), P(None, "ra", "cb"), P(None, "cb", "ra"), P(None, "ra"), P(None, "ra")),
        out_specs=P(None, "ra"),
        check_vma=False,
    )
```

```python
import jax
import jax.numpy as jnp
from jax import lax
from jax.experimental import pallas as pl
from jax.experimental.pallas import tpu as pltpu
from jax.sharding import PartitionSpec as P

MESH = pl.DeviceIdType.MESH
BF = jnp.bfloat16
F32 = jnp.float32
RESIDUAL = 0.5
EPSILON = 1e-05

T, D, FF, LAYERS = 1536, 4096, 11264, 2
NC = 6
TC = T // NC
ZB = TC // 4
ZH = ZB // 2
YB = TC // 4
YH = YB // 2
R = TC // 16
DB = D // 16
DQ = D // 4
UT = 128
NJ = 3
NT = 2 * NJ
TILES = FF // 8 // UT
SHARED = 4 * NJ - TILES

GROUPS = {(l, k): [(0, 1), (1, 2), (2, 3)] if l + k == 0 else [(0, 3)] for l in range(LAYERS) for k in range(NC)}

SLOTS = {}


def slots(*names):
    for name in names:
        SLOTS.setdefault(name, len(SLOTS))


for l in range(LAYERS):
    for k in range(NC):
        for g in range(len(GROUPS[l, k])):
            for m in ("za", "zb", "zc", "hf", "hk", "hg"):
                slots((m, l, k, g, 0), (m, l, k, g, 1))
        for m in ("ya", "yb", "yc"):
            slots((m, l, k, 0), (m, l, k, 1))
        for m in ("xr", "st"):
            slots((m, l, k, 1), (m, l, k, 2), (m, l, k, 3))
    for j in range(NJ + 1):
        slots(("wr", l, j, 0), ("wr", l, j, 1))
        for cc in range(2):
            slots(("wm", l, j, cc), ("wp", l, j, cc), ("wo", l, j, cc, 0), ("wo", l, j, cc, 1), ("wd", l, j, cc))
for k in range(NC):
    for p in range(LAYERS + 1):
        slots(("xg", p, k, 1), ("xg", p, k, 2), ("xg", p, k, 3))
        for m in ("yf", "yk", "yg"):
            slots((m, p, k, 0), (m, p, k, 1))
    slots(*(("dd", k, n) for n in range(4)))
slots(*(("gain", i, d) for i in range(2) for d in (1, 2, 3)))
N_SLOTS = len(SLOTS)

HOP = {1: 1.9, 2: 2.7}
CORE_HOP = 1.0
FROM_HBM = 1.1
LINK = 92e3
CORE_LINK = 500e3
START = 3.5
TIMES = dict(B=0.1, C=0.2, D=0.06, E=0.9, G=0.15, H=0.15, I=0.25, J=0.35, K=0.08, L=0.06, M=0.05, W=0.12, V=0.06)
SLACK = dict(A=0.5, E=0.5, W=0.7)


def time_of(task):
    if task[0] in "ABC" and task[0] != "":
        first, last = GROUPS[task[1], task[2]][task[3]]
        return {"A": 0.4, "B": 0.08, "C": 0.1}[task[0]] * (last - first) + 0.05
    return TIMES[task[0]]


def plan():
    tasks = {}
    for l in range(LAYERS):
        for j in range(NJ + 1):
            size = 2 * (2 * DB * UT * 2 if j < NJ else NJ * UT * DB * 2)
            tasks["W", l, j] = ([], [
                (("wr", l, j, 0), "x+", size // 2, 1), (("wr", l, j, 1), "x-", size // 2, 1),
                (("wm", l, j), "x+", size, 1), (("wp", l, j), "x-", size, 1), (("wd", l, j), "c", size // 2, 0),
            ])
            tasks["V", l, j] = ([("wr", l, j, 0), ("wr", l, j, 1)], [
                (("wo", l, j, 0), "x+", size // 2, 1), (("wo", l, j, 1), "x-", size // 2, 1)])

    def ring(one, two, keys, size, axis):
        return [((m, *keys, h), axis + "+-"[h ^ (m == two and 0)], size, 1) for m in (one, two) for h in (0, 1)]

    def pair(m, keys, size, axis):
        return [((m, *keys, 0), axis + "+", size, 1), ((m, *keys, 1), axis + "-", size, 1)]

    def three(m, keys, size, axis):
        return [((m, *keys, 2), axis + "+", size, 2), ((m, *keys, 1), axis + "+", size, 1), ((m, *keys, 3), axis + "-", size, 1)]

    def gather(one, two, keys, size, axis):
        return [
            ((one, *keys, 0), axis + "+", size, 1), ((two, *keys, 1), axis + "-", size, 1),
            ((one, *keys, 1), axis + "+", size, 1), ((two, *keys, 0), axis + "-", size, 1)]

    for k in range(NC):
        for p in range(LAYERS + 1):
            size = YH * (DQ if p < LAYERS else DB) * 2
            tasks["K", p - 1, k] = ([("xg", p, k, d) for d in (1, 2, 3)], gather("yf", "yk", (p, k), size, "y"))
            tasks["L", p - 1, k] = ([("yf", p, k, 0), ("yk", p, k, 1)], pair("yg", (p, k), size, "y"))
        tasks["M", LAYERS - 1, k] = ([("yg", LAYERS, k, h) for h in (0, 1)], [(("dd", k), "c", 2 * size, 0)])
        for l in range(LAYERS):
            for g, (first, last) in enumerate(GROUPS[l, k]):
                zs, hs = ZH * 4 * UT * 2 * (last - first), ZH * 2 * UT * 2 * (last - first)
                keys = (l, k, g)
                need = [("yg", l, k, h) for h in (0, 1)] + [("yf", l, k, 1), ("yk", l, k, 0)]
                for j in range(first, last):
                    need += [("wm", l, j), ("wp", l, j), ("wo", l, j, 0), ("wo", l, j, 1), ("wd", l, j)]
                tasks["A", *keys] = (need, pair("za", keys, zs, "z") + pair("zb", keys, zs, "z"))
                tasks["B", *keys] = ([("za", *keys, h) for h in (0, 1)], pair("zc", keys, zs, "z"))
                tasks["C", *keys] = ([(m, *keys, h) for m in ("zb", "zc") for h in (0, 1)], gather("hf", "hk", keys, hs, "z"))
                tasks["D", *keys] = ([("hf", *keys, 0), ("hk", *keys, 1)], pair("hg", keys, hs, "z"))
            need = [(m, l, k, g, h) for g in range(len(GROUPS[l, k])) for m, h in (("hf", 1), ("hk", 0), ("hg", 0), ("hg", 1))]
            need += [("wm", l, NJ), ("wp", l, NJ), ("wo", l, NJ, 0), ("wo", l, NJ, 1), ("wd", l, NJ)]
            ys, xsz = YH * DQ * 2, R * DQ * 2
            tasks["E", l, k] = (need, pair("ya", (l, k), ys, "y") + pair("yb", (l, k), ys, "y"))
            tasks["G", l, k] = ([("ya", l, k, h) for h in (0, 1)], pair("yc", (l, k), ys, "y"))
            tasks["H", l, k] = ([(m, l, k, h) for m in ("yb", "yc") for h in (0, 1)], three("xr", (l, k), xsz, "x"))
            tasks["I", l, k] = ([("xr", l, k, d) for d in (1, 2, 3)], three("st", (l, k), R * 512, "z"))
            tasks["J", l, k] = ([("st", l, k, d) for d in (1, 2, 3)], three("xg", (l + 1, k), xsz if l + 1 < LAYERS else xsz // 4, "x"))
    return tasks


def order(report=None):
    tasks = plan()
    maker = {m[0]: t for t, (_, sends) in tasks.items() for m in sends}
    users = {}
    for t, (needs, _) in tasks.items():
        for m in needs:
            if m in maker:
                users.setdefault(maker[m], set()).add(t)
    rank = {}

    def rest(task):
        if task not in rank:
            rank[task] = time_of(task) + max((rest(u) + 2.0 for u in users.get(task, ())), default=0.0)
        return rank[task]

    arrive, free = {}, {}

    def transmit(sends, now, more=0.0):
        for m, link, size, hops in sends:
            done = max(now, free.get(link, 0.0)) + (size * hops / LINK if hops else size / CORE_LINK)
            arrive[m] = done + (HOP[hops] if hops else CORE_HOP) + more
            free[link] = done

    now = START
    done, out = set(), []
    for k in range(NC):
        x_in = YB * DB * 2
        transmit([(("xg", 0, k, 2), "x+", x_in, 2), (("xg", 0, k, 1), "x+", x_in, 1), (("xg", 0, k, 3), "x-", x_in, 1)], now, FROM_HBM)
        if k == 0:
            transmit(tasks["W", 0, 0][1], now, FROM_HBM)
            done.add(("W", 0, 0))
    left = [t for t in tasks if t not in done]
    while left:
        ready = []
        for t in left:
            needs, sends = tasks[t]
            at = None
            if t[0] == "W":
                before = ("W", t[1], t[2] - 1) if t[2] else ("W", t[1] - 1, NJ)
                if before in done:
                    at = max(free["x+"], free["x-"]) - SLACK["W"]
            elif all(m in arrive for m in needs):
                at = max(arrive[m] for m in needs)
                if t[0] in SLACK:
                    at = max(at, max(free.get(m[1], 0.0) for m in sends) - SLACK[t[0]])
            if at is not None:
                ready.append((at, t))
        at, t = min(ready, key=lambda r: (max(r[0], now), r[1][0] == "W", r[1][1:3], -rest(r[1])))
        begin = max(now, at)
        now = begin + time_of(t)
        transmit(tasks[t][1], now, FROM_HBM if t[0] == "W" else 0.0)
        left.remove(t)
        done.add(t)
        out.append(t)
        if report is not None:
            report.append((begin, now, t))
    return out


def kernel(
    x_hbm, wg_hbm, wu_hbm, wd_hbm, gain_hbm, shift_hbm, out_hbm,
    xs, wgu, wd, rel, rel_d, part, ra, rb, rc, hid, down, ya, yb, yc, ys, xr, mixed, st, st_in, nb, ov, ga, sh,
    recv, sent, local, go,
):
    ra_at, cb_at = lax.axis_index("ra"), lax.axis_index("cb")
    z, x = ra_at // 4, lax.rem(ra_at, 4)
    y, c = cb_at // 2, lax.rem(cb_at, 2)

    def turn(v, d):
        return lax.rem(v + d, 4)

    zp, zo, zm = turn(z, 1), turn(z, 2), turn(z, 3)
    yp, yo, ym = turn(y, 1), turn(y, 2), turn(y, 3)
    xp, xo, xm = turn(x, 1), turn(x, 2), turn(x, 3)

    def at_z(v):
        return (v * 4 + x, cb_at)

    def at_x(v):
        return (z * 4 + v, cb_at)

    def at_x_main(v):
        return (z * 4 + v, y * 2 + 1)

    def at_y(v):
        return (ra_at, v * 2 + c)

    other = (ra_at, y * 2 + (1 - c))

    peers = [at_z(zp), at_z(zo), at_z(zm), at_x(xp), at_x(xo), at_x(xm), at_y(yp), at_y(ym), other]
    peers += [(z * 4 + xp, y * 2 + (1 - c)), (z * 4 + xm, y * 2 + (1 - c))]
    barrier = pltpu.get_barrier_semaphore()
    for peer in peers:
        pl.semaphore_signal(barrier, inc=1, device_id=peer, device_id_type=MESH)
    pl.semaphore_wait(barrier, len(peers))

    def start(src, dst, name, dev):
        copy = pltpu.make_async_remote_copy(
            src_ref=src, dst_ref=dst, send_sem=sent.at[SLOTS[name]], recv_sem=recv.at[SLOTS[name]],
            device_id=dev, device_id_type=MESH,
        )
        copy.start()
        return copy

    def described(ref, name):
        return pltpu.make_async_remote_copy(
            src_ref=ref, dst_ref=ref, send_sem=sent.at[SLOTS[name]], recv_sem=recv.at[SLOTS[name]],
            device_id=other, device_id_type=MESH,
        )

    def arrived(dst, name):
        described(dst, name).wait_recv()

    def d_cols(v):
        return pl.ds(pl.multiple_of(v * DB, DB), DB)

    def tile_of(v):
        return jnp.minimum(v * NJ, TILES - NJ)

    def units(v, j):
        return pl.ds(pl.multiple_of((tile_of(v) + j) * UT, UT), UT)

    def gu_half(l, j, cc, owner, what):
        return wgu.at[l, 2 * j + cc, d_cols(owner), pl.ds(what * UT, UT)]

    def relay_ref(l, j, h):
        return rel.at[l, j, h] if j < NJ else rel_d.at[l, h]

    def w_half(l, j, cc, owner, h):
        if j < NJ:
            return gu_half(l, j, cc, owner, h)
        return wd.at[l, :, cc, pl.ds(h * 64, 64), d_cols(owner)]

    def w_whole(l, j, cc, owner):
        return wgu.at[l, 2 * j + cc, d_cols(owner), :] if j < NJ else wd.at[l, :, cc, :, d_cols(owner)]

    def program(core):
        waits = []

        def send(src, dst, name, dev):
            waits.append(start(src, dst, name, dev).wait_send)

        local_waits = {}

        def stage_w(l, j):
            if j < NJ:
                sources = (wg_hbm, wu_hbm)
                send(wg_hbm.at[l, :, units(xo, j)], rel.at[l, j, 0], ("wr", l, j, 0), at_x(xp))
                send(wu_hbm.at[l, :, units(xo, j)], rel.at[l, j, 1], ("wr", l, j, 1), at_x(xm))
                for dst_x, m in ((xp, "wm"), (xm, "wp")):
                    for what, src in enumerate(sources):
                        start(
                            src.at[l, :, units(dst_x, j)], gu_half(l, j, core, x, what), (m, l, j, core), at_x_main(dst_x)
                        )
                    waits.append(described(w_whole(l, j, core, x), (m, l, j, core)).wait_send)
                if core == 0:
                    for what, src in enumerate(sources):
                        start(src.at[l, :, units(x, j)], gu_half(l, j, core, x, what), ("wd", l, j, core), other)
                    waits.append(described(w_whole(l, j, core, x), ("wd", l, j, core)).wait_send)
                else:
                    mine = []
                    for what, src in enumerate(sources):
                        copy = pltpu.make_async_copy(
                            src.at[l, :, units(x, j)], gu_half(l, j, core, x, what), local.at[l * 7 + j * 2 + what]
                        )
                        copy.start()
                        mine.append(copy.wait)
                    local_waits[l, j] = mine
            else:
                def src(v, h=None):
                    if h is None:
                        return wd_hbm.at[l, pl.ds(tile_of(v), NJ)]
                    return wd_hbm.at[l, pl.ds(tile_of(v), NJ), pl.ds(h * 64, 64)]

                send(src(xo, 0), rel_d.at[l, 0], ("wr", l, j, 0), at_x(xp))
                send(src(xo, 1), rel_d.at[l, 1], ("wr", l, j, 1), at_x(xm))
                send(src(xp), w_whole(l, j, core, x), ("wm", l, j, core), at_x_main(xp))
                send(src(xm), w_whole(l, j, core, x), ("wp", l, j, core), at_x_main(xm))
                if core == 0:
                    send(src(x), w_whole(l, j, core, x), ("wd", l, j, core), other)
                else:
                    copy = pltpu.make_async_copy(src(x), w_whole(l, j, core, x), local.at[l * 7 + 6])
                    copy.start()
                    local_waits[l, j] = [copy.wait]

        def stage_v(l, j):
            for h, (to, owner) in enumerate(((xp, xm), (xm, xp))):
                arrived(relay_ref(l, j, h), ("wr", l, j, h))
                send(relay_ref(l, j, h), w_half(l, j, core, owner, h), ("wo", l, j, core, h), at_x_main(to))

        if core == 0:
            stage_w(0, 0)
            for stage, *key in order():
                if stage == "W":
                    pl.semaphore_wait(go, 1)
                    stage_w(*key)
                elif stage == "V":
                    stage_v(*key)
            for k in range(NC):
                for n, yy in enumerate((y, ym, yp, yo)):
                    arrived(ov.at[pl.ds(pl.multiple_of(k * TC + yy * YB, YB), YB), :], ("dd", k, n))
            copy = pltpu.make_async_copy(ov, out_hbm, local.at[0])
            copy.start()
            for wait in waits:
                wait()
            copy.wait()
            return

        def weights_ready(l, j):
            for wait in local_waits[l, j]:
                wait()
            arrived(w_whole(l, j, 0, x), ("wd", l, j, 0))
            for cc in range(2):
                arrived(w_whole(l, j, cc, xm), ("wm", l, j, cc))
                arrived(w_whole(l, j, cc, xp), ("wp", l, j, cc))
                arrived(w_half(l, j, cc, xo, 0), ("wo", l, j, cc, 0))
                arrived(w_half(l, j, cc, xo, 1), ("wo", l, j, cc, 1))

        def gathered(p, k, at, rows):
            if p < LAYERS:
                return xs.at[p, k, pl.ds(pl.multiple_of(at, rows), rows), :]
            return ov.at[pl.ds(pl.multiple_of(k * TC + at, rows), rows), :]

        def x_rows(v):
            return y * YB + v * R

        in_copies = []

        def input_send(k):
            rows = pl.ds(pl.multiple_of(k * TC + y * YB, YB), YB)
            dst = xs.at[0, k, pl.ds(pl.multiple_of(y * YB, YB), YB), d_cols(x)]
            for d in (2, 1, 3):
                send(x_hbm.at[rows, :], dst, ("xg", 0, k, d), at_x(turn(x, d)))
            copy = pltpu.make_async_copy(x_hbm.at[rows, :], dst, local.at[14 + k])
            copy.start()
            in_copies.append(copy)

        input_send(0)
        stage_w(0, 0)
        for k in range(1, NC):
            input_send(k)
        gain_copies = []
        for i, (src, dst) in enumerate(((gain_hbm, ga), (shift_hbm, sh))):
            for d in (1, 3, 2):
                send(src, dst.at[x], ("gain", i, d), at_x(turn(x, d)))
            copy = pltpu.make_async_copy(src, dst.at[x], local.at[14 + NC + i])
            copy.start()
            gain_copies.append(copy)

        gates_ready = set()

        def stage_a(l, k, g):
            first, last = GROUPS[l, k][g]
            if g == 0:
                arrived(gathered(l, k, ym * YB + YH, YH), ("yf", l, k, 1))
                arrived(gathered(l, k, yp * YB, YH), ("yk", l, k, 0))
                arrived(gathered(l, k, yo * YB, YH), ("yg", l, k, 0))
                arrived(gathered(l, k, yo * YB + YH, YH), ("yg", l, k, 1))
            for j in range(first, last):
                if (l, j) not in gates_ready:
                    weights_ready(l, j)
                    gates_ready.add((l, j))

            def tiles(j, carry):
                for n in (0, 1):
                    value = jnp.dot(xs[l, k], wgu[l, 2 * j + n], preferred_element_type=F32).astype(BF)
                    for o in range(4):
                        for h in (0, 1):
                            at = o * ZB + h * ZH
                            part[l, k, j, o, h, :, n * 256:(n + 1) * 256] = value[at:at + ZH]
                return carry

            lax.fori_loop(first, last, tiles, 0)
            js = pl.ds(first, last - first)
            send(part.at[l, k, js, zo, 0], ra.at[l, k, js, 0], ("za", l, k, g, 0), at_z(zp))
            send(part.at[l, k, js, zo, 1], ra.at[l, k, js, 1], ("za", l, k, g, 1), at_z(zm))
            send(part.at[l, k, js, zp, 1], rb.at[l, k, js, 0], ("zb", l, k, g, 0), at_z(zp))
            send(part.at[l, k, js, zm, 0], rb.at[l, k, js, 1], ("zb", l, k, g, 1), at_z(zm))

        def stage_b(l, k, g):
            first, last = GROUPS[l, k][g]
            js = pl.ds(first, last - first)
            for h, to in enumerate((zp, zm)):
                arrived(ra.at[l, k, js, h], ("za", l, k, g, h))
                for j in range(first, last):
                    part[l, k, j, to, h] = (part[l, k, j, to, h].astype(F32) + ra[l, k, j, h].astype(F32)).astype(BF)
                send(part.at[l, k, js, to, h], rc.at[l, k, js, h], ("zc", l, k, g, h), at_z(to))

        def hid_ref(l, k, g, o, h):
            first, last = GROUPS[l, k][g]
            rows = pl.ds(pl.multiple_of(o * ZB + h * ZH, ZH), ZH)
            return hid.at[l, k, pl.ds(2 * first, 2 * (last - first)), rows, :]

        def stage_c(l, k, g):
            first, last = GROUPS[l, k][g]
            js = pl.ds(first, last - first)
            for h in (0, 1):
                arrived(rb.at[l, k, js, 1 - h], ("zb", l, k, g, 1 - h))
                arrived(rc.at[l, k, js, h], ("zc", l, k, g, h))
                for j in range(first, last):
                    total = (
                        part[l, k, j, z, h].astype(F32) + rc[l, k, j, h].astype(F32) + rb[l, k, j, 1 - h].astype(F32)
                    )
                    for n in (0, 1):
                        gate, up = total[:, n * 256:n * 256 + UT], total[:, n * 256 + UT:(n + 1) * 256]
                        value = gate * jax.nn.sigmoid(gate) * up
                        if j < SHARED:
                            value = jnp.where(x == 3, jnp.zeros_like(value), value)
                        hid[l, k, 2 * j + n, pl.ds(pl.multiple_of(z * ZB + h * ZH, ZH), ZH), :] = value.astype(BF)
                if h == 0:
                    ref = hid_ref(l, k, g, z, 0)
                    send(ref, ref, ("hf", l, k, g, 0), at_z(zp))
            ref = hid_ref(l, k, g, z, 1)
            send(ref, ref, ("hk", l, k, g, 1), at_z(zm))
            send(ref, ref, ("hf", l, k, g, 1), at_z(zp))
            ref = hid_ref(l, k, g, z, 0)
            send(ref, ref, ("hk", l, k, g, 0), at_z(zm))

        def stage_d(l, k, g):
            for h, (owner, m, to) in enumerate(((zm, "hf", zp), (zp, "hk", zm))):
                ref = hid_ref(l, k, g, owner, h)
                arrived(ref, (m, l, k, g, h))
                send(ref, ref, ("hg", l, k, g, h), at_z(to))

        def stage_e(l, k):
            for g in range(len(GROUPS[l, k])):
                arrived(hid_ref(l, k, g, zm, 1), ("hf", l, k, g, 1))
                arrived(hid_ref(l, k, g, zp, 0), ("hk", l, k, g, 0))
                arrived(hid_ref(l, k, g, zo, 0), ("hg", l, k, g, 0))
                arrived(hid_ref(l, k, g, zo, 1), ("hg", l, k, g, 1))
            if (l, NJ) not in gates_ready:
                weights_ready(l, NJ)
                gates_ready.add((l, NJ))

            def columns(n, carry):
                lhs = jnp.concatenate([hid[l, k, t] for t in range(NT)], axis=1)
                for i in (0, 1):
                    cols = pl.ds(pl.multiple_of(n * 512 + i * 256, 256), 256)
                    rhs = wd[l, :, :, :, cols].reshape(NT * UT, 256)
                    value = jnp.dot(lhs, rhs, preferred_element_type=F32).astype(BF)
                    for yy in range(4):
                        for h in (0, 1):
                            at = yy * YB + h * YH
                            down[l, k, yy, h, :, cols] = value[at:at + YH]
                return carry

            lax.fori_loop(0, DQ // 512, columns, 0)
            send(down.at[l, k, yo, 0], ya.at[l, k, 0], ("ya", l, k, 0), at_y(yp))
            send(down.at[l, k, yo, 1], ya.at[l, k, 1], ("ya", l, k, 1), at_y(ym))
            send(down.at[l, k, yp, 1], yb.at[l, k, 0], ("yb", l, k, 0), at_y(yp))
            send(down.at[l, k, ym, 0], yb.at[l, k, 1], ("yb", l, k, 1), at_y(ym))

        def stage_g(l, k):
            for h, to in enumerate((yp, ym)):
                arrived(ya.at[l, k, h], ("ya", l, k, h))
                down[l, k, to, h] = (down[l, k, to, h].astype(F32) + ya[l, k, h].astype(F32)).astype(BF)
                send(down.at[l, k, to, h], yc.at[l, k, h], ("yc", l, k, h), at_y(to))

        def stage_h(l, k):
            for h in (0, 1):
                arrived(yb.at[l, k, 1 - h], ("yb", l, k, 1 - h))
                arrived(yc.at[l, k, h], ("yc", l, k, h))
                total = down[l, k, y, h].astype(F32) + yc[l, k, h].astype(F32) + yb[l, k, 1 - h].astype(F32)
                ys[l, k, 2 * h] = total[:R].astype(BF)
                ys[l, k, 2 * h + 1] = total[R:].astype(BF)
            for d in (2, 1, 3):
                send(ys.at[l, k, turn(x, d)], xr.at[l, k, d - 1], ("xr", l, k, d), at_x(turn(x, d)))

        def stage_i(l, k):
            rows = pl.ds(pl.multiple_of(x_rows(x), R), R)
            value = RESIDUAL * xs[l, k, rows, :].astype(F32) + ys[l, k, x].astype(F32)
            for d in (1, 3, 2):
                arrived(xr.at[l, k, d - 1], ("xr", l, k, d))
                value = value + xr[l, k, d - 1].astype(F32)
            mixed[l, k] = value
            row_sum = jnp.sum(value, axis=1, keepdims=True)
            row_squares = jnp.sum(value * value, axis=1, keepdims=True)
            lane = lax.broadcasted_iota(jnp.int32, (R, 128), 1)
            st[l, k] = jnp.where(lane == 0, row_sum, jnp.where(lane == 1, row_squares, 0.0))
            for d in (2, 1, 3):
                send(st.at[l, k], st_in.at[l, k, d - 1], ("st", l, k, d), at_z(turn(z, d)))

        def stage_j(l, k):
            if l == 0 and k == 0:
                for i, dst in enumerate((ga, sh)):
                    for d in (1, 3, 2):
                        arrived(dst.at[turn(x, 4 - d)], ("gain", i, d))
                    gain_copies[i].wait()
            stats = st[l, k]
            for d in (1, 3, 2):
                arrived(st_in.at[l, k, d - 1], ("st", l, k, d))
                stats = stats + st_in[l, k, d - 1]
            mean = stats[:, 0:1] / D
            var = stats[:, 1:2] / D - mean * mean
            scale = lax.rsqrt(var + EPSILON)
            rows = pl.ds(pl.multiple_of(x_rows(x), R), R)
            for q in range(4):
                cols = slice(q * DB, (q + 1) * DB)
                normed = (mixed[l, k, :, cols] - mean) * scale
                value = (normed * ga[q, l:l + 1, :] + sh[q, l:l + 1, :]).astype(BF)
                if l + 1 < LAYERS:
                    xs[l + 1, k, rows, cols] = value
                else:
                    nb[k, q] = value
            if l + 1 == LAYERS:
                ov[pl.ds(pl.multiple_of(k * TC + x_rows(x), R), R), :] = nb[k, x]
            dst = gathered(l + 1, k, x_rows(x), R)
            for d in (2, 1, 3):
                src = dst if l + 1 < LAYERS else nb.at[k, turn(x, d)]
                send(src, dst, ("xg", l + 1, k, d), at_x(turn(x, d)))

        def stage_k(l, k):
            p = l + 1
            for d in (1, 3, 2):
                owner = turn(x, 4 - d)
                if p == 0:
                    ref = xs.at[0, k, pl.ds(pl.multiple_of(y * YB, YB), YB), d_cols(owner)]
                else:
                    ref = gathered(p, k, x_rows(owner), R)
                arrived(ref, ("xg", p, k, d))
            if p == 0:
                in_copies[k].wait()
            for h in (0, 1):
                ref = gathered(p, k, y * YB + h * YH, YH)
                send(ref, ref, ("yf", p, k, h), at_y(yp))
                ref = gathered(p, k, y * YB + (1 - h) * YH, YH)
                send(ref, ref, ("yk", p, k, 1 - h), at_y(ym))
            if p == LAYERS:
                ref = gathered(p, k, y * YB, YB)
                send(ref, ref, ("dd", k, 0), other)

        def stage_l(l, k):
            p = l + 1
            for h, (owner, m, to) in enumerate(((ym, "yf", yp), (yp, "yk", ym))):
                ref = gathered(p, k, owner * YB + h * YH, YH)
                arrived(ref, (m, p, k, h))
                send(ref, ref, ("yg", p, k, h), at_y(to))
            if p == LAYERS:
                for n, (owner, m, h) in enumerate(((ym, "yf", 1), (yp, "yk", 0))):
                    arrived(gathered(p, k, owner * YB + h * YH, YH), (m, p, k, h))
                    ref = gathered(p, k, owner * YB, YB)
                    send(ref, ref, ("dd", k, 1 + n), other)

        def stage_m(l, k):
            p = l + 1
            for h in (0, 1):
                arrived(gathered(p, k, yo * YB + h * YH, YH), ("yg", p, k, h))
            ref = gathered(p, k, yo * YB, YB)
            send(ref, ref, ("dd", k, 3), other)

        def stage_w_both(l, j):
            pl.semaphore_signal(go, inc=1, device_id=other, device_id_type=MESH)
            stage_w(l, j)

        stages = dict(
            A=stage_a, B=stage_b, C=stage_c, D=stage_d, E=stage_e, G=stage_g, H=stage_h, I=stage_i, J=stage_j,
            K=stage_k, L=stage_l, M=stage_m, W=stage_w_both, V=stage_v,
        )
        for stage, *key in order():
            stages[stage](*key)
        copy = pltpu.make_async_copy(ov, out_hbm, local.at[16 + NC])
        copy.start()
        for wait in waits:
            wait()
        copy.wait()

    @pl.when(c == 0)
    def _():
        program(0)

    @pl.when(c == 1)
    def _():
        program(1)


def solution(mesh):
    dma = pltpu.SemaphoreType.DMA

    def per_device(inputs, gate_weight, up_weight, down_weight, norm_gain, norm_shift):
        any_space = pl.BlockSpec(memory_space=pl.ANY)
        return pl.pallas_call(
            kernel,
            out_shape=jax.ShapeDtypeStruct((T, DB), BF),
            in_specs=[any_space] * 6,
            out_specs=any_space,
            scratch_shapes=[
                pltpu.VMEM((2, NC, TC, DQ), BF),
                pltpu.VMEM((2, NT, DQ, 2 * UT), BF),
                pltpu.VMEM((2, NJ, 2, UT, DQ), BF),
                pltpu.VMEM((2, NJ, 2, DB, UT), BF),
                pltpu.VMEM((2, 2, NJ, UT // 2, DB), BF),
                pltpu.VMEM((2, NC, NJ, 4, 2, ZH, 4 * UT), BF),
                pltpu.VMEM((2, NC, NJ, 2, ZH, 4 * UT), BF),
                pltpu.VMEM((2, NC, NJ, 2, ZH, 4 * UT), BF),
                pltpu.VMEM((2, NC, NJ, 2, ZH, 4 * UT), BF),
                pltpu.VMEM((2, NC, NT, TC, UT), BF),
                pltpu.VMEM((2, NC, 4, 2, YH, DQ), BF),
                pltpu.VMEM((2, NC, 2, YH, DQ), BF),
                pltpu.VMEM((2, NC, 2, YH, DQ), BF),
                pltpu.VMEM((2, NC, 2, YH, DQ), BF),
                pltpu.VMEM((2, NC, 4, R, DQ), BF),
                pltpu.VMEM((2, NC, 3, R, DQ), BF),
                pltpu.VMEM((2, NC, R, DQ), F32),
                pltpu.VMEM((2, NC, R, 128), F32),
                pltpu.VMEM((2, NC, 3, R, 128), F32),
                pltpu.VMEM((NC, 4, R, DB), BF),
                pltpu.VMEM((T, DB), BF),
                pltpu.VMEM((4, 2, DB), F32),
                pltpu.VMEM((4, 2, DB), F32),
                dma((N_SLOTS,)),
                dma((N_SLOTS,)),
                dma((17 + NC,)),
                pltpu.SemaphoreType.REGULAR,
            ],
            compiler_params=pltpu.CompilerParams(
                collective_id=0, has_side_effects=True, vmem_limit_bytes=63 * 1024 * 1024
            ),
        )(inputs, gate_weight, up_weight, down_weight.reshape(LAYERS, TILES, UT, DB), norm_gain, norm_shift)

    return jax.shard_map(
        per_device,
        mesh=mesh,
        in_specs=(P(None, "ra"), P(None, "ra", "cb"), P(None, "ra", "cb"), P(None, "cb", "ra"), P(None, "ra"), P(None, "ra")),
        out_specs=P(None, "ra"),
        check_vma=False,
    )
```

```python
import jax
import jax.numpy as jnp
from jax import lax
from jax.experimental import pallas as pl
from jax.experimental.pallas import tpu as pltpu
from jax.sharding import PartitionSpec as P

MESH = pl.DeviceIdType.MESH
BF = jnp.bfloat16
F32 = jnp.float32
RESIDUAL = 0.5
EPSILON = 1e-05

T, D, FF, LAYERS = 1536, 4096, 11264, 2
NC = 6
TC = T // NC
ZB = TC // 4
ZH = ZB // 2
YB = TC // 4
YH = YB // 2
R = TC // 16
DB = D // 16
DQ = D // 4
UT = 128
NJ = 3
NT = 2 * NJ
TILES = FF // 8 // UT
SHARED = 4 * NJ - TILES

GROUPS = {(l, k): [(0, 1), (1, 2), (2, 3)] for l in range(LAYERS) for k in range(NC)}

SLOTS = {}


def slots(*names):
    for name in names:
        SLOTS.setdefault(name, len(SLOTS))


for l in range(LAYERS):
    for k in range(NC):
        for g in range(len(GROUPS[l, k])):
            for m in ("za", "zb", "zc", "hf", "hk", "hg"):
                slots((m, l, k, g, 0), (m, l, k, g, 1))
        for m in ("ya", "yb", "yc"):
            slots((m, l, k, 0), (m, l, k, 1))
        for m in ("xr", "st"):
            slots((m, l, k, 1), (m, l, k, 2), (m, l, k, 3))
    for j in range(NJ + 1):
        slots(("wr", l, j, 0), ("wr", l, j, 1))
        for cc in range(2):
            slots(("wm", l, j, cc), ("wp", l, j, cc), ("wo", l, j, cc, 0), ("wo", l, j, cc, 1), ("wd", l, j, cc))
for k in range(NC):
    for p in range(LAYERS + 1):
        slots(("xg", p, k, 1), ("xg", p, k, 2), ("xg", p, k, 3))
        for m in ("yf", "yk", "yg"):
            slots((m, p, k, 0), (m, p, k, 1))
    slots(*(("dd", k, n) for n in range(4)), *(("xq", k, d) for d in (1, 2, 3)))
slots(*(("gain", i, d) for i in range(4) for d in (1, 2, 3)))
N_SLOTS = len(SLOTS)
N_SENT = 320
WAIT_LATER = 30

HOP = {1: 1.9, 2: 2.7}
CORE_HOP = 1.0
FROM_HBM = 1.1
LINK = 92e3
CORE_LINK = 500e3
START = 3.5
TIMES = dict(D=0.06, E=0.9, G=0.15, H=0.15, I=0.25, J=0.35, Q=0.08, K=0.08, L=0.06, M=0.05, W=0.12, V=0.06, X=0.05)
SLACK = dict(A=1.5, E=0.5, W=0.5, X=1.0)
FILL = [
    [("X", 0, 1), ("X", 0, 2), ("W", 0, 1), ("W", 0, 2), ("X", 0, 3), ("X", 0, 4), ("X", 0, 5), ("W", 0, 3)],
    [("W", 1, j) for j in range(NJ + 1)],
]
NOT_BEFORE = {("W", 1, 1): 0.0, ("W", 1, 2): 55.0, ("W", 1, 3): 60.0}
SUM_AXIS, UNIT_AXIS = "zx", "xz"


def time_of(task):
    if task[0] in "ABC":
        first, last = GROUPS[task[1], task[2]][task[3]]
        return {"A": 0.43, "B": 0.1, "C": 0.1}[task[0]] * (last - first) + 0.05
    return TIMES[task[0]]


def pair(m, keys, size, axis):
    return [((m, *keys, 0), axis + "+", size, 1), ((m, *keys, 1), axis + "-", size, 1)]


def three(m, keys, size, axis):
    return [((m, *keys, 2), axis + "+", size, 2), ((m, *keys, 1), axis + "+", size, 1), ((m, *keys, 3), axis + "-", size, 1)]


def both_ways(one, two, keys, size, axis):
    return [
        ((one, *keys, 0), axis + "+", size, 1), ((two, *keys, 1), axis + "-", size, 1),
        ((one, *keys, 1), axis + "+", size, 1), ((two, *keys, 0), axis + "-", size, 1)]


def plan():
    tasks = {}
    for l in range(LAYERS):
        axis = UNIT_AXIS[l]
        for j in range(NJ + 1):
            size = 2 * (2 * DB * UT * 2 if j < NJ else NJ * UT * DB * 2)
            tasks["W", l, j] = ([], pair("wr", (l, j), size // 2, axis) + [
                (("wm", l, j), axis + "+", size, 1), (("wp", l, j), axis + "-", size, 1), (("wd", l, j), "c", size // 2, 0)])
            tasks["V", l, j] = ([("wr", l, j, 0), ("wr", l, j, 1)], pair("wo", (l, j), size // 2, axis))
    block = YB * DB * 2
    for k in range(NC):
        tasks["X", 0, k] = ([], three("xg", (0, k), block, "x"))
        tasks["Q", 0, k] = ([("xq", k, d) for d in (1, 2, 3)], three("xg", (1, k), block, "z"))
        for p in range(LAYERS + 1):
            size = YH * (DQ if p < LAYERS else DB) * 2
            tasks["K", p - 1, k] = ([("xg", p, k, d) for d in (1, 2, 3)], both_ways("yf", "yk", (p, k), size, "y"))
            tasks["L", p - 1, k] = ([("yf", p, k, 0), ("yk", p, k, 1)], pair("yg", (p, k), size, "y"))
        tasks["M", LAYERS - 1, k] = ([("yg", LAYERS, k, h) for h in (0, 1)], [(("dd", k), "c", 2 * size, 0)])
        for l in range(LAYERS):
            axis, other_axis = SUM_AXIS[l], UNIT_AXIS[l]
            for g, (first, last) in enumerate(GROUPS[l, k]):
                zs, hs = ZH * 4 * UT * 2 * (last - first), ZH * 2 * UT * 2 * (last - first)
                keys = (l, k, g)
                need = [("yg", l, k, h) for h in (0, 1)] + [("yf", l, k, 1), ("yk", l, k, 0)]
                for j in range(first, last):
                    need += [("wm", l, j), ("wp", l, j), ("wo", l, j, 0), ("wo", l, j, 1), ("wd", l, j)]
                tasks["A", *keys] = (need, pair("za", keys, zs, axis) + pair("zb", keys, zs, axis))
                tasks["B", *keys] = ([("za", *keys, h) for h in (0, 1)], pair("zc", keys, zs, axis))
                tasks["C", *keys] = ([(m, *keys, h) for m in ("zb", "zc") for h in (0, 1)], both_ways("hf", "hk", keys, hs, axis))
                tasks["D", *keys] = ([("hf", *keys, 0), ("hk", *keys, 1)], pair("hg", keys, hs, axis))
            need = [(m, l, k, g, h) for g in range(len(GROUPS[l, k])) for m, h in (("hf", 1), ("hk", 0), ("hg", 0), ("hg", 1))]
            need += [("wm", l, NJ), ("wp", l, NJ), ("wo", l, NJ, 0), ("wo", l, NJ, 1), ("wd", l, NJ)]
            ys, xsz = YH * DQ * 2, R * DQ * 2
            tasks["E", l, k] = (need, pair("ya", (l, k), ys, "y") + pair("yb", (l, k), ys, "y"))
            tasks["G", l, k] = ([("ya", l, k, h) for h in (0, 1)], pair("yc", (l, k), ys, "y"))
            tasks["H", l, k] = ([(m, l, k, h) for m in ("yb", "yc") for h in (0, 1)], three("xr", (l, k), xsz, other_axis))
            tasks["I", l, k] = ([("xr", l, k, d) for d in (1, 2, 3)], three("st", (l, k), R * 512, axis))
            out = ("xq", (k,)) if l + 1 < LAYERS else ("xg", (l + 1, k))
            tasks["J", l, k] = ([("st", l, k, d) for d in (1, 2, 3)], three(*out, xsz // 4, other_axis))
    return tasks


def order(report=None):
    tasks = plan()
    maker = {m[0]: t for t, (_, sends) in tasks.items() for m in sends}
    users = {}
    for t, (needs, _) in tasks.items():
        for m in needs:
            if m in maker:
                users.setdefault(maker[m], set()).add(t)
    rank = {}

    def rest(task):
        if task not in rank:
            rank[task] = time_of(task) + max((rest(u) + 2.0 for u in users.get(task, ())), default=0.0)
        return rank[task]

    arrive, free = {}, {}

    def transmit(task, now):
        more = FROM_HBM if task[0] in "WX" else 0.0
        for m, link, size, hops in tasks[task][1]:
            done = max(now, free.get(link, 0.0)) + (size * hops / LINK if hops else size / CORE_LINK)
            arrive[m] = done + (HOP[hops] if hops else CORE_HOP) + more
            free[link] = done

    now = START
    fill = [list(tasks_of) for tasks_of in FILL]
    out = [("X", 0, 0), ("W", 0, 0)]
    for t in out:
        transmit(t, now)
    left = [t for t in tasks if t not in out]
    while left:
        ready = []
        for t in left:
            needs, sends = tasks[t]
            at = None
            if t[0] in "WX":
                if any(queue and queue[0] == t for queue in fill):
                    at = max(free.get(m[1], 0.0) for m in sends if m[1] != "c") - SLACK[t[0]]
                    at = max(at, NOT_BEFORE.get(t, 0.0))
            elif all(m in arrive for m in needs):
                at = max(arrive[m] for m in needs)
                if t[0] in SLACK:
                    at = max(at, max(free.get(m[1], 0.0) for m in sends) - SLACK[t[0]])
            if at is not None:
                ready.append((at, t))
        at, t = min(ready, key=lambda r: (max(r[0], now), r[1][0] in "WX", r[1][1:3], -rest(r[1])))
        begin = max(now, at)
        now = begin + time_of(t)
        for queue in fill:
            if queue and queue[0] == t:
                queue.pop(0)
        transmit(t, now)
        left.remove(t)
        out.append(t)
        if report is not None:
            report.append((begin, now, t))
    return out


def kernel(
    x_hbm, wg_hbm, wu_hbm, wd_hbm, gain_hbm, shift_hbm, out_hbm,
    xs, wgu, wd, rel, rel_d, part, ra, rb, rc, hid, down, ya, yb, yc, ys, xr, mixed, st, st_in, nb, ov, gains,
    recv, sent, local, go,
):
    ra_at, cb_at = lax.axis_index("ra"), lax.axis_index("cb")
    z, x = ra_at // 4, lax.rem(ra_at, 4)
    y, c = cb_at // 2, lax.rem(cb_at, 2)

    def turn(v, d):
        return lax.rem(v + d, 4)

    zp, zo, zm = turn(z, 1), turn(z, 2), turn(z, 3)
    yp, yo, ym = turn(y, 1), turn(y, 2), turn(y, 3)
    xp, xo, xm = turn(x, 1), turn(x, 2), turn(x, 3)

    def at_z(v):
        return (v * 4 + x, cb_at)

    def at_x(v):
        return (z * 4 + v, cb_at)

    def at_sum(l, v):
        return at_z(v) if SUM_AXIS[l] == "z" else at_x(v)

    def at_unit(l, v):
        return at_x(v) if UNIT_AXIS[l] == "x" else at_z(v)

    def at_unit_main(l, v):
        return (z * 4 + v, y * 2 + 1) if UNIT_AXIS[l] == "x" else (v * 4 + x, y * 2 + 1)

    sums = [(zp, zo, zm, z), (xp, xo, xm, x)]
    unit_at = [(xp, xo, xm, x), (zp, zo, zm, z)]

    def at_y(v):
        return (ra_at, v * 2 + c)

    other = (ra_at, y * 2 + (1 - c))

    peers = [at_z(zp), at_z(zo), at_z(zm), at_x(xp), at_x(xo), at_x(xm), at_y(yp), at_y(ym), other]
    peers += [(z * 4 + xp, y * 2 + (1 - c)), (z * 4 + xm, y * 2 + (1 - c))]
    peers += [(zp * 4 + x, y * 2 + (1 - c)), (zm * 4 + x, y * 2 + (1 - c))]
    barrier = pltpu.get_barrier_semaphore()
    for peer in peers:
        pl.semaphore_signal(barrier, inc=1, device_id=peer, device_id_type=MESH)
    pl.semaphore_wait(barrier, len(peers))

    def arrived(dst, name):
        pltpu.make_async_remote_copy(
            src_ref=dst, dst_ref=dst, send_sem=sent.at[0], recv_sem=recv.at[SLOTS[name]],
            device_id=other, device_id_type=MESH,
        ).wait_recv()

    def d_cols(v):
        return pl.ds(pl.multiple_of(v * DB, DB), DB)

    def tile_of(v):
        return jnp.minimum(v * NJ, TILES - NJ)

    def units(v, j):
        return pl.ds(pl.multiple_of((tile_of(v) + j) * UT, UT), UT)

    def gu_half(l, j, cc, owner, what):
        return wgu.at[l, 2 * j + cc, d_cols(owner), pl.ds(what * UT, UT)]

    def relay_ref(l, j, h):
        return rel.at[l, j, h] if j < NJ else rel_d.at[l, h]

    def w_half(l, j, cc, owner, h):
        if j < NJ:
            return gu_half(l, j, cc, owner, h)
        return wd.at[l, :, cc, pl.ds(h * 64, 64), d_cols(owner)]

    def w_whole(l, j, cc, owner):
        return wgu.at[l, 2 * j + cc, d_cols(owner), :] if j < NJ else wd.at[l, :, cc, :, d_cols(owner)]

    def program(core):
        waits = []
        local_waits = {}

        def send(src, dst, name, dev):
            pltpu.make_async_remote_copy(
                src_ref=src, dst_ref=dst, send_sem=sent.at[len(waits)], recv_sem=recv.at[SLOTS[name]],
                device_id=dev, device_id_type=MESH,
            ).start()

        def all_sent(like):
            waits.append(
                pltpu.make_async_remote_copy(
                    src_ref=like, dst_ref=like, send_sem=sent.at[len(waits)], recv_sem=recv.at[0],
                    device_id=other, device_id_type=MESH,
                ).wait_send
            )

        done = []

        def wait_sent(keep):
            while len(waits) - len(done) > keep:
                waits[len(done)]()
                done.append(True)

        def stage_w(l, j):
            up, opposite, back, me = unit_at[l]
            if j < NJ:
                sources = (wg_hbm, wu_hbm)
                send(wg_hbm.at[l, :, units(opposite, j)], rel.at[l, j, 0], ("wr", l, j, 0), at_unit(l, up))
                send(wu_hbm.at[l, :, units(opposite, j)], rel.at[l, j, 1], ("wr", l, j, 1), at_unit(l, back))
                for what, src in enumerate(sources):
                    for to, m in ((up, "wm"), (back, "wp")):
                        send(
                            src.at[l, :, units(to, j)], gu_half(l, j, core, me, what), (m, l, j, core), at_unit_main(l, to)
                        )
                if core == 0:
                    for what, src in enumerate(sources):
                        send(src.at[l, :, units(me, j)], gu_half(l, j, core, me, what), ("wd", l, j, core), other)
                else:
                    mine = []
                    for what, src in enumerate(sources):
                        copy = pltpu.make_async_copy(
                            src.at[l, :, units(me, j)], gu_half(l, j, core, me, what), local.at[l * 7 + j * 2 + what]
                        )
                        copy.start()
                        mine.append(copy.wait)
                    local_waits[l, j] = mine
                all_sent(wgu.at[l, 0:4 - core, 0:DB, :])
            else:
                def src(v, h=None):
                    if h is None:
                        return wd_hbm.at[l, pl.ds(tile_of(v), NJ)]
                    return wd_hbm.at[l, pl.ds(tile_of(v), NJ), pl.ds(h * 64, 64)]

                send(src(opposite, 0), rel_d.at[l, 0], ("wr", l, j, 0), at_unit(l, up))
                send(src(opposite, 1), rel_d.at[l, 1], ("wr", l, j, 1), at_unit(l, back))
                send(src(up), w_whole(l, j, core, me), ("wm", l, j, core), at_unit_main(l, up))
                send(src(back), w_whole(l, j, core, me), ("wp", l, j, core), at_unit_main(l, back))
                if core == 0:
                    send(src(me), w_whole(l, j, core, me), ("wd", l, j, core), other)
                else:
                    copy = pltpu.make_async_copy(src(me), w_whole(l, j, core, me), local.at[l * 7 + 6])
                    copy.start()
                    local_waits[l, j] = [copy.wait]
                all_sent(wgu.at[l, 0:4 - core, 0:NJ * UT, :])

        def stage_v(l, j):
            up, _, back, _ = unit_at[l]
            for h, (to, owner) in enumerate(((up, back), (back, up))):
                arrived(relay_ref(l, j, h), ("wr", l, j, h))
                send(relay_ref(l, j, h), w_half(l, j, core, owner, h), ("wo", l, j, core, h), at_unit_main(l, to))
            all_sent(wgu.at[l, 0, 0:DB if j < NJ else NJ * UT, :])

        if core == 0:
            for i, (stage, *key) in enumerate([t for t in order() if t[0] in "WV"]):
                if stage == "W":
                    if i:
                        pl.semaphore_wait(go, 1)
                    stage_w(*key)
                else:
                    stage_v(*key)
            for k in range(NC):
                for n, yy in enumerate((y, ym, yp, yo)):
                    arrived(ov.at[pl.ds(pl.multiple_of(k * TC + yy * YB, YB), YB), :], ("dd", k, n))
            copy = pltpu.make_async_copy(ov, out_hbm, local.at[0])
            copy.start()
            wait_sent(0)
            copy.wait()
            return

        def weights_ready(l, j):
            up, opposite, back, me = unit_at[l]
            for wait in local_waits[l, j]:
                wait()
            arrived(w_whole(l, j, 0, me), ("wd", l, j, 0))
            for cc in range(2):
                arrived(w_whole(l, j, cc, back), ("wm", l, j, cc))
                arrived(w_whole(l, j, cc, up), ("wp", l, j, cc))
                arrived(w_half(l, j, cc, opposite, 0), ("wo", l, j, cc, 0))
                arrived(w_half(l, j, cc, opposite, 1), ("wo", l, j, cc, 1))

        def gathered(p, k, at, rows):
            if p < LAYERS:
                return xs.at[p, k, pl.ds(pl.multiple_of(at, rows), rows), :]
            return ov.at[pl.ds(pl.multiple_of(k * TC + at, rows), rows), :]

        def part_rows(v):
            return y * YB + v * R

        in_copies = {}
        y_block = pl.ds(pl.multiple_of(y * YB, YB), YB)

        def stage_x(l, k):
            rows = pl.ds(pl.multiple_of(k * TC + y * YB, YB), YB)
            dst = xs.at[0, k, y_block, d_cols(x)]
            for d in (2, 1, 3):
                send(x_hbm.at[rows, :], dst, ("xg", 0, k, d), at_x(turn(x, d)))
            all_sent(ov.at[0:3 * YB, :])
            in_copies[k] = pltpu.make_async_copy(x_hbm.at[rows, :], dst, local.at[14 + k])
            in_copies[k].start()

        gain_copies = []

        def gains_send():
            for i, (src, axis) in enumerate(((gain_hbm, 0), (shift_hbm, 0), (gain_hbm, 1), (shift_hbm, 1))):
                me = unit_at[axis][3]
                for d in (1, 3, 2):
                    send(src, gains.at[i, me], ("gain", i, d), at_unit(axis, turn(me, d)))
                all_sent(gains.at[i, 0:3])
                copy = pltpu.make_async_copy(src, gains.at[i, me], local.at[14 + NC + i])
                copy.start()
                gain_copies.append(copy)

        seen = set()

        def stage_a(l, k, g):
            first, last = GROUPS[l, k][g]
            if g == 0:
                arrived(gathered(l, k, ym * YB + YH, YH), ("yf", l, k, 1))
                arrived(gathered(l, k, yp * YB, YH), ("yk", l, k, 0))
                arrived(gathered(l, k, yo * YB, YH), ("yg", l, k, 0))
                arrived(gathered(l, k, yo * YB + YH, YH), ("yg", l, k, 1))
            for j in range(first, last):
                if (l, j) not in seen:
                    weights_ready(l, j)
                    seen.add((l, j))

            def tiles(j, carry):
                for n in (0, 1):
                    value = jnp.dot(xs[l, k], wgu[l, 2 * j + n], preferred_element_type=F32).astype(BF)
                    for o in range(4):
                        for h in (0, 1):
                            at = o * ZB + h * ZH
                            part[l, k, j, o, h, :, n * 256:(n + 1) * 256] = value[at:at + ZH]
                return carry

            lax.fori_loop(first, last, tiles, 0)
            js = pl.ds(first, last - first)
            up, opposite, back, _ = sums[l]
            send(part.at[l, k, js, opposite, 0], ra.at[l, k, js, 0], ("za", l, k, g, 0), at_sum(l, up))
            send(part.at[l, k, js, opposite, 1], ra.at[l, k, js, 1], ("za", l, k, g, 1), at_sum(l, back))
            send(part.at[l, k, js, up, 1], rb.at[l, k, js, 0], ("zb", l, k, g, 0), at_sum(l, up))
            send(part.at[l, k, js, back, 0], rb.at[l, k, js, 1], ("zb", l, k, g, 1), at_sum(l, back))
            all_sent(part.at[l, k, js, 0:2])

        def stage_b(l, k, g):
            first, last = GROUPS[l, k][g]
            js = pl.ds(first, last - first)
            up, _, back, _ = sums[l]
            for h, to in enumerate((up, back)):
                arrived(ra.at[l, k, js, h], ("za", l, k, g, h))
                for j in range(first, last):
                    part[l, k, j, to, h] = (part[l, k, j, to, h].astype(F32) + ra[l, k, j, h].astype(F32)).astype(BF)
                send(part.at[l, k, js, to, h], rc.at[l, k, js, h], ("zc", l, k, g, h), at_sum(l, to))
            all_sent(part.at[l, k, js, 0])

        def hid_ref(l, k, g, o, h):
            first, last = GROUPS[l, k][g]
            rows = pl.ds(pl.multiple_of(o * ZB + h * ZH, ZH), ZH)
            return hid.at[l, k, pl.ds(2 * first, 2 * (last - first)), rows, :]

        def stage_c(l, k, g):
            first, last = GROUPS[l, k][g]
            js = pl.ds(first, last - first)
            up, _, back, me = sums[l]
            for h in (0, 1):
                arrived(rb.at[l, k, js, 1 - h], ("zb", l, k, g, 1 - h))
                arrived(rc.at[l, k, js, h], ("zc", l, k, g, h))
                for j in range(first, last):
                    total = (
                        part[l, k, j, me, h].astype(F32) + rc[l, k, j, h].astype(F32) + rb[l, k, j, 1 - h].astype(F32)
                    )
                    for n in (0, 1):
                        gate, lift = total[:, n * 256:n * 256 + UT], total[:, n * 256 + UT:(n + 1) * 256]
                        value = gate * jax.nn.sigmoid(gate) * lift
                        if j < SHARED:
                            value = jnp.where(unit_at[l][3] == 3, jnp.zeros_like(value), value)
                        hid[l, k, 2 * j + n, pl.ds(pl.multiple_of(me * ZB + h * ZH, ZH), ZH), :] = value.astype(BF)
                if h == 0:
                    ref = hid_ref(l, k, g, me, 0)
                    send(ref, ref, ("hf", l, k, g, 0), at_sum(l, up))
            ref = hid_ref(l, k, g, me, 1)
            send(ref, ref, ("hk", l, k, g, 1), at_sum(l, back))
            send(ref, ref, ("hf", l, k, g, 1), at_sum(l, up))
            ref = hid_ref(l, k, g, me, 0)
            send(ref, ref, ("hk", l, k, g, 0), at_sum(l, back))
            all_sent(hid.at[l, k, pl.ds(2 * first, 2 * (last - first)), 0:4 * ZH, :])

        def stage_d(l, k, g):
            first, last = GROUPS[l, k][g]
            up, _, back, _ = sums[l]
            for h, (owner, m, to) in enumerate(((back, "hf", up), (up, "hk", back))):
                ref = hid_ref(l, k, g, owner, h)
                arrived(ref, (m, l, k, g, h))
                send(ref, ref, ("hg", l, k, g, h), at_sum(l, to))
            all_sent(hid.at[l, k, pl.ds(2 * first, 2 * (last - first)), 0:2 * ZH, :])

        def stage_e(l, k):
            up, opposite, back, _ = sums[l]
            for g in range(len(GROUPS[l, k])):
                arrived(hid_ref(l, k, g, back, 1), ("hf", l, k, g, 1))
                arrived(hid_ref(l, k, g, up, 0), ("hk", l, k, g, 0))
                arrived(hid_ref(l, k, g, opposite, 0), ("hg", l, k, g, 0))
                arrived(hid_ref(l, k, g, opposite, 1), ("hg", l, k, g, 1))
            if (l, NJ) not in seen:
                weights_ready(l, NJ)
                seen.add((l, NJ))

            def columns(n, carry):
                lhs = jnp.concatenate([hid[l, k, t] for t in range(NT)], axis=1)
                for i in (0, 1):
                    cols = pl.ds(pl.multiple_of(n * 512 + i * 256, 256), 256)
                    rhs = wd[l, :, :, :, cols].reshape(NT * UT, 256)
                    value = jnp.dot(lhs, rhs, preferred_element_type=F32).astype(BF)
                    for yy in range(4):
                        for h in (0, 1):
                            at = yy * YB + h * YH
                            down[l, k, yy, h, :, cols] = value[at:at + YH]
                return carry

            lax.fori_loop(0, DQ // 512, columns, 0)
            send(down.at[l, k, yo, 0], ya.at[l, k, 0], ("ya", l, k, 0), at_y(yp))
            send(down.at[l, k, yo, 1], ya.at[l, k, 1], ("ya", l, k, 1), at_y(ym))
            send(down.at[l, k, yp, 1], yb.at[l, k, 0], ("yb", l, k, 0), at_y(yp))
            send(down.at[l, k, ym, 0], yb.at[l, k, 1], ("yb", l, k, 1), at_y(ym))
            all_sent(down.at[l, k, 0:2])

        def stage_g(l, k):
            for h, to in enumerate((yp, ym)):
                arrived(ya.at[l, k, h], ("ya", l, k, h))
                down[l, k, to, h] = (down[l, k, to, h].astype(F32) + ya[l, k, h].astype(F32)).astype(BF)
                send(down.at[l, k, to, h], yc.at[l, k, h], ("yc", l, k, h), at_y(to))
            all_sent(down.at[l, k, 0])

        def stage_h(l, k):
            for h in (0, 1):
                arrived(yb.at[l, k, 1 - h], ("yb", l, k, 1 - h))
                arrived(yc.at[l, k, h], ("yc", l, k, h))
                total = down[l, k, y, h].astype(F32) + yc[l, k, h].astype(F32) + yb[l, k, 1 - h].astype(F32)
                ys[l, k, 2 * h] = total[:R].astype(BF)
                ys[l, k, 2 * h + 1] = total[R:].astype(BF)
            me = unit_at[l][3]
            for d in (2, 1, 3):
                send(ys.at[l, k, turn(me, d)], xr.at[l, k, d - 1], ("xr", l, k, d), at_unit(l, turn(me, d)))
            all_sent(ys.at[l, k, 0:3])

        def stage_i(l, k):
            me = unit_at[l][3]
            rows = pl.ds(pl.multiple_of(part_rows(me), R), R)
            value = RESIDUAL * xs[l, k, rows, :].astype(F32) + ys[l, k, me].astype(F32)
            for d in (1, 3, 2):
                arrived(xr.at[l, k, d - 1], ("xr", l, k, d))
                value = value + xr[l, k, d - 1].astype(F32)
            mixed[l, k] = value
            row_sum = jnp.sum(value, axis=1, keepdims=True)
            row_squares = jnp.sum(value * value, axis=1, keepdims=True)
            lane = lax.broadcasted_iota(jnp.int32, (R, 128), 1)
            st[l, k] = jnp.where(lane == 0, row_sum, jnp.where(lane == 1, row_squares, 0.0))
            for d in (2, 1, 3):
                send(st.at[l, k], st_in.at[l, k, d - 1], ("st", l, k, d), at_sum(l, turn(sums[l][3], d)))
            all_sent(st_in.at[l, k])

        def stage_j(l, k):
            me = unit_at[l][3]
            if ("gain", l) not in seen:
                seen.add(("gain", l))
                for i in (2 * l, 2 * l + 1):
                    for d in (1, 3, 2):
                        arrived(gains.at[i, turn(me, 4 - d)], ("gain", i, d))
                    gain_copies[i].wait()
            stats = st[l, k]
            for d in (1, 3, 2):
                arrived(st_in.at[l, k, d - 1], ("st", l, k, d))
                stats = stats + st_in[l, k, d - 1]
            mean = stats[:, 0:1] / D
            var = stats[:, 1:2] / D - mean * mean
            scale = lax.rsqrt(var + EPSILON)
            for q in range(4):
                cols = slice(q * DB, (q + 1) * DB)
                normed = (mixed[l, k, :, cols] - mean) * scale
                nb[l, k, q] = (normed * gains[2 * l, q, l:l + 1, :] + gains[2 * l + 1, q, l:l + 1, :]).astype(BF)

            if l + 1 < LAYERS:
                dst = xs.at[1, k, pl.ds(pl.multiple_of(part_rows(me), R), R), d_cols(z)]
            else:
                dst = gathered(LAYERS, k, part_rows(me), R)
            dst[...] = nb[l, k, me]
            for d in (2, 1, 3):
                name = ("xq", k, d) if l + 1 < LAYERS else ("xg", LAYERS, k, d)
                send(nb.at[l, k, turn(me, d)], dst, name, at_unit(l, turn(me, d)))
            all_sent(nb.at[l, k, 0:3])

        def stage_q(l, k):
            for d in (1, 3, 2):
                rows = pl.ds(pl.multiple_of(part_rows(turn(x, 4 - d)), R), R)
                arrived(xs.at[1, k, rows, d_cols(z)], ("xq", k, d))
            ref = xs.at[1, k, y_block, d_cols(z)]
            for d in (2, 1, 3):
                send(ref, ref, ("xg", 1, k, d), at_z(turn(z, d)))
            all_sent(ov.at[0:3 * YB, :])

        def stage_k(l, k):
            p = l + 1
            for d in (1, 3, 2):
                owner = turn(x if p == 0 else z, 4 - d)
                if p < LAYERS:
                    ref = xs.at[p, k, y_block, d_cols(owner)]
                else:
                    ref = gathered(p, k, part_rows(owner), R)
                arrived(ref, ("xg", p, k, d))
            if p == 0:
                in_copies[k].wait()
            for h in (0, 1):
                ref = gathered(p, k, y * YB + h * YH, YH)
                send(ref, ref, ("yf", p, k, h), at_y(yp))
                ref = gathered(p, k, y * YB + (1 - h) * YH, YH)
                send(ref, ref, ("yk", p, k, 1 - h), at_y(ym))
            if p == LAYERS:
                ref = gathered(p, k, y * YB, YB)
                send(ref, ref, ("dd", k, 0), other)
                all_sent(ov.at[0:6 * YH, :])
            else:
                all_sent(xs.at[p, k, 0:4 * YH, :])

        def stage_l(l, k):
            p = l + 1
            for h, (owner, m, to) in enumerate(((ym, "yf", yp), (yp, "yk", ym))):
                ref = gathered(p, k, owner * YB + h * YH, YH)
                arrived(ref, (m, p, k, h))
                send(ref, ref, ("yg", p, k, h), at_y(to))
            if p == LAYERS:
                for n, (owner, m, h) in enumerate(((ym, "yf", 1), (yp, "yk", 0))):
                    arrived(gathered(p, k, owner * YB + h * YH, YH), (m, p, k, h))
                    ref = gathered(p, k, owner * YB, YB)
                    send(ref, ref, ("dd", k, 1 + n), other)
                all_sent(ov.at[0:6 * YH, :])
            else:
                all_sent(xs.at[p, k, 0:2 * YH, :])

        def stage_m(l, k):
            p = l + 1
            for h in (0, 1):
                arrived(gathered(p, k, yo * YB + h * YH, YH), ("yg", p, k, h))
            ref = gathered(p, k, yo * YB, YB)
            send(ref, ref, ("dd", k, 3), other)
            all_sent(ov.at[0:YB, :])

        def stage_w_both(l, j):
            if l + j == 0:
                stage_w(l, j)
                gains_send()
                return
            pl.semaphore_signal(go, inc=1, device_id=other, device_id_type=MESH)
            stage_w(l, j)

        stages = dict(
            A=stage_a, B=stage_b, C=stage_c, D=stage_d, E=stage_e, G=stage_g, H=stage_h, I=stage_i, J=stage_j,
            K=stage_k, L=stage_l, M=stage_m, Q=stage_q, W=stage_w_both, V=stage_v, X=stage_x,
        )
        for stage, *key in order():
            stages[stage](*key)
            wait_sent(WAIT_LATER)
        copy = pltpu.make_async_copy(ov, out_hbm, local.at[18 + NC])
        copy.start()
        wait_sent(0)
        copy.wait()

    @pl.when(c == 0)
    def _():
        program(0)

    @pl.when(c == 1)
    def _():
        program(1)


def solution(mesh):
    dma = pltpu.SemaphoreType.DMA

    def per_device(inputs, gate_weight, up_weight, down_weight, norm_gain, norm_shift):
        any_space = pl.BlockSpec(memory_space=pl.ANY)
        return pl.pallas_call(
            kernel,
            out_shape=jax.ShapeDtypeStruct((T, DB), BF),
            in_specs=[any_space] * 6,
            out_specs=any_space,
            scratch_shapes=[
                pltpu.VMEM((2, NC, TC, DQ), BF),
                pltpu.VMEM((2, NT, DQ, 2 * UT), BF),
                pltpu.VMEM((2, NJ, 2, UT, DQ), BF),
                pltpu.VMEM((2, NJ, 2, DB, UT), BF),
                pltpu.VMEM((2, 2, NJ, UT // 2, DB), BF),
                pltpu.VMEM((2, NC, NJ, 4, 2, ZH, 4 * UT), BF),
                pltpu.VMEM((2, NC, NJ, 2, ZH, 4 * UT), BF),
                pltpu.VMEM((2, NC, NJ, 2, ZH, 4 * UT), BF),
                pltpu.VMEM((2, NC, NJ, 2, ZH, 4 * UT), BF),
                pltpu.VMEM((2, NC, NT, TC, UT), BF),
                pltpu.VMEM((2, NC, 4, 2, YH, DQ), BF),
                pltpu.VMEM((2, NC, 2, YH, DQ), BF),
                pltpu.VMEM((2, NC, 2, YH, DQ), BF),
                pltpu.VMEM((2, NC, 2, YH, DQ), BF),
                pltpu.VMEM((2, NC, 4, R, DQ), BF),
                pltpu.VMEM((2, NC, 3, R, DQ), BF),
                pltpu.VMEM((2, NC, R, DQ), F32),
                pltpu.VMEM((2, NC, R, 128), F32),
                pltpu.VMEM((2, NC, 3, R, 128), F32),
                pltpu.VMEM((2, NC, 4, R, DB), BF),
                pltpu.VMEM((T, DB), BF),
                pltpu.VMEM((4, 4, 2, DB), F32),
                dma((N_SLOTS,)),
                dma((N_SENT,)),
                dma((19 + NC,)),
                pltpu.SemaphoreType.REGULAR,
            ],
            compiler_params=pltpu.CompilerParams(
                collective_id=0, has_side_effects=True, vmem_limit_bytes=63 * 1024 * 1024
            ),
        )(inputs, gate_weight, up_weight, down_weight.reshape(LAYERS, TILES, UT, DB), norm_gain, norm_shift)

    return jax.shard_map(
        per_device,
        mesh=mesh,
        in_specs=(P(None, "ra"), P(None, "ra", "cb"), P(None, "ra", "cb"), P(None, "cb", "ra"), P(None, "ra"), P(None, "ra")),
        out_specs=P(None, "ra"),
        check_vma=False,
    )
```

```python
import jax
import jax.numpy as jnp
from jax import lax
from jax.experimental import pallas as pl
from jax.experimental.pallas import tpu as pltpu
from jax.sharding import PartitionSpec as P

MESH = pl.DeviceIdType.MESH
BF = jnp.bfloat16
F32 = jnp.float32
RESIDUAL = 0.5
EPSILON = 1e-05

T, D, FF, LAYERS = 1536, 4096, 11264, 2
NC = 6
TC = T // NC
ZB = TC // 4
ZH = ZB // 2
YB = TC // 4
YH = YB // 2
R = TC // 16
DB = D // 16
DQ = D // 4
UT = 128
NJ = 3
NT = 2 * NJ
TILES = FF // 8 // UT
SHARED = 4 * NJ - TILES

GROUPS = {(l, k): [(0, 1), (1, 2), (2, 3)] for l in range(LAYERS) for k in range(NC)}

SLOTS = {}


def slots(*names):
    for name in names:
        SLOTS.setdefault(name, len(SLOTS))


for k in range(NC):
    for g in range(max(len(GROUPS[l, k]) for l in range(LAYERS))):
        slots(("za", k, g), ("zc", k, g), ("h0", k, g))
    slots(*((m, k) for m in ("h1", "ya", "yc", "xr", "st", "xq", "xg", "y0", "y1", "y2")))
for l in range(LAYERS):
    for j in range(NJ + 1):
        slots(("wr", l, j), ("w", l, j))
slots(("dd",), ("gain",))
N_SLOTS = len(SLOTS)
N_SENT = 40
WAIT_LATER = 30

HOP = {1: 1.9, 2: 2.7}
CORE_HOP = 1.0
FROM_HBM = 1.1
LINK = 92e3
CORE_LINK = 500e3
START = 3.5
TIMES = dict(D=0.06, E=0.9, G=0.15, H=0.15, I=0.25, J=0.35, Q=0.08, K=0.08, L=0.06, M=0.05, W=0.12, V=0.06, X=0.05)
SLACK = dict(A=1.5, E=0.5, W=0.5, X=1.0)
FILL = [
    [("X", 0, 1), ("X", 0, 2), ("W", 0, 1), ("W", 0, 2), ("X", 0, 3), ("X", 0, 4), ("X", 0, 5), ("W", 0, 3)],
    [("W", 1, j) for j in range(NJ + 1)],
]
NOT_BEFORE = {("W", 1, 1): 0.0, ("W", 1, 2): 55.0, ("W", 1, 3): 60.0}
SUM_AXIS, UNIT_AXIS = "zx", "xz"


def time_of(task):
    if task[0] in "ABC":
        first, last = GROUPS[task[1], task[2]][task[3]]
        return {"A": 0.43, "B": 0.1, "C": 0.1}[task[0]] * (last - first) + 0.05
    return TIMES[task[0]]


def pair(m, keys, size, axis):
    return [((m, *keys, 0), axis + "+", size, 1), ((m, *keys, 1), axis + "-", size, 1)]


def three(m, keys, size, axis):
    return [((m, *keys, 2), axis + "+", size, 2), ((m, *keys, 1), axis + "+", size, 1), ((m, *keys, 3), axis + "-", size, 1)]


def both_ways(one, two, keys, size, axis):
    return [
        ((one, *keys, 0), axis + "+", size, 1), ((two, *keys, 1), axis + "-", size, 1),
        ((one, *keys, 1), axis + "+", size, 1), ((two, *keys, 0), axis + "-", size, 1)]


def plan():
    tasks = {}
    for l in range(LAYERS):
        axis = UNIT_AXIS[l]
        for j in range(NJ + 1):
            size = 2 * (2 * DB * UT * 2 if j < NJ else NJ * UT * DB * 2)
            tasks["W", l, j] = ([], pair("wr", (l, j), size // 2, axis) + [
                (("wm", l, j), axis + "+", size, 1), (("wp", l, j), axis + "-", size, 1), (("wd", l, j), "c", size // 2, 0)])
            tasks["V", l, j] = ([("wr", l, j, 0), ("wr", l, j, 1)], pair("wo", (l, j), size // 2, axis))
    block = YB * DB * 2
    for k in range(NC):
        tasks["X", 0, k] = ([], three("xg", (0, k), block, "x"))
        tasks["Q", 0, k] = ([("xq", k, d) for d in (1, 2, 3)], three("xg", (1, k), block, "z"))
        for p in range(LAYERS + 1):
            size = YH * (DQ if p < LAYERS else DB) * 2
            tasks["K", p - 1, k] = ([("xg", p, k, d) for d in (1, 2, 3)], both_ways("yf", "yk", (p, k), size, "y"))
            tasks["L", p - 1, k] = ([("yf", p, k, 0), ("yk", p, k, 1)], pair("yg", (p, k), size, "y"))
        tasks["M", LAYERS - 1, k] = ([("yg", LAYERS, k, h) for h in (0, 1)], [(("dd", k), "c", 2 * size, 0)])
        for l in range(LAYERS):
            axis, other_axis = SUM_AXIS[l], UNIT_AXIS[l]
            for g, (first, last) in enumerate(GROUPS[l, k]):
                zs, hs = ZH * 4 * UT * 2 * (last - first), ZH * 2 * UT * 2 * (last - first)
                keys = (l, k, g)
                need = [("yg", l, k, h) for h in (0, 1)] + [("yf", l, k, 1), ("yk", l, k, 0)]
                for j in range(first, last):
                    need += [("wm", l, j), ("wp", l, j), ("wo", l, j, 0), ("wo", l, j, 1), ("wd", l, j)]
                tasks["A", *keys] = (need, pair("za", keys, zs, axis) + pair("zb", keys, zs, axis))
                tasks["B", *keys] = ([("za", *keys, h) for h in (0, 1)], pair("zc", keys, zs, axis))
                tasks["C", *keys] = ([(m, *keys, h) for m in ("zb", "zc") for h in (0, 1)], both_ways("hf", "hk", keys, hs, axis))
                tasks["D", *keys] = ([("hf", *keys, 0), ("hk", *keys, 1)], pair("hg", keys, hs, axis))
            need = [(m, l, k, g, h) for g in range(len(GROUPS[l, k])) for m, h in (("hf", 1), ("hk", 0), ("hg", 0), ("hg", 1))]
            need += [("wm", l, NJ), ("wp", l, NJ), ("wo", l, NJ, 0), ("wo", l, NJ, 1), ("wd", l, NJ)]
            ys, xsz = YH * DQ * 2, R * DQ * 2
            tasks["E", l, k] = (need, pair("ya", (l, k), ys, "y") + pair("yb", (l, k), ys, "y"))
            tasks["G", l, k] = ([("ya", l, k, h) for h in (0, 1)], pair("yc", (l, k), ys, "y"))
            tasks["H", l, k] = ([(m, l, k, h) for m in ("yb", "yc") for h in (0, 1)], three("xr", (l, k), xsz, other_axis))
            tasks["I", l, k] = ([("xr", l, k, d) for d in (1, 2, 3)], three("st", (l, k), R * 512, axis))
            out = ("xq", (k,)) if l + 1 < LAYERS else ("xg", (l + 1, k))
            tasks["J", l, k] = ([("st", l, k, d) for d in (1, 2, 3)], three(*out, xsz // 4, other_axis))
    return tasks


def order(report=None):
    tasks = plan()
    maker = {m[0]: t for t, (_, sends) in tasks.items() for m in sends}
    users = {}
    for t, (needs, _) in tasks.items():
        for m in needs:
            if m in maker:
                users.setdefault(maker[m], set()).add(t)
    rank = {}

    def rest(task):
        if task not in rank:
            rank[task] = time_of(task) + max((rest(u) + 2.0 for u in users.get(task, ())), default=0.0)
        return rank[task]

    arrive, free = {}, {}

    def transmit(task, now):
        more = FROM_HBM if task[0] in "WX" else 0.0
        for m, link, size, hops in tasks[task][1]:
            done = max(now, free.get(link, 0.0)) + (size * hops / LINK if hops else size / CORE_LINK)
            arrive[m] = done + (HOP[hops] if hops else CORE_HOP) + more
            free[link] = done

    now = START
    fill = [list(tasks_of) for tasks_of in FILL]
    out = [("X", 0, 0), ("W", 0, 0)]
    for t in out:
        transmit(t, now)
    left = [t for t in tasks if t not in out]
    while left:
        ready = []
        for t in left:
            needs, sends = tasks[t]
            at = None
            if t[0] in "WX":
                if any(queue and queue[0] == t for queue in fill):
                    at = max(free.get(m[1], 0.0) for m in sends if m[1] != "c") - SLACK[t[0]]
                    at = max(at, NOT_BEFORE.get(t, 0.0))
            elif all(m in arrive for m in needs):
                at = max(arrive[m] for m in needs)
                if t[0] in SLACK:
                    at = max(at, max(free.get(m[1], 0.0) for m in sends) - SLACK[t[0]])
            if at is not None:
                ready.append((at, t))
        at, t = min(ready, key=lambda r: (max(r[0], now), r[1][0] in "WX", r[1][1:3], -rest(r[1])))
        begin = max(now, at)
        now = begin + time_of(t)
        for queue in fill:
            if queue and queue[0] == t:
                queue.pop(0)
        transmit(t, now)
        left.remove(t)
        out.append(t)
        if report is not None:
            report.append((begin, now, t))
    return out


def kernel(
    x_hbm, wg_hbm, wu_hbm, wd_hbm, gain_hbm, shift_hbm, out_hbm,
    xs, wgu, wd, rel, rel_d, part, ra, rb, rc, hid, down, ya, yb, yc, ys, xr, mixed, st, st_in, nb, ov, gains,
    recv, sent, local, go,
):
    ra_at, cb_at = lax.axis_index("ra"), lax.axis_index("cb")
    z, x = ra_at // 4, lax.rem(ra_at, 4)
    y, c = cb_at // 2, lax.rem(cb_at, 2)

    def turn(v, d):
        return lax.rem(v + d, 4)

    zp, zo, zm = turn(z, 1), turn(z, 2), turn(z, 3)
    yp, yo, ym = turn(y, 1), turn(y, 2), turn(y, 3)
    xp, xo, xm = turn(x, 1), turn(x, 2), turn(x, 3)

    def at_z(v):
        return (v * 4 + x, cb_at)

    def at_x(v):
        return (z * 4 + v, cb_at)

    def at_sum(l, v):
        return at_z(v) if SUM_AXIS[l] == "z" else at_x(v)

    def at_unit(l, v):
        return at_x(v) if UNIT_AXIS[l] == "x" else at_z(v)

    def at_unit_main(l, v):
        return (z * 4 + v, y * 2 + 1) if UNIT_AXIS[l] == "x" else (v * 4 + x, y * 2 + 1)

    sums = [(zp, zo, zm, z), (xp, xo, xm, x)]
    unit_at = [(xp, xo, xm, x), (zp, zo, zm, z)]

    def at_y(v):
        return (ra_at, v * 2 + c)

    other = (ra_at, y * 2 + (1 - c))

    peers = [at_z(zp), at_z(zo), at_z(zm), at_x(xp), at_x(xo), at_x(xm), at_y(yp), at_y(ym), other]
    peers += [(z * 4 + xp, y * 2 + (1 - c)), (z * 4 + xm, y * 2 + (1 - c))]
    peers += [(zp * 4 + x, y * 2 + (1 - c)), (zm * 4 + x, y * 2 + (1 - c))]
    barrier = pltpu.get_barrier_semaphore()
    for peer in peers:
        pl.semaphore_signal(barrier, inc=1, device_id=peer, device_id_type=MESH)
    pl.semaphore_wait(barrier, len(peers))

    def arrived(dst, name):
        pltpu.make_async_remote_copy(
            src_ref=dst, dst_ref=dst, send_sem=sent.at[0], recv_sem=recv.at[SLOTS[name]],
            device_id=other, device_id_type=MESH,
        ).wait_recv()

    def d_cols(v):
        return pl.ds(pl.multiple_of(v * DB, DB), DB)

    def tile_of(v):
        return jnp.minimum(v * NJ, TILES - NJ)

    def units(v, j):
        return pl.ds(pl.multiple_of((tile_of(v) + j) * UT, UT), UT)

    def gu_half(l, j, cc, owner, what):
        return wgu.at[l, 2 * j + cc, d_cols(owner), pl.ds(what * UT, UT)]

    def relay_ref(l, j, h):
        return rel.at[l, j, h] if j < NJ else rel_d.at[l, h]

    def w_half(l, j, cc, owner, h):
        if j < NJ:
            return gu_half(l, j, cc, owner, h)
        return wd.at[l, :, cc, pl.ds(h * 64, 64), d_cols(owner)]

    def w_whole(l, j, cc, owner):
        return wgu.at[l, 2 * j + cc, d_cols(owner), :] if j < NJ else wd.at[l, :, cc, :, d_cols(owner)]

    def program(core):
        waits = []
        local_waits = {}

        def send(src, dst, name, dev):
            pltpu.make_async_remote_copy(
                src_ref=src, dst_ref=dst, send_sem=sent.at[len(waits) % N_SENT], recv_sem=recv.at[SLOTS[name]],
                device_id=dev, device_id_type=MESH,
            ).start()

        def all_sent(like):
            waits.append(
                pltpu.make_async_remote_copy(
                    src_ref=like, dst_ref=like, send_sem=sent.at[len(waits) % N_SENT], recv_sem=recv.at[0],
                    device_id=other, device_id_type=MESH,
                ).wait_send
            )

        done = []

        def wait_sent(keep):
            while len(waits) - len(done) > keep:
                waits[len(done)]()
                done.append(True)

        def stage_w(l, j):
            up, opposite, back, me = unit_at[l]
            if j < NJ:
                sources = (wg_hbm, wu_hbm)
                send(wg_hbm.at[l, :, units(opposite, j)], rel.at[l, j, 0], ("wr", l, j), at_unit(l, up))
                send(wu_hbm.at[l, :, units(opposite, j)], rel.at[l, j, 1], ("wr", l, j), at_unit(l, back))
                for what, src in enumerate(sources):
                    for to in (up, back):
                        send(
                            src.at[l, :, units(to, j)], gu_half(l, j, core, me, what), ("w", l, j), at_unit_main(l, to)
                        )
                if core == 0:
                    for what, src in enumerate(sources):
                        send(src.at[l, :, units(me, j)], gu_half(l, j, core, me, what), ("w", l, j), other)
                else:
                    mine = []
                    for what, src in enumerate(sources):
                        copy = pltpu.make_async_copy(
                            src.at[l, :, units(me, j)], gu_half(l, j, core, me, what), local.at[l * 7 + j * 2 + what]
                        )
                        copy.start()
                        mine.append(copy.wait)
                    local_waits[l, j] = mine
                all_sent(wgu.at[l, 0:4 - core, 0:DB, :])
            else:
                def src(v, h=None):
                    if h is None:
                        return wd_hbm.at[l, pl.ds(tile_of(v), NJ)]
                    return wd_hbm.at[l, pl.ds(tile_of(v), NJ), pl.ds(h * 64, 64)]

                send(src(opposite, 0), rel_d.at[l, 0], ("wr", l, j), at_unit(l, up))
                send(src(opposite, 1), rel_d.at[l, 1], ("wr", l, j), at_unit(l, back))
                send(src(up), w_whole(l, j, core, me), ("w", l, j), at_unit_main(l, up))
                send(src(back), w_whole(l, j, core, me), ("w", l, j), at_unit_main(l, back))
                if core == 0:
                    send(src(me), w_whole(l, j, core, me), ("w", l, j), other)
                else:
                    copy = pltpu.make_async_copy(src(me), w_whole(l, j, core, me), local.at[l * 7 + 6])
                    copy.start()
                    local_waits[l, j] = [copy.wait]
                all_sent(wgu.at[l, 0:4 - core, 0:NJ * UT, :])

        def stage_v(l, j):
            up, _, back, _ = unit_at[l]
            arrived(rel.at[l, j] if j < NJ else rel_d.at[l], ("wr", l, j))
            for h, (to, owner) in enumerate(((up, back), (back, up))):
                send(relay_ref(l, j, h), w_half(l, j, core, owner, h), ("w", l, j), at_unit_main(l, to))
            all_sent(wgu.at[l, 0, 0:DB if j < NJ else NJ * UT, :])

        if core == 0:
            for i, (stage, *key) in enumerate([t for t in order() if t[0] in "WV"]):
                if stage == "W":
                    if i:
                        pl.semaphore_wait(go, 1)
                    stage_w(*key)
                else:
                    stage_v(*key)
            arrived(ov, ("dd",))
            copy = pltpu.make_async_copy(ov, out_hbm, local.at[0])
            copy.start()
            wait_sent(0)
            copy.wait()
            return

        def weights_ready(l, j):
            for wait in local_waits[l, j]:
                wait()
            arrived(wgu.at[l, 0:2, 0:7 * DB // 2, :] if j < NJ else wgu.at[l, 0:3, 0:7 * UT, :], ("w", l, j))

        def gathered(p, k, at, rows):
            if p < LAYERS:
                return xs.at[p, k, pl.ds(pl.multiple_of(at, rows), rows), :]
            return ov.at[pl.ds(pl.multiple_of(k * TC + at, rows), rows), :]

        def part_rows(v):
            return y * YB + v * R

        in_copies = {}
        y_block = pl.ds(pl.multiple_of(y * YB, YB), YB)

        def stage_x(l, k):
            rows = pl.ds(pl.multiple_of(k * TC + y * YB, YB), YB)
            dst = xs.at[0, k, y_block, d_cols(x)]
            for d in (2, 1, 3):
                send(x_hbm.at[rows, :], dst, ("xg", k), at_x(turn(x, d)))
            all_sent(ov.at[0:3 * YB, :])
            in_copies[k] = pltpu.make_async_copy(x_hbm.at[rows, :], dst, local.at[14 + k])
            in_copies[k].start()

        gain_copies = []

        def gains_send():
            for i, (src, axis) in enumerate(((gain_hbm, 0), (shift_hbm, 0), (gain_hbm, 1), (shift_hbm, 1))):
                me = unit_at[axis][3]
                for d in (1, 3, 2):
                    send(src, gains.at[i, me], ("gain",), at_unit(axis, turn(me, d)))
                all_sent(gains.at[i, 0:3])
                copy = pltpu.make_async_copy(src, gains.at[i, me], local.at[14 + NC + i])
                copy.start()
                gain_copies.append(copy)

        seen = set()

        def stage_a(l, k, g):
            first, last = GROUPS[l, k][g]
            if g == 0:
                arrived(xs.at[l, k, 0:YB, :], ("y1", k))
                arrived(xs.at[l, k, 0:YB, :], ("y2", k))
            for j in range(first, last):
                if (l, j) not in seen:
                    weights_ready(l, j)
                    seen.add((l, j))

            def tiles(j, carry):
                for n in (0, 1):
                    value = jnp.dot(xs[l, k], wgu[l, 2 * j + n], preferred_element_type=F32).astype(BF)
                    for o in range(4):
                        for h in (0, 1):
                            at = o * ZB + h * ZH
                            part[l, k, j, o, h, :, n * 256:(n + 1) * 256] = value[at:at + ZH]
                return carry

            lax.fori_loop(first, last, tiles, 0)
            js = pl.ds(first, last - first)
            up, opposite, back, _ = sums[l]
            send(part.at[l, k, js, opposite, 0], ra.at[l, k, js, 0], ("za", k, g), at_sum(l, up))
            send(part.at[l, k, js, opposite, 1], ra.at[l, k, js, 1], ("za", k, g), at_sum(l, back))
            send(part.at[l, k, js, up, 1], rb.at[l, k, js, 0], ("zc", k, g), at_sum(l, up))
            send(part.at[l, k, js, back, 0], rb.at[l, k, js, 1], ("zc", k, g), at_sum(l, back))
            all_sent(part.at[l, k, js, 0:2])

        def stage_b(l, k, g):
            first, last = GROUPS[l, k][g]
            js = pl.ds(first, last - first)
            up, _, back, _ = sums[l]
            arrived(ra.at[l, k, js], ("za", k, g))
            for h, to in enumerate((up, back)):
                for j in range(first, last):
                    part[l, k, j, to, h] = (part[l, k, j, to, h].astype(F32) + ra[l, k, j, h].astype(F32)).astype(BF)
                send(part.at[l, k, js, to, h], rc.at[l, k, js, h], ("zc", k, g), at_sum(l, to))
            all_sent(part.at[l, k, js, 0])

        def hid_ref(l, k, g, o, h):
            first, last = GROUPS[l, k][g]
            rows = pl.ds(pl.multiple_of(o * ZB + h * ZH, ZH), ZH)
            return hid.at[l, k, pl.ds(2 * first, 2 * (last - first)), rows, :]

        def stage_c(l, k, g):
            first, last = GROUPS[l, k][g]
            js = pl.ds(first, last - first)
            up, _, back, me = sums[l]
            arrived(part.at[l, k, js, 0:2], ("zc", k, g))
            for h in (0, 1):
                for j in range(first, last):
                    total = (
                        part[l, k, j, me, h].astype(F32) + rc[l, k, j, h].astype(F32) + rb[l, k, j, 1 - h].astype(F32)
                    )
                    for n in (0, 1):
                        gate, lift = total[:, n * 256:n * 256 + UT], total[:, n * 256 + UT:(n + 1) * 256]
                        value = gate * jax.nn.sigmoid(gate) * lift
                        if j < SHARED:
                            value = jnp.where(unit_at[l][3] == 3, jnp.zeros_like(value), value)
                        hid[l, k, 2 * j + n, pl.ds(pl.multiple_of(me * ZB + h * ZH, ZH), ZH), :] = value.astype(BF)
                if h == 0:
                    ref = hid_ref(l, k, g, me, 0)
                    send(ref, ref, ("h0", k, g), at_sum(l, up))
            ref = hid_ref(l, k, g, me, 1)
            send(ref, ref, ("h0", k, g), at_sum(l, back))
            send(ref, ref, ("h1", k), at_sum(l, up))
            ref = hid_ref(l, k, g, me, 0)
            send(ref, ref, ("h1", k), at_sum(l, back))
            all_sent(hid.at[l, k, pl.ds(2 * first, 2 * (last - first)), 0:4 * ZH, :])

        def stage_d(l, k, g):
            first, last = GROUPS[l, k][g]
            up, _, back, _ = sums[l]
            arrived(hid.at[l, k, pl.ds(2 * first, 2 * (last - first)), 0:2 * ZH, :], ("h0", k, g))
            for h, (owner, to) in enumerate(((back, up), (up, back))):
                ref = hid_ref(l, k, g, owner, h)
                send(ref, ref, ("h1", k), at_sum(l, to))
            all_sent(hid.at[l, k, pl.ds(2 * first, 2 * (last - first)), 0:2 * ZH, :])

        def stage_e(l, k):
            arrived(hid.at[l, k, :, 0:4 * ZH, :], ("h1", k))
            if (l, NJ) not in seen:
                weights_ready(l, NJ)
                seen.add((l, NJ))

            def columns(n, carry):
                lhs = jnp.concatenate([hid[l, k, t] for t in range(NT)], axis=1)
                for i in (0, 1):
                    cols = pl.ds(pl.multiple_of(n * 512 + i * 256, 256), 256)
                    rhs = wd[l, :, :, :, cols].reshape(NT * UT, 256)
                    value = jnp.dot(lhs, rhs, preferred_element_type=F32).astype(BF)
                    for yy in range(4):
                        for h in (0, 1):
                            at = yy * YB + h * YH
                            down[l, k, yy, h, :, cols] = value[at:at + YH]
                return carry

            lax.fori_loop(0, DQ // 512, columns, 0)
            send(down.at[l, k, yo, 0], ya.at[l, k, 0], ("ya", k), at_y(yp))
            send(down.at[l, k, yo, 1], ya.at[l, k, 1], ("ya", k), at_y(ym))
            send(down.at[l, k, yp, 1], yb.at[l, k, 0], ("yc", k), at_y(yp))
            send(down.at[l, k, ym, 0], yb.at[l, k, 1], ("yc", k), at_y(ym))
            all_sent(down.at[l, k, 0:2])

        def stage_g(l, k):
            arrived(ya.at[l, k], ("ya", k))
            for h, to in enumerate((yp, ym)):
                down[l, k, to, h] = (down[l, k, to, h].astype(F32) + ya[l, k, h].astype(F32)).astype(BF)
                send(down.at[l, k, to, h], yc.at[l, k, h], ("yc", k), at_y(to))
            all_sent(down.at[l, k, 0])

        def stage_h(l, k):
            arrived(down.at[l, k, 0:2], ("yc", k))
            for h in (0, 1):
                total = down[l, k, y, h].astype(F32) + yc[l, k, h].astype(F32) + yb[l, k, 1 - h].astype(F32)
                ys[l, k, 2 * h] = total[:R].astype(BF)
                ys[l, k, 2 * h + 1] = total[R:].astype(BF)
            me = unit_at[l][3]
            for d in (2, 1, 3):
                send(ys.at[l, k, turn(me, d)], xr.at[l, k, d - 1], ("xr", k), at_unit(l, turn(me, d)))
            all_sent(ys.at[l, k, 0:3])

        def stage_i(l, k):
            me = unit_at[l][3]
            rows = pl.ds(pl.multiple_of(part_rows(me), R), R)
            value = RESIDUAL * xs[l, k, rows, :].astype(F32) + ys[l, k, me].astype(F32)
            arrived(xr.at[l, k], ("xr", k))
            for d in (1, 3, 2):
                value = value + xr[l, k, d - 1].astype(F32)
            mixed[l, k] = value
            row_sum = jnp.sum(value, axis=1, keepdims=True)
            row_squares = jnp.sum(value * value, axis=1, keepdims=True)
            lane = lax.broadcasted_iota(jnp.int32, (R, 128), 1)
            st[l, k] = jnp.where(lane == 0, row_sum, jnp.where(lane == 1, row_squares, 0.0))
            for d in (2, 1, 3):
                send(st.at[l, k], st_in.at[l, k, d - 1], ("st", k), at_sum(l, turn(sums[l][3], d)))
            all_sent(st_in.at[l, k])

        def stage_j(l, k):
            me = unit_at[l][3]
            if ("gain",) not in seen:
                seen.add(("gain",))
                arrived(gains.at[0:3], ("gain",))
                for copy in gain_copies:
                    copy.wait()
            stats = st[l, k]
            arrived(st_in.at[l, k], ("st", k))
            for d in (1, 3, 2):
                stats = stats + st_in[l, k, d - 1]
            mean = stats[:, 0:1] / D
            var = stats[:, 1:2] / D - mean * mean
            scale = lax.rsqrt(var + EPSILON)
            for q in range(4):
                cols = slice(q * DB, (q + 1) * DB)
                normed = (mixed[l, k, :, cols] - mean) * scale
                nb[l, k, q] = (normed * gains[2 * l, q, l:l + 1, :] + gains[2 * l + 1, q, l:l + 1, :]).astype(BF)

            if l + 1 < LAYERS:
                dst = xs.at[1, k, pl.ds(pl.multiple_of(part_rows(me), R), R), d_cols(z)]
            else:
                dst = gathered(LAYERS, k, part_rows(me), R)
            dst[...] = nb[l, k, me]
            for d in (2, 1, 3):
                name = ("xq", k) if l + 1 < LAYERS else ("xg", k)
                send(nb.at[l, k, turn(me, d)], dst, name, at_unit(l, turn(me, d)))
            all_sent(nb.at[l, k, 0:3])

        def stage_q(l, k):
            arrived(nb.at[0, k, 0:3], ("xq", k))
            ref = xs.at[1, k, y_block, d_cols(z)]
            for d in (2, 1, 3):
                send(ref, ref, ("xg", k), at_z(turn(z, d)))
            all_sent(ov.at[0:3 * YB, :])

        def stage_k(l, k):
            p = l + 1
            arrived(ov.at[0:3 * YB, :] if p < LAYERS else nb.at[1, k, 0:3], ("xg", k))
            if p == 0:
                in_copies[k].wait()
            for h in (0, 1):
                ref = gathered(p, k, y * YB + h * YH, YH)
                send(ref, ref, (("y0", "y1")[h], k), at_y(yp))
                ref = gathered(p, k, y * YB + (1 - h) * YH, YH)
                send(ref, ref, (("y0", "y1")[h], k), at_y(ym))
            if p == LAYERS:
                ref = gathered(p, k, y * YB, YB)
                send(ref, ref, ("dd",), other)
                all_sent(ov.at[0:6 * YH, :])
            else:
                all_sent(xs.at[p, k, 0:4 * YH, :])

        def stage_l(l, k):
            p = l + 1
            halves = (lambda n: xs.at[p, k, 0:n * YH, :]) if p < LAYERS else (lambda n: ov.at[0:n * YH, :])
            arrived(halves(2), ("y0", k))
            for h, (owner, to) in enumerate(((ym, yp), (yp, ym))):
                ref = gathered(p, k, owner * YB + h * YH, YH)
                send(ref, ref, ("y2", k), at_y(to))
            if p == LAYERS:
                arrived(halves(2), ("y1", k))
                for owner in (ym, yp):
                    ref = gathered(p, k, owner * YB, YB)
                    send(ref, ref, ("dd",), other)
                all_sent(ov.at[0:6 * YH, :])
            else:
                all_sent(xs.at[p, k, 0:2 * YH, :])

        def stage_m(l, k):
            p = l + 1
            arrived(ov.at[0:YB, :], ("y2", k))
            ref = gathered(p, k, yo * YB, YB)
            send(ref, ref, ("dd",), other)
            all_sent(ov.at[0:YB, :])

        def stage_w_both(l, j):
            if l + j == 0:
                stage_w(l, j)
                gains_send()
                return
            pl.semaphore_signal(go, inc=1, device_id=other, device_id_type=MESH)
            stage_w(l, j)

        stages = dict(
            A=stage_a, B=stage_b, C=stage_c, D=stage_d, E=stage_e, G=stage_g, H=stage_h, I=stage_i, J=stage_j,
            K=stage_k, L=stage_l, M=stage_m, Q=stage_q, W=stage_w_both, V=stage_v, X=stage_x,
        )
        for stage, *key in order():
            stages[stage](*key)
            wait_sent(WAIT_LATER)
        copy = pltpu.make_async_copy(ov, out_hbm, local.at[18 + NC])
        copy.start()
        wait_sent(0)
        copy.wait()

    @pl.when(c == 0)
    def _():
        program(0)

    @pl.when(c == 1)
    def _():
        program(1)


def solution(mesh):
    dma = pltpu.SemaphoreType.DMA

    def per_device(inputs, gate_weight, up_weight, down_weight, norm_gain, norm_shift):
        any_space = pl.BlockSpec(memory_space=pl.ANY)
        return pl.pallas_call(
            kernel,
            out_shape=jax.ShapeDtypeStruct((T, DB), BF),
            in_specs=[any_space] * 6,
            out_specs=any_space,
            scratch_shapes=[
                pltpu.VMEM((2, NC, TC, DQ), BF),
                pltpu.VMEM((2, NT, DQ, 2 * UT), BF),
                pltpu.VMEM((2, NJ, 2, UT, DQ), BF),
                pltpu.VMEM((2, NJ, 2, DB, UT), BF),
                pltpu.VMEM((2, 2, NJ, UT // 2, DB), BF),
                pltpu.VMEM((2, NC, NJ, 4, 2, ZH, 4 * UT), BF),
                pltpu.VMEM((2, NC, NJ, 2, ZH, 4 * UT), BF),
                pltpu.VMEM((2, NC, NJ, 2, ZH, 4 * UT), BF),
                pltpu.VMEM((2, NC, NJ, 2, ZH, 4 * UT), BF),
                pltpu.VMEM((2, NC, NT, TC, UT), BF),
                pltpu.VMEM((2, NC, 4, 2, YH, DQ), BF),
                pltpu.VMEM((2, NC, 2, YH, DQ), BF),
                pltpu.VMEM((2, NC, 2, YH, DQ), BF),
                pltpu.VMEM((2, NC, 2, YH, DQ), BF),
                pltpu.VMEM((2, NC, 4, R, DQ), BF),
                pltpu.VMEM((2, NC, 3, R, DQ), BF),
                pltpu.VMEM((2, NC, R, DQ), F32),
                pltpu.VMEM((2, NC, R, 128), F32),
                pltpu.VMEM((2, NC, 3, R, 128), F32),
                pltpu.VMEM((2, NC, 4, R, DB), BF),
                pltpu.VMEM((T, DB), BF),
                pltpu.VMEM((4, 4, 2, DB), F32),
                dma((N_SLOTS,)),
                dma((N_SENT,)),
                dma((19 + NC,)),
                pltpu.SemaphoreType.REGULAR,
            ],
            compiler_params=pltpu.CompilerParams(
                collective_id=0, has_side_effects=True, vmem_limit_bytes=63 * 1024 * 1024
            ),
        )(inputs, gate_weight, up_weight, down_weight.reshape(LAYERS, TILES, UT, DB), norm_gain, norm_shift)

    return jax.shard_map(
        per_device,
        mesh=mesh,
        in_specs=(P(None, "ra"), P(None, "ra", "cb"), P(None, "ra", "cb"), P(None, "cb", "ra"), P(None, "ra"), P(None, "ra")),
        out_specs=P(None, "ra"),
        check_vma=False,
    )
```

```python
import jax
import jax.numpy as jnp
from jax import lax
from jax.experimental import pallas as pl
from jax.experimental.pallas import tpu as pltpu
from jax.sharding import PartitionSpec as P

MESH = pl.DeviceIdType.MESH
BF = jnp.bfloat16
F32 = jnp.float32
RESIDUAL = 0.5
EPSILON = 1e-05

T, D, FF, LAYERS = 1536, 4096, 11264, 2
NC = 6
TC = T // NC
ZB = TC // 4
ZH = ZB // 2
YB = TC // 4
YH = YB // 2
R = TC // 16
DB = D // 16
DQ = D // 4
UT = 128
NJ = 3
NT = 2 * NJ
TILES = FF // 8 // UT
SHARED = 4 * NJ - TILES

GROUPS = {(l, k): [(0, 1), (1, 2), (2, 3)] if l == 0 else [(0, 1), (1, 3)] for l in range(LAYERS) for k in range(NC)}

SLOTS = {}


def slots(*names):
    for name in names:
        SLOTS.setdefault(name, len(SLOTS))


for k in range(NC):
    for g in range(max(len(GROUPS[l, k]) for l in range(LAYERS))):
        slots(("za", k, g), ("zc", k, g), ("h0", k, g))
    slots(*((m, k) for m in ("h1", "ya", "yc", "xr", "st", "xq", "xg", "y0", "y1", "y2")))
for l in range(LAYERS):
    for j in range(NJ + 1):
        slots(("wr", l, j), ("w", l, j))
slots(("gain",), *(("dd", k) for k in range(NC)))
N_SLOTS = len(SLOTS)
N_SENT = 40
WAIT_LATER = 30

SUM_AXIS, UNIT_AXIS = "zx", "xz"
ORDER = [
    ("X", 0, 0), ("W", 0, 0), ("W", 1, 0), ("W", 1, 1), ("S", 0, 0), ("X", 0, 2), ("X", 0, 3), ("X", 0, 4),
    ("W", 1, 2), ("X", 0, 1), ("V", 0, 0), ("X", 0, 5), ("K", -1, 0), ("S", 0, 2), ("S", 0, 3), ("W", 0, 1),
    ("L", -1, 0), ("K", -1, 2), ("S", 0, 4), ("K", -1, 3), ("A", 0, 0, 0), ("V", 1, 0), ("L", -1, 2), ("V", 0, 1),
    ("W", 0, 2), ("L", -1, 3), ("K", -1, 4), ("B", 0, 0, 0), ("S", 0, 1), ("A", 0, 2, 0), ("A", 0, 2, 1),
    ("A", 0, 0, 1), ("L", -1, 4), ("C", 0, 0, 0), ("A", 0, 3, 0), ("A", 0, 3, 1), ("V", 0, 2), ("B", 0, 2, 0),
    ("B", 0, 0, 1), ("B", 0, 2, 1), ("A", 0, 4, 1), ("S", 0, 5), ("W", 0, 3), ("D", 0, 0, 0), ("K", -1, 1),
    ("A", 0, 4, 0), ("A", 0, 0, 2), ("A", 0, 2, 2), ("C", 0, 2, 1), ("C", 0, 0, 1), ("B", 0, 0, 2), ("B", 0, 3, 0),
    ("L", -1, 1), ("B", 0, 2, 2), ("C", 0, 2, 0), ("A", 0, 3, 2), ("V", 0, 3), ("D", 0, 2, 1), ("C", 0, 0, 2),
    ("K", -1, 5), ("D", 0, 0, 1), ("B", 0, 3, 1), ("C", 0, 2, 2), ("A", 0, 4, 2), ("D", 0, 2, 0), ("D", 0, 0, 2),
    ("B", 0, 3, 2), ("A", 0, 1, 0), ("L", -1, 5), ("D", 0, 2, 2), ("C", 0, 3, 1), ("C", 0, 3, 0), ("A", 0, 1, 2),
    ("B", 0, 4, 2), ("B", 0, 4, 0), ("E", 0, 0), ("C", 0, 3, 2), ("B", 0, 1, 0), ("E", 0, 2), ("D", 0, 3, 0),
    ("B", 0, 4, 1), ("B", 0, 1, 2), ("D", 0, 3, 1), ("A", 0, 1, 1), ("G", 0, 0), ("C", 0, 4, 2), ("D", 0, 3, 2),
    ("A", 0, 5, 2), ("C", 0, 4, 0), ("G", 0, 2), ("A", 0, 5, 0), ("C", 0, 4, 1), ("B", 0, 1, 1), ("C", 0, 1, 2),
    ("C", 0, 1, 0), ("H", 0, 0), ("A", 0, 5, 1), ("E", 0, 3), ("B", 0, 5, 0), ("H", 0, 2), ("D", 0, 4, 1),
    ("D", 0, 4, 0), ("C", 0, 1, 1), ("D", 0, 4, 2), ("B", 0, 5, 2), ("I", 0, 0), ("B", 0, 5, 1), ("D", 0, 1, 0),
    ("D", 0, 1, 2), ("G", 0, 3), ("D", 0, 1, 1), ("C", 0, 5, 0), ("E", 0, 4), ("C", 0, 5, 2), ("C", 0, 5, 1),
    ("I", 0, 2), ("J", 0, 0), ("E", 0, 1), ("H", 0, 3), ("D", 0, 5, 0), ("D", 0, 5, 2), ("D", 0, 5, 1), ("G", 0, 4),
    ("Q", 0, 0), ("J", 0, 2), ("G", 0, 1), ("E", 0, 5), ("I", 0, 3), ("H", 0, 4), ("Q", 0, 2), ("K", 0, 0),
    ("H", 0, 1), ("V", 1, 2), ("G", 0, 5), ("J", 0, 3), ("I", 0, 4), ("V", 1, 1), ("L", 0, 0), ("K", 0, 2),
    ("I", 0, 1), ("H", 0, 5), ("Q", 0, 3), ("J", 0, 4), ("A", 1, 0, 0), ("L", 0, 2), ("A", 1, 0, 1), ("K", 0, 3),
    ("I", 0, 5), ("J", 0, 1), ("B", 1, 0, 0), ("Q", 0, 4), ("A", 1, 2, 0), ("B", 1, 0, 1), ("A", 1, 2, 1),
    ("L", 0, 3), ("J", 0, 5), ("Q", 0, 1), ("C", 1, 0, 0), ("B", 1, 2, 0), ("K", 0, 4), ("C", 1, 0, 1),
    ("B", 1, 2, 1), ("A", 1, 3, 1), ("Q", 0, 5), ("W", 1, 3), ("D", 1, 0, 1), ("L", 0, 4), ("K", 0, 1),
    ("A", 1, 3, 0), ("C", 1, 2, 1), ("B", 1, 3, 1), ("C", 1, 2, 0), ("A", 1, 4, 0), ("B", 1, 3, 0), ("K", 0, 5),
    ("A", 1, 4, 1), ("L", 0, 1), ("B", 1, 4, 0), ("D", 1, 2, 0), ("C", 1, 3, 1), ("D", 1, 2, 1), ("V", 1, 3),
    ("C", 1, 3, 0), ("L", 0, 5), ("D", 1, 0, 0), ("B", 1, 4, 1), ("A", 1, 1, 0), ("C", 1, 4, 0), ("A", 1, 1, 1),
    ("A", 1, 5, 0), ("D", 1, 3, 1), ("D", 1, 3, 0), ("A", 1, 5, 1), ("C", 1, 4, 1), ("B", 1, 1, 0), ("E", 1, 2),
    ("E", 1, 0), ("B", 1, 1, 1), ("E", 1, 3), ("D", 1, 4, 0), ("B", 1, 5, 1), ("D", 1, 4, 1), ("G", 1, 2),
    ("C", 1, 1, 0), ("G", 1, 0), ("B", 1, 5, 0), ("C", 1, 1, 1), ("G", 1, 3), ("C", 1, 5, 1), ("E", 1, 4),
    ("C", 1, 5, 0), ("D", 1, 1, 0), ("H", 1, 2), ("D", 1, 1, 1), ("H", 1, 3), ("H", 1, 0), ("D", 1, 5, 1),
    ("D", 1, 5, 0), ("G", 1, 4), ("E", 1, 1), ("I", 1, 2), ("E", 1, 5), ("I", 1, 3), ("H", 1, 4), ("I", 1, 0),
    ("G", 1, 1), ("J", 1, 2), ("G", 1, 5), ("J", 1, 3), ("J", 1, 0), ("H", 1, 1), ("I", 1, 4), ("K", 1, 2),
    ("H", 1, 5), ("K", 1, 3), ("J", 1, 4), ("I", 1, 1), ("L", 1, 2), ("K", 1, 0), ("L", 1, 3), ("I", 1, 5),
    ("L", 1, 0), ("M", 1, 3), ("M", 1, 2), ("J", 1, 1), ("K", 1, 4), ("J", 1, 5), ("M", 1, 0), ("L", 1, 4),
    ("K", 1, 1), ("K", 1, 5), ("L", 1, 1), ("M", 1, 4), ("L", 1, 5), ("M", 1, 1), ("M", 1, 5),
]


def kernel(
    x_hbm, wg_hbm, wu_hbm, wd_hbm, gain_hbm, shift_hbm, out_hbm,
    xs, wgu, wd, rel, rel_d, part, ra, rb, rc, hid, down, ya, yb, yc, ys, xr, mixed, st, st_in, nb, ov, gains,
    recv, sent, local, go,
):
    ra_at, cb_at = lax.axis_index("ra"), lax.axis_index("cb")
    z, x = ra_at // 4, lax.rem(ra_at, 4)
    y, c = cb_at // 2, lax.rem(cb_at, 2)

    def turn(v, d):
        return lax.rem(v + d, 4)

    zp, zo, zm = turn(z, 1), turn(z, 2), turn(z, 3)
    yp, yo, ym = turn(y, 1), turn(y, 2), turn(y, 3)
    xp, xo, xm = turn(x, 1), turn(x, 2), turn(x, 3)

    def at_z(v):
        return (v * 4 + x, cb_at)

    def at_x(v):
        return (z * 4 + v, cb_at)

    def at_sum(l, v):
        return at_z(v) if SUM_AXIS[l] == "z" else at_x(v)

    def at_unit(l, v):
        return at_x(v) if UNIT_AXIS[l] == "x" else at_z(v)

    def at_unit_main(l, v):
        return (z * 4 + v, y * 2 + 1) if UNIT_AXIS[l] == "x" else (v * 4 + x, y * 2 + 1)

    sums = [(zp, zo, zm, z), (xp, xo, xm, x)]
    unit_at = [(xp, xo, xm, x), (zp, zo, zm, z)]

    def at_y(v):
        return (ra_at, v * 2 + c)

    other = (ra_at, y * 2 + (1 - c))

    peers = [at_z(zp), at_z(zo), at_z(zm), at_x(xp), at_x(xo), at_x(xm), at_y(yp), at_y(ym), other]
    peers += [(z * 4 + xp, y * 2 + (1 - c)), (z * 4 + xm, y * 2 + (1 - c))]
    peers += [(zp * 4 + x, y * 2 + (1 - c)), (zm * 4 + x, y * 2 + (1 - c))]
    barrier = pltpu.get_barrier_semaphore()
    for peer in peers:
        pl.semaphore_signal(barrier, inc=1, device_id=peer, device_id_type=MESH)
    pl.semaphore_wait(barrier, len(peers))

    def arrived(dst, name):
        pltpu.make_async_remote_copy(
            src_ref=dst, dst_ref=dst, send_sem=sent.at[0], recv_sem=recv.at[SLOTS[name]],
            device_id=other, device_id_type=MESH,
        ).wait_recv()

    def d_cols(v):
        return pl.ds(pl.multiple_of(v * DB, DB), DB)

    def tile_of(v):
        return jnp.minimum(v * NJ, TILES - NJ)

    def units(v, j):
        return pl.ds(pl.multiple_of((tile_of(v) + j) * UT, UT), UT)

    def gu_half(l, j, cc, owner, what):
        return wgu.at[l, 2 * j + cc, d_cols(owner), pl.ds(what * UT, UT)]

    def relay_ref(l, j, h):
        return rel.at[l, j, h] if j < NJ else rel_d.at[l, h]

    def w_half(l, j, cc, owner, h):
        if j < NJ:
            return gu_half(l, j, cc, owner, h)
        return wd.at[l, :, cc, pl.ds(h * 64, 64), d_cols(owner)]

    def w_whole(l, j, cc, owner):
        return wgu.at[l, 2 * j + cc, d_cols(owner), :] if j < NJ else wd.at[l, :, cc, :, d_cols(owner)]

    def program(core):
        waits = []
        local_waits = {}

        def send(src, dst, name, dev):
            pltpu.make_async_remote_copy(
                src_ref=src, dst_ref=dst, send_sem=sent.at[len(waits) % N_SENT], recv_sem=recv.at[SLOTS[name]],
                device_id=dev, device_id_type=MESH,
            ).start()

        def all_sent(like):
            waits.append(
                pltpu.make_async_remote_copy(
                    src_ref=like, dst_ref=like, send_sem=sent.at[len(waits) % N_SENT], recv_sem=recv.at[0],
                    device_id=other, device_id_type=MESH,
                ).wait_send
            )

        done = []

        def wait_sent(keep):
            while len(waits) - len(done) > keep:
                waits[len(done)]()
                done.append(True)

        def stage_w(l, j):
            up, opposite, back, me = unit_at[l]
            if j < NJ:
                sources = (wg_hbm, wu_hbm)
                send(wg_hbm.at[l, :, units(opposite, j)], rel.at[l, j, 0], ("wr", l, j), at_unit(l, up))
                send(wu_hbm.at[l, :, units(opposite, j)], rel.at[l, j, 1], ("wr", l, j), at_unit(l, back))
                for what, src in enumerate(sources):
                    for to in (up, back):
                        send(
                            src.at[l, :, units(to, j)], gu_half(l, j, core, me, what), ("w", l, j), at_unit_main(l, to)
                        )
                if core == 0:
                    for what, src in enumerate(sources):
                        send(src.at[l, :, units(me, j)], gu_half(l, j, core, me, what), ("w", l, j), other)
                else:
                    mine = []
                    for what, src in enumerate(sources):
                        copy = pltpu.make_async_copy(
                            src.at[l, :, units(me, j)], gu_half(l, j, core, me, what), local.at[l * 7 + j * 2 + what]
                        )
                        copy.start()
                        mine.append(copy.wait)
                    local_waits[l, j] = mine
                all_sent(wgu.at[l, 0:4 - core, 0:DB, :])
            else:
                def src(v, h=None):
                    if h is None:
                        return wd_hbm.at[l, pl.ds(tile_of(v), NJ)]
                    return wd_hbm.at[l, pl.ds(tile_of(v), NJ), pl.ds(h * 64, 64)]

                send(src(opposite, 0), rel_d.at[l, 0], ("wr", l, j), at_unit(l, up))
                send(src(opposite, 1), rel_d.at[l, 1], ("wr", l, j), at_unit(l, back))
                send(src(up), w_whole(l, j, core, me), ("w", l, j), at_unit_main(l, up))
                send(src(back), w_whole(l, j, core, me), ("w", l, j), at_unit_main(l, back))
                if core == 0:
                    send(src(me), w_whole(l, j, core, me), ("w", l, j), other)
                else:
                    copy = pltpu.make_async_copy(src(me), w_whole(l, j, core, me), local.at[l * 7 + 6])
                    copy.start()
                    local_waits[l, j] = [copy.wait]
                all_sent(wgu.at[l, 0:4 - core, 0:NJ * UT, :])

        def stage_v(l, j):
            up, _, back, _ = unit_at[l]
            arrived(rel.at[l, j] if j < NJ else rel_d.at[l], ("wr", l, j))
            for h, (to, owner) in enumerate(((up, back), (back, up))):
                send(relay_ref(l, j, h), w_half(l, j, core, owner, h), ("w", l, j), at_unit_main(l, to))
            all_sent(wgu.at[l, 0, 0:DB if j < NJ else NJ * UT, :])

        if core == 0:
            for i, (stage, *key) in enumerate([t for t in ORDER if t[0] in "WV"]):
                if stage == "W":
                    if i:
                        pl.semaphore_wait(go, 1)
                    stage_w(*key)
                else:
                    stage_v(*key)
            copies = []
            for k in range(NC):
                rows = pl.ds(k * TC, TC)
                arrived(ov.at[rows, :], ("dd", k))
                copies.append(pltpu.make_async_copy(ov.at[rows, :], out_hbm.at[rows, :], local.at[k]))
                copies[-1].start()
            wait_sent(0)
            for copy in copies:
                copy.wait()
            return

        def weights_ready(l, j):
            for wait in local_waits[l, j]:
                wait()
            arrived(wgu.at[l, 0:2, 0:7 * DB // 2, :] if j < NJ else wgu.at[l, 0:3, 0:7 * UT, :], ("w", l, j))

        def gathered(p, k, at, rows):
            if p < LAYERS:
                return xs.at[p, k, pl.ds(pl.multiple_of(at, rows), rows), :]
            return ov.at[pl.ds(pl.multiple_of(k * TC + at, rows), rows), :]

        def part_rows(v):
            return y * YB + v * R

        in_copies = {}
        out_copies = []
        y_block = pl.ds(pl.multiple_of(y * YB, YB), YB)

        def stage_x(l, k):
            def half(h):
                rows = pl.ds(pl.multiple_of(k * TC + y * YB + h * YH, YH), YH)
                return x_hbm.at[rows, :], xs.at[0, k, pl.ds(pl.multiple_of(y * YB + h * YH, YH), YH), d_cols(x)]

            for h, name in enumerate((("xq", k), ("xg", k))):
                send(*half(h), name, at_x(xp))
                send(*half(1 - h), name, at_x(xm))
            all_sent(ov.at[0:2 * YB, :])
            rows = pl.ds(pl.multiple_of(k * TC + y * YB, YB), YB)
            in_copies[k] = pltpu.make_async_copy(x_hbm.at[rows, :], xs.at[0, k, y_block, d_cols(x)], local.at[14 + k])
            in_copies[k].start()

        def stage_s(l, k):
            arrived(ov.at[0:YB, :], ("xq", k))
            for h, (owner, to) in enumerate(((xm, xp), (xp, xm))):
                ref = xs.at[0, k, pl.ds(pl.multiple_of(y * YB + h * YH, YH), YH), d_cols(owner)]
                send(ref, ref, ("xg", k), at_x(to))
            all_sent(ov.at[0:YB, :])

        gain_copies = []

        def gains_send():
            for i, (src, axis) in enumerate(((gain_hbm, 0), (shift_hbm, 0), (gain_hbm, 1), (shift_hbm, 1))):
                me = unit_at[axis][3]
                for d in (1, 3, 2):
                    send(src, gains.at[i, me], ("gain",), at_unit(axis, turn(me, d)))
                all_sent(gains.at[i, 0:3])
                copy = pltpu.make_async_copy(src, gains.at[i, me], local.at[14 + NC + i])
                copy.start()
                gain_copies.append(copy)

        seen = set()

        def stage_a(l, k, g):
            first, last = GROUPS[l, k][g]
            if ("x", l, k) not in seen:
                seen.add(("x", l, k))
                arrived(xs.at[l, k, 0:YB, :], ("y1", k))
                arrived(xs.at[l, k, 0:YB, :], ("y2", k))
            for j in range(first, last):
                if (l, j) not in seen:
                    weights_ready(l, j)
                    seen.add((l, j))

            def tiles(j, carry):
                rhs = jnp.concatenate([wgu[l, 2 * j], wgu[l, 2 * j + 1]], axis=1)
                value = jnp.dot(xs[l, k], rhs, preferred_element_type=F32).astype(BF)
                for o in range(4):
                    for h in (0, 1):
                        at = o * ZB + h * ZH
                        part[l, k, j, o, h] = value[at:at + ZH]
                return carry

            lax.fori_loop(first, last, tiles, 0)
            js = pl.ds(first, last - first)
            up, opposite, back, _ = sums[l]
            send(part.at[l, k, js, opposite, 0], ra.at[l, k, js, 0], ("za", k, g), at_sum(l, up))
            send(part.at[l, k, js, opposite, 1], ra.at[l, k, js, 1], ("za", k, g), at_sum(l, back))
            send(part.at[l, k, js, up, 1], rb.at[l, k, js, 0], ("zc", k, g), at_sum(l, up))
            send(part.at[l, k, js, back, 0], rb.at[l, k, js, 1], ("zc", k, g), at_sum(l, back))
            all_sent(part.at[l, k, js, 0:2])

        def stage_b(l, k, g):
            first, last = GROUPS[l, k][g]
            js = pl.ds(first, last - first)
            up, _, back, _ = sums[l]
            arrived(ra.at[l, k, js], ("za", k, g))
            for h, to in enumerate((up, back)):
                for j in range(first, last):
                    part[l, k, j, to, h] = (part[l, k, j, to, h].astype(F32) + ra[l, k, j, h].astype(F32)).astype(BF)
                send(part.at[l, k, js, to, h], rc.at[l, k, js, h], ("zc", k, g), at_sum(l, to))
            all_sent(part.at[l, k, js, 0])

        def hid_ref(l, k, g, o, h):
            first, last = GROUPS[l, k][g]
            rows = pl.ds(pl.multiple_of(o * ZB + h * ZH, ZH), ZH)
            return hid.at[l, k, pl.ds(2 * first, 2 * (last - first)), rows, :]

        def stage_c(l, k, g):
            first, last = GROUPS[l, k][g]
            js = pl.ds(first, last - first)
            up, _, back, me = sums[l]
            arrived(part.at[l, k, js, 0:2], ("zc", k, g))
            for h in (0, 1):
                for j in range(first, last):
                    total = (
                        part[l, k, j, me, h].astype(F32) + rc[l, k, j, h].astype(F32) + rb[l, k, j, 1 - h].astype(F32)
                    )
                    for n in (0, 1):
                        gate, lift = total[:, n * 256:n * 256 + UT], total[:, n * 256 + UT:(n + 1) * 256]
                        value = gate * jax.nn.sigmoid(gate) * lift
                        if j < SHARED:
                            value = jnp.where(unit_at[l][3] == 3, jnp.zeros_like(value), value)
                        hid[l, k, 2 * j + n, pl.ds(pl.multiple_of(me * ZB + h * ZH, ZH), ZH), :] = value.astype(BF)
                if h == 0:
                    ref = hid_ref(l, k, g, me, 0)
                    send(ref, ref, ("h0", k, g), at_sum(l, up))
            ref = hid_ref(l, k, g, me, 1)
            send(ref, ref, ("h0", k, g), at_sum(l, back))
            send(ref, ref, ("h1", k), at_sum(l, up))
            ref = hid_ref(l, k, g, me, 0)
            send(ref, ref, ("h1", k), at_sum(l, back))
            all_sent(hid.at[l, k, pl.ds(2 * first, 2 * (last - first)), 0:4 * ZH, :])

        def stage_d(l, k, g):
            first, last = GROUPS[l, k][g]
            up, _, back, _ = sums[l]
            arrived(hid.at[l, k, pl.ds(2 * first, 2 * (last - first)), 0:2 * ZH, :], ("h0", k, g))
            for h, (owner, to) in enumerate(((back, up), (up, back))):
                ref = hid_ref(l, k, g, owner, h)
                send(ref, ref, ("h1", k), at_sum(l, to))
            all_sent(hid.at[l, k, pl.ds(2 * first, 2 * (last - first)), 0:2 * ZH, :])

        def stage_e(l, k):
            arrived(hid.at[l, k, :, 0:4 * ZH, :], ("h1", k))
            if (l, NJ) not in seen:
                weights_ready(l, NJ)
                seen.add((l, NJ))

            def columns(n, carry):
                lhs = jnp.concatenate([hid[l, k, t] for t in range(NT)], axis=1)
                cols = pl.ds(pl.multiple_of(n * 512, 512), 512)
                rhs = wd[l, :, :, :, cols].reshape(NT * UT, 512)
                value = jnp.dot(lhs, rhs, preferred_element_type=F32).astype(BF)
                for yy in range(4):
                    for h in (0, 1):
                        at = yy * YB + h * YH
                        down[l, k, yy, h, :, cols] = value[at:at + YH]
                return carry

            lax.fori_loop(0, DQ // 512, columns, 0)
            send(down.at[l, k, yo, 0], ya.at[l, k, 0], ("ya", k), at_y(yp))
            send(down.at[l, k, yo, 1], ya.at[l, k, 1], ("ya", k), at_y(ym))
            send(down.at[l, k, yp, 1], yb.at[l, k, 0], ("yc", k), at_y(yp))
            send(down.at[l, k, ym, 0], yb.at[l, k, 1], ("yc", k), at_y(ym))
            all_sent(down.at[l, k, 0:2])

        def stage_g(l, k):
            arrived(ya.at[l, k], ("ya", k))
            for h, to in enumerate((yp, ym)):
                down[l, k, to, h] = (down[l, k, to, h].astype(F32) + ya[l, k, h].astype(F32)).astype(BF)
                send(down.at[l, k, to, h], yc.at[l, k, h], ("yc", k), at_y(to))
            all_sent(down.at[l, k, 0])

        def stage_h(l, k):
            arrived(down.at[l, k, 0:2], ("yc", k))
            for h in (0, 1):
                total = down[l, k, y, h].astype(F32) + yc[l, k, h].astype(F32) + yb[l, k, 1 - h].astype(F32)
                ys[l, k, 2 * h] = total[:R].astype(BF)
                ys[l, k, 2 * h + 1] = total[R:].astype(BF)
            me = unit_at[l][3]
            for d in (2, 1, 3):
                send(ys.at[l, k, turn(me, d)], xr.at[l, k, d - 1], ("xr", k), at_unit(l, turn(me, d)))
            all_sent(ys.at[l, k, 0:3])

        def stage_i(l, k):
            me = unit_at[l][3]
            rows = pl.ds(pl.multiple_of(part_rows(me), R), R)
            value = RESIDUAL * xs[l, k, rows, :].astype(F32) + ys[l, k, me].astype(F32)
            arrived(xr.at[l, k], ("xr", k))
            for d in (1, 3, 2):
                value = value + xr[l, k, d - 1].astype(F32)
            mixed[l, k] = value
            row_sum = jnp.sum(value, axis=1, keepdims=True)
            row_squares = jnp.sum(value * value, axis=1, keepdims=True)
            lane = lax.broadcasted_iota(jnp.int32, (R, 128), 1)
            st[l, k] = jnp.where(lane == 0, row_sum, jnp.where(lane == 1, row_squares, 0.0))
            for d in (2, 1, 3):
                send(st.at[l, k], st_in.at[l, k, d - 1], ("st", k), at_sum(l, turn(sums[l][3], d)))
            all_sent(st_in.at[l, k])

        def stage_j(l, k):
            me = unit_at[l][3]
            if ("gain",) not in seen:
                seen.add(("gain",))
                arrived(gains.at[0:3], ("gain",))
                for copy in gain_copies:
                    copy.wait()
            stats = st[l, k]
            arrived(st_in.at[l, k], ("st", k))
            for d in (1, 3, 2):
                stats = stats + st_in[l, k, d - 1]
            mean = stats[:, 0:1] / D
            var = stats[:, 1:2] / D - mean * mean
            scale = lax.rsqrt(var + EPSILON)
            for q in range(4):
                cols = slice(q * DB, (q + 1) * DB)
                normed = (mixed[l, k, :, cols] - mean) * scale
                nb[l, k, q] = (normed * gains[2 * l, q, l:l + 1, :] + gains[2 * l + 1, q, l:l + 1, :]).astype(BF)

            if l + 1 < LAYERS:
                dst = xs.at[1, k, pl.ds(pl.multiple_of(part_rows(me), R), R), d_cols(z)]
            else:
                dst = gathered(LAYERS, k, part_rows(me), R)
            dst[...] = nb[l, k, me]
            for d in (2, 1, 3):
                name = ("xq", k) if l + 1 < LAYERS else ("xg", k)
                send(nb.at[l, k, turn(me, d)], dst, name, at_unit(l, turn(me, d)))
            all_sent(nb.at[l, k, 0:3])

        def stage_q(l, k):
            arrived(nb.at[0, k, 0:3], ("xq", k))
            ref = xs.at[1, k, y_block, d_cols(z)]
            for d in (2, 1, 3):
                send(ref, ref, ("xg", k), at_z(turn(z, d)))
            all_sent(ov.at[0:3 * YB, :])

        def stage_k(l, k):
            p = l + 1
            got = (ov.at[0:2 * YB, :], ov.at[0:3 * YB, :], nb.at[1, k, 0:3])[p]
            arrived(got, ("xg", k))
            if p == 0:
                in_copies[k].wait()
            for h in (0, 1):
                ref = gathered(p, k, y * YB + h * YH, YH)
                send(ref, ref, (("y0", "y1")[h], k), at_y(yp))
                ref = gathered(p, k, y * YB + (1 - h) * YH, YH)
                send(ref, ref, (("y0", "y1")[h], k), at_y(ym))
            if p == LAYERS:
                ref = gathered(p, k, y * YB, YB)
                send(ref, ref, ("dd", k), other)
                all_sent(ov.at[0:6 * YH, :])
            else:
                all_sent(xs.at[p, k, 0:4 * YH, :])

        def stage_l(l, k):
            p = l + 1
            halves = (lambda n: xs.at[p, k, 0:n * YH, :]) if p < LAYERS else (lambda n: ov.at[0:n * YH, :])
            arrived(halves(2), ("y0", k))
            for h, (owner, to) in enumerate(((ym, yp), (yp, ym))):
                ref = gathered(p, k, owner * YB + h * YH, YH)
                send(ref, ref, ("y2", k), at_y(to))
            if p == LAYERS:
                arrived(halves(2), ("y1", k))
                for owner in (ym, yp):
                    ref = gathered(p, k, owner * YB, YB)
                    send(ref, ref, ("dd", k), other)
                all_sent(ov.at[0:6 * YH, :])
            else:
                all_sent(xs.at[p, k, 0:2 * YH, :])

        def stage_m(l, k):
            p = l + 1
            arrived(ov.at[0:YB, :], ("y2", k))
            ref = gathered(p, k, yo * YB, YB)
            send(ref, ref, ("dd", k), other)
            all_sent(ov.at[0:YB, :])
            rows = pl.ds(k * TC, TC)
            out_copies.append(pltpu.make_async_copy(ov.at[rows, :], out_hbm.at[rows, :], local.at[14 + k]))
            out_copies[-1].start()

        def stage_w_both(l, j):
            if l + j == 0:
                stage_w(l, j)
                gains_send()
                return
            pl.semaphore_signal(go, inc=1, device_id=other, device_id_type=MESH)
            stage_w(l, j)

        stages = dict(
            A=stage_a, B=stage_b, C=stage_c, D=stage_d, E=stage_e, G=stage_g, H=stage_h, I=stage_i, J=stage_j,
            K=stage_k, L=stage_l, M=stage_m, Q=stage_q, W=stage_w_both, V=stage_v, X=stage_x, S=stage_s,
        )
        for stage, *key in ORDER:
            stages[stage](*key)
            wait_sent(WAIT_LATER)
        wait_sent(0)
        for copy in out_copies:
            copy.wait()

    @pl.when(c == 0)
    def _():
        program(0)

    @pl.when(c == 1)
    def _():
        program(1)


def solution(mesh):
    dma = pltpu.SemaphoreType.DMA

    def per_device(inputs, gate_weight, up_weight, down_weight, norm_gain, norm_shift):
        any_space = pl.BlockSpec(memory_space=pl.ANY)
        return pl.pallas_call(
            kernel,
            out_shape=jax.ShapeDtypeStruct((T, DB), BF),
            in_specs=[any_space] * 6,
            out_specs=any_space,
            scratch_shapes=[
                pltpu.VMEM((2, NC, TC, DQ), BF),
                pltpu.VMEM((2, NT, DQ, 2 * UT), BF),
                pltpu.VMEM((2, NJ, 2, UT, DQ), BF),
                pltpu.VMEM((2, NJ, 2, DB, UT), BF),
                pltpu.VMEM((2, 2, NJ, UT // 2, DB), BF),
                pltpu.VMEM((2, NC, NJ, 4, 2, ZH, 4 * UT), BF),
                pltpu.VMEM((2, NC, NJ, 2, ZH, 4 * UT), BF),
                pltpu.VMEM((2, NC, NJ, 2, ZH, 4 * UT), BF),
                pltpu.VMEM((2, NC, NJ, 2, ZH, 4 * UT), BF),
                pltpu.VMEM((2, NC, NT, TC, UT), BF),
                pltpu.VMEM((2, NC, 4, 2, YH, DQ), BF),
                pltpu.VMEM((2, NC, 2, YH, DQ), BF),
                pltpu.VMEM((2, NC, 2, YH, DQ), BF),
                pltpu.VMEM((2, NC, 2, YH, DQ), BF),
                pltpu.VMEM((2, NC, 4, R, DQ), BF),
                pltpu.VMEM((2, NC, 3, R, DQ), BF),
                pltpu.VMEM((2, NC, R, DQ), F32),
                pltpu.VMEM((2, NC, R, 128), F32),
                pltpu.VMEM((2, NC, 3, R, 128), F32),
                pltpu.VMEM((2, NC, 4, R, DB), BF),
                pltpu.VMEM((T, DB), BF),
                pltpu.VMEM((4, 4, 2, DB), F32),
                dma((N_SLOTS,)),
                dma((N_SENT,)),
                dma((19 + NC,)),
                pltpu.SemaphoreType.REGULAR,
            ],
            compiler_params=pltpu.CompilerParams(
                collective_id=0, has_side_effects=True, vmem_limit_bytes=63 * 1024 * 1024
            ),
        )(inputs, gate_weight, up_weight, down_weight.reshape(LAYERS, TILES, UT, DB), norm_gain, norm_shift)

    return jax.shard_map(
        per_device,
        mesh=mesh,
        in_specs=(P(None, "ra"), P(None, "ra", "cb"), P(None, "ra", "cb"), P(None, "cb", "ra"), P(None, "ra"), P(None, "ra")),
        out_specs=P(None, "ra"),
        check_vma=False,
    )
```

```python
import jax
import jax.numpy as jnp
from jax import lax
from jax.experimental import pallas as pl
from jax.experimental.pallas import tpu as pltpu
from jax.sharding import PartitionSpec as P

MESH = pl.DeviceIdType.MESH
BF = jnp.bfloat16
F32 = jnp.float32
RESIDUAL = 0.5
EPSILON = 1e-05

T, D, FF, LAYERS = 1536, 4096, 11264, 2
NC = 6
TC = T // NC
ZB = TC // 4
ZH = ZB // 2
YB = TC // 4
YH = YB // 2
R = TC // 16
DB = D // 16
DQ = D // 4
UT = 128
NJ = 3
NT = 2 * NJ
TILES = FF // 8 // UT
SHARED = 4 * NJ - TILES

GROUPS = {(l, k): [(0, 1), (1, 2), (2, 3)] for l in range(LAYERS) for k in range(NC)}

SLOTS = {}


def slots(*names):
    for name in names:
        SLOTS.setdefault(name, len(SLOTS))


for k in range(NC):
    for g in range(max(len(GROUPS[l, k]) for l in range(LAYERS))):
        slots(("za", k, g), ("zc", k, g), ("h0", k, g))
    slots(*((m, k) for m in ("h1", "ya", "yc", "xr", "st", "xq", "xg", "y0", "y1", "y2")))
for l in range(LAYERS):
    for j in range(NJ + 1):
        slots(("wr", l, j), ("w", l, j))
slots(("gain",), *(("dd", k) for k in range(NC)))
N_SLOTS = len(SLOTS)
N_SENT = 40
WAIT_LATER = 30

SUM_AXIS, UNIT_AXIS = "zx", "xz"
ORDER = [
    ("X", 0, 0), ("W", 0, 0), ("W", 1, 0), ("X", 0, 3), ("W", 1, 2), ("X", 0, 5), ("S", 0, 0), ("V", 0, 0),
    ("S", 0, 3), ("X", 0, 2), ("S", 0, 5), ("K", -1, 0), ("W", 0, 2), ("K", -1, 3), ("W", 1, 1), ("K", -1, 5),
    ("S", 0, 2), ("X", 0, 4), ("L", -1, 0), ("V", 0, 2), ("V", 1, 2), ("W", 0, 1), ("L", -1, 3), ("L", -1, 5),
    ("K", -1, 2), ("A", 0, 0, 0), ("A", 0, 3, 0), ("A", 0, 3, 2), ("A", 0, 5, 0), ("L", -1, 2), ("B", 0, 0, 0),
    ("V", 0, 1), ("A", 0, 5, 2), ("X", 0, 1), ("B", 0, 3, 0), ("S", 0, 4), ("A", 0, 0, 2), ("B", 0, 3, 2),
    ("W", 0, 3), ("B", 0, 5, 0), ("A", 0, 2, 0), ("B", 0, 5, 2), ("A", 0, 3, 1), ("K", -1, 4), ("A", 0, 5, 1),
    ("C", 0, 5, 0), ("C", 0, 3, 2), ("A", 0, 0, 1), ("B", 0, 3, 1), ("L", -1, 4), ("S", 0, 1), ("C", 0, 3, 0),
    ("B", 0, 5, 1), ("C", 0, 5, 2), ("D", 0, 3, 2), ("B", 0, 2, 0), ("A", 0, 2, 2), ("C", 0, 3, 1), ("B", 0, 0, 1),
    ("C", 0, 5, 1), ("V", 0, 3), ("D", 0, 3, 0), ("B", 0, 0, 2), ("A", 0, 2, 1), ("D", 0, 5, 0), ("D", 0, 5, 2),
    ("K", -1, 1), ("D", 0, 3, 1), ("C", 0, 0, 0), ("D", 0, 5, 1), ("B", 0, 2, 2), ("C", 0, 0, 1), ("A", 0, 4, 1),
    ("C", 0, 0, 2), ("C", 0, 2, 0), ("B", 0, 2, 1), ("A", 0, 4, 0), ("L", -1, 1), ("E", 0, 3), ("A", 0, 4, 2),
    ("D", 0, 0, 1), ("C", 0, 2, 2), ("E", 0, 5), ("D", 0, 0, 2), ("D", 0, 0, 0), ("A", 0, 1, 1), ("G", 0, 3),
    ("B", 0, 4, 1), ("C", 0, 2, 1), ("A", 0, 1, 2), ("A", 0, 1, 0), ("B", 0, 4, 0), ("G", 0, 5), ("B", 0, 4, 2),
    ("E", 0, 0), ("D", 0, 2, 2), ("B", 0, 1, 1), ("H", 0, 3), ("B", 0, 1, 2), ("D", 0, 2, 0), ("D", 0, 2, 1),
    ("B", 0, 1, 0), ("H", 0, 5), ("C", 0, 4, 1), ("C", 0, 4, 0), ("C", 0, 4, 2), ("G", 0, 0), ("C", 0, 1, 1),
    ("C", 0, 1, 2), ("I", 0, 3), ("E", 0, 2), ("D", 0, 4, 1), ("C", 0, 1, 0), ("D", 0, 4, 0), ("D", 0, 4, 2),
    ("I", 0, 5), ("D", 0, 1, 2), ("D", 0, 1, 1), ("J", 0, 3), ("D", 0, 1, 0), ("H", 0, 0), ("G", 0, 2), ("V", 1, 0),
    ("E", 0, 4), ("J", 0, 5), ("Q", 0, 3), ("E", 0, 1), ("I", 0, 0), ("Q", 0, 5), ("G", 0, 4), ("V", 1, 1),
    ("H", 0, 2), ("K", 0, 3), ("J", 0, 0), ("G", 0, 1), ("K", 0, 5), ("H", 0, 4), ("I", 0, 2), ("L", 0, 3),
    ("Q", 0, 0), ("H", 0, 1), ("L", 0, 5), ("I", 0, 4), ("J", 0, 2), ("A", 1, 3, 1), ("K", 0, 0), ("A", 1, 3, 2),
    ("I", 0, 1), ("A", 1, 3, 0), ("Q", 0, 2), ("A", 1, 5, 1), ("J", 0, 4), ("A", 1, 5, 2), ("L", 0, 0),
    ("B", 1, 3, 1), ("J", 0, 1), ("B", 1, 3, 0), ("A", 1, 5, 0), ("B", 1, 5, 1), ("K", 0, 2), ("Q", 0, 4),
    ("B", 1, 5, 2), ("B", 1, 3, 2), ("A", 1, 0, 0), ("A", 1, 0, 2), ("Q", 0, 1), ("L", 0, 2), ("C", 1, 3, 0),
    ("A", 1, 0, 1), ("W", 1, 3), ("C", 1, 5, 2), ("B", 1, 0, 0), ("K", 0, 4), ("C", 1, 3, 2), ("B", 1, 0, 2),
    ("C", 1, 5, 1), ("B", 1, 5, 0), ("K", 0, 1), ("C", 1, 3, 1), ("A", 1, 2, 0), ("B", 1, 0, 1), ("A", 1, 2, 1),
    ("D", 1, 5, 2), ("L", 0, 4), ("C", 1, 5, 0), ("D", 1, 3, 0), ("C", 1, 0, 2), ("D", 1, 3, 2), ("A", 1, 2, 2),
    ("L", 0, 1), ("V", 1, 3), ("D", 1, 3, 1), ("D", 1, 5, 1), ("C", 1, 0, 1), ("C", 1, 0, 0), ("B", 1, 2, 0),
    ("A", 1, 4, 0), ("A", 1, 4, 1), ("B", 1, 2, 1), ("D", 1, 5, 0), ("D", 1, 0, 2), ("A", 1, 4, 2), ("B", 1, 2, 2),
    ("D", 1, 0, 1), ("A", 1, 1, 1), ("D", 1, 0, 0), ("A", 1, 1, 0), ("B", 1, 4, 0), ("E", 1, 3), ("B", 1, 4, 1),
    ("A", 1, 1, 2), ("C", 1, 2, 1), ("E", 1, 5), ("B", 1, 4, 2), ("B", 1, 1, 1), ("C", 1, 2, 0), ("C", 1, 2, 2),
    ("G", 1, 3), ("E", 1, 0), ("B", 1, 1, 0), ("B", 1, 1, 2), ("G", 1, 5), ("C", 1, 4, 0), ("C", 1, 4, 1),
    ("C", 1, 4, 2), ("H", 1, 3), ("D", 1, 2, 0), ("D", 1, 2, 1), ("G", 1, 0), ("D", 1, 2, 2), ("C", 1, 1, 1),
    ("C", 1, 1, 0), ("C", 1, 1, 2), ("D", 1, 4, 1), ("D", 1, 4, 0), ("D", 1, 4, 2), ("H", 1, 5), ("E", 1, 2),
    ("D", 1, 1, 2), ("D", 1, 1, 0), ("D", 1, 1, 1), ("H", 1, 0), ("I", 1, 3), ("E", 1, 4), ("I", 1, 5), ("G", 1, 2),
    ("E", 1, 1), ("I", 1, 0), ("J", 1, 3), ("J", 1, 5), ("G", 1, 4), ("H", 1, 2), ("G", 1, 1), ("K", 1, 3),
    ("J", 1, 0), ("H", 1, 4), ("K", 1, 5), ("I", 1, 2), ("H", 1, 1), ("K", 1, 0), ("I", 1, 4), ("L", 1, 3),
    ("L", 1, 5), ("J", 1, 2), ("L", 1, 0), ("I", 1, 1), ("J", 1, 4), ("K", 1, 2), ("M", 1, 5), ("M", 1, 3),
    ("M", 1, 0), ("J", 1, 1), ("K", 1, 4), ("L", 1, 2), ("K", 1, 1), ("L", 1, 4), ("M", 1, 2), ("L", 1, 1),
    ("M", 1, 4), ("M", 1, 1),
]


def kernel(
    x_hbm, wg_hbm, wu_hbm, wd_hbm, gain_hbm, shift_hbm, out_hbm,
    xs, wgu, wd, rel, rel_d, part, ra, rb, rc, hid, down, ya, yb, yc, ys, xr, mixed, st, st_in, nb, ov, gains,
    recv, sent, local, go,
):
    ra_at, cb_at = lax.axis_index("ra"), lax.axis_index("cb")
    z, x = ra_at // 4, lax.rem(ra_at, 4)
    y, c = cb_at // 2, lax.rem(cb_at, 2)

    def turn(v, d):
        return lax.rem(v + d, 4)

    zp, zo, zm = turn(z, 1), turn(z, 2), turn(z, 3)
    yp, yo, ym = turn(y, 1), turn(y, 2), turn(y, 3)
    xp, xo, xm = turn(x, 1), turn(x, 2), turn(x, 3)

    def at_z(v):
        return (v * 4 + x, cb_at)

    def at_x(v):
        return (z * 4 + v, cb_at)

    def at_sum(l, v):
        return at_z(v) if SUM_AXIS[l] == "z" else at_x(v)

    def at_unit(l, v):
        return at_x(v) if UNIT_AXIS[l] == "x" else at_z(v)

    def at_unit_main(l, v):
        return (z * 4 + v, y * 2 + 1) if UNIT_AXIS[l] == "x" else (v * 4 + x, y * 2 + 1)

    sums = [(zp, zo, zm, z), (xp, xo, xm, x)]
    unit_at = [(xp, xo, xm, x), (zp, zo, zm, z)]

    def at_y(v):
        return (ra_at, v * 2 + c)

    other = (ra_at, y * 2 + (1 - c))

    peers = [at_z(zp), at_z(zo), at_z(zm), at_x(xp), at_x(xo), at_x(xm), at_y(yp), at_y(ym), other]
    peers += [(z * 4 + xp, y * 2 + (1 - c)), (z * 4 + xm, y * 2 + (1 - c))]
    peers += [(zp * 4 + x, y * 2 + (1 - c)), (zm * 4 + x, y * 2 + (1 - c))]
    barrier = pltpu.get_barrier_semaphore()
    for peer in peers:
        pl.semaphore_signal(barrier, inc=1, device_id=peer, device_id_type=MESH)
    pl.semaphore_wait(barrier, len(peers))

    def arrived(dst, name):
        pltpu.make_async_remote_copy(
            src_ref=dst, dst_ref=dst, send_sem=sent.at[0], recv_sem=recv.at[SLOTS[name]],
            device_id=other, device_id_type=MESH,
        ).wait_recv()

    def d_cols(v):
        return pl.ds(pl.multiple_of(v * DB, DB), DB)

    def tile_of(v):
        return jnp.minimum(v * NJ, TILES - NJ)

    def units(v, j):
        return pl.ds(pl.multiple_of((tile_of(v) + j) * UT, UT), UT)

    def gu_half(l, j, cc, owner, what):
        return wgu.at[l, 2 * j + cc, d_cols(owner), pl.ds(what * UT, UT)]

    def relay_ref(l, j, h):
        return rel.at[l, j, h] if j < NJ else rel_d.at[l, h]

    def w_half(l, j, cc, owner, h):
        if j < NJ:
            return gu_half(l, j, cc, owner, h)
        return wd.at[l, :, cc, pl.ds(h * 64, 64), d_cols(owner)]

    def w_whole(l, j, cc, owner):
        return wgu.at[l, 2 * j + cc, d_cols(owner), :] if j < NJ else wd.at[l, :, cc, :, d_cols(owner)]

    def program(core):
        waits = []
        local_waits = {}

        def send(src, dst, name, dev):
            pltpu.make_async_remote_copy(
                src_ref=src, dst_ref=dst, send_sem=sent.at[len(waits) % N_SENT], recv_sem=recv.at[SLOTS[name]],
                device_id=dev, device_id_type=MESH,
            ).start()

        def all_sent(like):
            waits.append(
                pltpu.make_async_remote_copy(
                    src_ref=like, dst_ref=like, send_sem=sent.at[len(waits) % N_SENT], recv_sem=recv.at[0],
                    device_id=other, device_id_type=MESH,
                ).wait_send
            )

        done = []

        def wait_sent(keep):
            while len(waits) - len(done) > keep:
                waits[len(done)]()
                done.append(True)

        def stage_w(l, j):
            up, opposite, back, me = unit_at[l]
            if j < NJ:
                sources = (wg_hbm, wu_hbm)
                send(wg_hbm.at[l, :, units(opposite, j)], rel.at[l, j, 0], ("wr", l, j), at_unit(l, up))
                send(wu_hbm.at[l, :, units(opposite, j)], rel.at[l, j, 1], ("wr", l, j), at_unit(l, back))
                for what, src in enumerate(sources):
                    for to in (up, back):
                        send(
                            src.at[l, :, units(to, j)], gu_half(l, j, core, me, what), ("w", l, j), at_unit_main(l, to)
                        )
                if core == 0:
                    for what, src in enumerate(sources):
                        send(src.at[l, :, units(me, j)], gu_half(l, j, core, me, what), ("w", l, j), other)
                else:
                    mine = []
                    for what, src in enumerate(sources):
                        copy = pltpu.make_async_copy(
                            src.at[l, :, units(me, j)], gu_half(l, j, core, me, what), local.at[l * 7 + j * 2 + what]
                        )
                        copy.start()
                        mine.append(copy.wait)
                    local_waits[l, j] = mine
                all_sent(wgu.at[l, 0:4 - core, 0:DB, :])
            else:
                def src(v, h=None):
                    if h is None:
                        return wd_hbm.at[l, pl.ds(tile_of(v), NJ)]
                    return wd_hbm.at[l, pl.ds(tile_of(v), NJ), pl.ds(h * 64, 64)]

                send(src(opposite, 0), rel_d.at[l, 0], ("wr", l, j), at_unit(l, up))
                send(src(opposite, 1), rel_d.at[l, 1], ("wr", l, j), at_unit(l, back))
                send(src(up), w_whole(l, j, core, me), ("w", l, j), at_unit_main(l, up))
                send(src(back), w_whole(l, j, core, me), ("w", l, j), at_unit_main(l, back))
                if core == 0:
                    send(src(me), w_whole(l, j, core, me), ("w", l, j), other)
                else:
                    copy = pltpu.make_async_copy(src(me), w_whole(l, j, core, me), local.at[l * 7 + 6])
                    copy.start()
                    local_waits[l, j] = [copy.wait]
                all_sent(wgu.at[l, 0:4 - core, 0:NJ * UT, :])

        def stage_v(l, j):
            up, _, back, _ = unit_at[l]
            arrived(rel.at[l, j] if j < NJ else rel_d.at[l], ("wr", l, j))
            for h, (to, owner) in enumerate(((up, back), (back, up))):
                send(relay_ref(l, j, h), w_half(l, j, core, owner, h), ("w", l, j), at_unit_main(l, to))
            all_sent(wgu.at[l, 0, 0:DB if j < NJ else NJ * UT, :])

        if core == 0:
            for i, (stage, *key) in enumerate([t for t in ORDER if t[0] in "WV"]):
                if stage == "W":
                    if i:
                        pl.semaphore_wait(go, 1)
                    stage_w(*key)
                else:
                    stage_v(*key)
            copies = []
            for k in range(NC):
                rows = pl.ds(k * TC, TC)
                arrived(ov.at[rows, :], ("dd", k))
                copies.append(pltpu.make_async_copy(ov.at[rows, :], out_hbm.at[rows, :], local.at[k]))
                copies[-1].start()
            wait_sent(0)
            for copy in copies:
                copy.wait()
            return

        def weights_ready(l, j):
            for wait in local_waits[l, j]:
                wait()
            arrived(wgu.at[l, 0:2, 0:7 * DB // 2, :] if j < NJ else wgu.at[l, 0:3, 0:7 * UT, :], ("w", l, j))

        def gathered(p, k, at, rows):
            if p < LAYERS:
                return xs.at[p, k, pl.ds(pl.multiple_of(at, rows), rows), :]
            return ov.at[pl.ds(pl.multiple_of(k * TC + at, rows), rows), :]

        def part_rows(v):
            return y * YB + v * R

        in_copies = {}
        out_copies = []
        y_block = pl.ds(pl.multiple_of(y * YB, YB), YB)

        def stage_x(l, k):
            def half(h):
                rows = pl.ds(pl.multiple_of(k * TC + y * YB + h * YH, YH), YH)
                return x_hbm.at[rows, :], xs.at[0, k, pl.ds(pl.multiple_of(y * YB + h * YH, YH), YH), d_cols(x)]

            for h, name in enumerate((("xq", k), ("xg", k))):
                send(*half(h), name, at_x(xp))
                send(*half(1 - h), name, at_x(xm))
            all_sent(ov.at[0:2 * YB, :])
            rows = pl.ds(pl.multiple_of(k * TC + y * YB, YB), YB)
            in_copies[k] = pltpu.make_async_copy(x_hbm.at[rows, :], xs.at[0, k, y_block, d_cols(x)], local.at[14 + k])
            in_copies[k].start()

        def stage_s(l, k):
            arrived(ov.at[0:YB, :], ("xq", k))
            for h, (owner, to) in enumerate(((xm, xp), (xp, xm))):
                ref = xs.at[0, k, pl.ds(pl.multiple_of(y * YB + h * YH, YH), YH), d_cols(owner)]
                send(ref, ref, ("xg", k), at_x(to))
            all_sent(ov.at[0:YB, :])

        gain_copies = []

        def gains_send():
            for i, (src, axis) in enumerate(((gain_hbm, 0), (shift_hbm, 0), (gain_hbm, 1), (shift_hbm, 1))):
                me = unit_at[axis][3]
                for d in (1, 3, 2):
                    send(src, gains.at[i, me], ("gain",), at_unit(axis, turn(me, d)))
                all_sent(gains.at[i, 0:3])
                copy = pltpu.make_async_copy(src, gains.at[i, me], local.at[14 + NC + i])
                copy.start()
                gain_copies.append(copy)

        seen = set()

        def stage_a(l, k, g):
            first, last = GROUPS[l, k][g]
            if ("x", l, k) not in seen:
                seen.add(("x", l, k))
                arrived(xs.at[l, k, 0:YB, :], ("y1", k))
                arrived(xs.at[l, k, 0:YB, :], ("y2", k))
            for j in range(first, last):
                if (l, j) not in seen:
                    weights_ready(l, j)
                    seen.add((l, j))

            def tiles(j, carry):
                rhs = jnp.concatenate([wgu[l, 2 * j], wgu[l, 2 * j + 1]], axis=1)
                value = jnp.dot(xs[l, k], rhs, preferred_element_type=F32).astype(BF)
                for o in range(4):
                    for h in (0, 1):
                        at = o * ZB + h * ZH
                        part[l, k, j, o, h] = value[at:at + ZH]
                return carry

            lax.fori_loop(first, last, tiles, 0)
            js = pl.ds(first, last - first)
            up, opposite, back, _ = sums[l]
            send(part.at[l, k, js, opposite, 0], ra.at[l, k, js, 0], ("za", k, g), at_sum(l, up))
            send(part.at[l, k, js, opposite, 1], ra.at[l, k, js, 1], ("za", k, g), at_sum(l, back))
            send(part.at[l, k, js, up, 1], rb.at[l, k, js, 0], ("zc", k, g), at_sum(l, up))
            send(part.at[l, k, js, back, 0], rb.at[l, k, js, 1], ("zc", k, g), at_sum(l, back))
            all_sent(part.at[l, k, js, 0:2])

        def stage_b(l, k, g):
            first, last = GROUPS[l, k][g]
            js = pl.ds(first, last - first)
            up, _, back, _ = sums[l]
            arrived(ra.at[l, k, js], ("za", k, g))
            for h, to in enumerate((up, back)):
                for j in range(first, last):
                    part[l, k, j, to, h] = (part[l, k, j, to, h].astype(F32) + ra[l, k, j, h].astype(F32)).astype(BF)
                send(part.at[l, k, js, to, h], rc.at[l, k, js, h], ("zc", k, g), at_sum(l, to))
            all_sent(part.at[l, k, js, 0])

        def hid_ref(l, k, g, o, h):
            first, last = GROUPS[l, k][g]
            rows = pl.ds(pl.multiple_of(o * ZB + h * ZH, ZH), ZH)
            return hid.at[l, k, pl.ds(2 * first, 2 * (last - first)), rows, :]

        def stage_c(l, k, g):
            first, last = GROUPS[l, k][g]
            js = pl.ds(first, last - first)
            up, _, back, me = sums[l]
            arrived(part.at[l, k, js, 0:2], ("zc", k, g))
            for h in (0, 1):
                for j in range(first, last):
                    total = (
                        part[l, k, j, me, h].astype(F32) + rc[l, k, j, h].astype(F32) + rb[l, k, j, 1 - h].astype(F32)
                    )
                    for n in (0, 1):
                        gate, lift = total[:, n * 256:n * 256 + UT], total[:, n * 256 + UT:(n + 1) * 256]
                        value = gate * jax.nn.sigmoid(gate) * lift
                        if j < SHARED:
                            value = jnp.where(unit_at[l][3] == 3, jnp.zeros_like(value), value)
                        hid[l, k, 2 * j + n, pl.ds(pl.multiple_of(me * ZB + h * ZH, ZH), ZH), :] = value.astype(BF)
                if h == 0:
                    ref = hid_ref(l, k, g, me, 0)
                    send(ref, ref, ("h0", k, g), at_sum(l, up))
            ref = hid_ref(l, k, g, me, 1)
            send(ref, ref, ("h0", k, g), at_sum(l, back))
            send(ref, ref, ("h1", k), at_sum(l, up))
            ref = hid_ref(l, k, g, me, 0)
            send(ref, ref, ("h1", k), at_sum(l, back))
            all_sent(hid.at[l, k, pl.ds(2 * first, 2 * (last - first)), 0:4 * ZH, :])

        def stage_d(l, k, g):
            first, last = GROUPS[l, k][g]
            up, _, back, _ = sums[l]
            arrived(hid.at[l, k, pl.ds(2 * first, 2 * (last - first)), 0:2 * ZH, :], ("h0", k, g))
            for h, (owner, to) in enumerate(((back, up), (up, back))):
                ref = hid_ref(l, k, g, owner, h)
                send(ref, ref, ("h1", k), at_sum(l, to))
            all_sent(hid.at[l, k, pl.ds(2 * first, 2 * (last - first)), 0:2 * ZH, :])

        def stage_e(l, k):
            arrived(hid.at[l, k, :, 0:4 * ZH, :], ("h1", k))
            if (l, NJ) not in seen:
                weights_ready(l, NJ)
                seen.add((l, NJ))

            def columns(n, carry):
                lhs = jnp.concatenate([hid[l, k, t] for t in range(NT)], axis=1)
                cols = pl.ds(pl.multiple_of(n * 512, 512), 512)
                rhs = wd[l, :, :, :, cols].reshape(NT * UT, 512)
                value = jnp.dot(lhs, rhs, preferred_element_type=F32).astype(BF)
                for yy in range(4):
                    for h in (0, 1):
                        at = yy * YB + h * YH
                        down[l, k, yy, h, :, cols] = value[at:at + YH]
                return carry

            lax.fori_loop(0, DQ // 512, columns, 0)
            send(down.at[l, k, yo, 0], ya.at[l, k, 0], ("ya", k), at_y(yp))
            send(down.at[l, k, yo, 1], ya.at[l, k, 1], ("ya", k), at_y(ym))
            send(down.at[l, k, yp, 1], yb.at[l, k, 0], ("yc", k), at_y(yp))
            send(down.at[l, k, ym, 0], yb.at[l, k, 1], ("yc", k), at_y(ym))
            all_sent(down.at[l, k, 0:2])

        def stage_g(l, k):
            arrived(ya.at[l, k], ("ya", k))
            for h, to in enumerate((yp, ym)):
                down[l, k, to, h] = (down[l, k, to, h].astype(F32) + ya[l, k, h].astype(F32)).astype(BF)
                send(down.at[l, k, to, h], yc.at[l, k, h], ("yc", k), at_y(to))
            all_sent(down.at[l, k, 0])

        def stage_h(l, k):
            arrived(down.at[l, k, 0:2], ("yc", k))
            for h in (0, 1):
                total = down[l, k, y, h].astype(F32) + yc[l, k, h].astype(F32) + yb[l, k, 1 - h].astype(F32)
                ys[l, k, 2 * h] = total[:R].astype(BF)
                ys[l, k, 2 * h + 1] = total[R:].astype(BF)
            me = unit_at[l][3]
            for d in (2, 1, 3):
                send(ys.at[l, k, turn(me, d)], xr.at[l, k, d - 1], ("xr", k), at_unit(l, turn(me, d)))
            all_sent(ys.at[l, k, 0:3])

        def stage_i(l, k):
            me = unit_at[l][3]
            rows = pl.ds(pl.multiple_of(part_rows(me), R), R)
            value = RESIDUAL * xs[l, k, rows, :].astype(F32) + ys[l, k, me].astype(F32)
            arrived(xr.at[l, k], ("xr", k))
            for d in (1, 3, 2):
                value = value + xr[l, k, d - 1].astype(F32)
            mixed[l, k] = value
            row_sum = jnp.sum(value, axis=1, keepdims=True)
            row_squares = jnp.sum(value * value, axis=1, keepdims=True)
            lane = lax.broadcasted_iota(jnp.int32, (R, 128), 1)
            st[l, k] = jnp.where(lane == 0, row_sum, jnp.where(lane == 1, row_squares, 0.0))
            for d in (2, 1, 3):
                send(st.at[l, k], st_in.at[l, k, d - 1], ("st", k), at_sum(l, turn(sums[l][3], d)))
            all_sent(st_in.at[l, k])

        def stage_j(l, k):
            me = unit_at[l][3]
            if ("gain",) not in seen:
                seen.add(("gain",))
                arrived(gains.at[0:3], ("gain",))
                for copy in gain_copies:
                    copy.wait()
            stats = st[l, k]
            arrived(st_in.at[l, k], ("st", k))
            for d in (1, 3, 2):
                stats = stats + st_in[l, k, d - 1]
            mean = stats[:, 0:1] / D
            var = stats[:, 1:2] / D - mean * mean
            scale = lax.rsqrt(var + EPSILON)
            for q in range(4):
                cols = slice(q * DB, (q + 1) * DB)
                normed = (mixed[l, k, :, cols] - mean) * scale
                nb[l, k, q] = (normed * gains[2 * l, q, l:l + 1, :] + gains[2 * l + 1, q, l:l + 1, :]).astype(BF)

            if l + 1 < LAYERS:
                dst = xs.at[1, k, pl.ds(pl.multiple_of(part_rows(me), R), R), d_cols(z)]
            else:
                dst = gathered(LAYERS, k, part_rows(me), R)
            dst[...] = nb[l, k, me]
            for d in (2, 1, 3):
                name = ("xq", k) if l + 1 < LAYERS else ("xg", k)
                send(nb.at[l, k, turn(me, d)], dst, name, at_unit(l, turn(me, d)))
            all_sent(nb.at[l, k, 0:3])

        def stage_q(l, k):
            arrived(nb.at[0, k, 0:3], ("xq", k))
            ref = xs.at[1, k, y_block, d_cols(z)]
            for d in (2, 1, 3):
                send(ref, ref, ("xg", k), at_z(turn(z, d)))
            all_sent(ov.at[0:3 * YB, :])

        def stage_k(l, k):
            p = l + 1
            got = (ov.at[0:2 * YB, :], ov.at[0:3 * YB, :], nb.at[1, k, 0:3])[p]
            arrived(got, ("xg", k))
            if p == 0:
                in_copies[k].wait()
            for h in (0, 1):
                ref = gathered(p, k, y * YB + h * YH, YH)
                send(ref, ref, (("y0", "y1")[h], k), at_y(yp))
                ref = gathered(p, k, y * YB + (1 - h) * YH, YH)
                send(ref, ref, (("y0", "y1")[h], k), at_y(ym))
            if p == LAYERS:
                ref = gathered(p, k, y * YB, YB)
                send(ref, ref, ("dd", k), other)
                all_sent(ov.at[0:6 * YH, :])
            else:
                all_sent(xs.at[p, k, 0:4 * YH, :])

        def stage_l(l, k):
            p = l + 1
            halves = (lambda n: xs.at[p, k, 0:n * YH, :]) if p < LAYERS else (lambda n: ov.at[0:n * YH, :])
            arrived(halves(2), ("y0", k))
            for h, (owner, to) in enumerate(((ym, yp), (yp, ym))):
                ref = gathered(p, k, owner * YB + h * YH, YH)
                send(ref, ref, ("y2", k), at_y(to))
            if p == LAYERS:
                arrived(halves(2), ("y1", k))
                for owner in (ym, yp):
                    ref = gathered(p, k, owner * YB, YB)
                    send(ref, ref, ("dd", k), other)
                all_sent(ov.at[0:6 * YH, :])
            else:
                all_sent(xs.at[p, k, 0:2 * YH, :])

        def stage_m(l, k):
            p = l + 1
            arrived(ov.at[0:YB, :], ("y2", k))
            ref = gathered(p, k, yo * YB, YB)
            send(ref, ref, ("dd", k), other)
            all_sent(ov.at[0:YB, :])
            rows = pl.ds(k * TC, TC)
            out_copies.append(pltpu.make_async_copy(ov.at[rows, :], out_hbm.at[rows, :], local.at[14 + k]))
            out_copies[-1].start()

        def stage_w_both(l, j):
            if l + j == 0:
                stage_w(l, j)
                gains_send()
                return
            pl.semaphore_signal(go, inc=1, device_id=other, device_id_type=MESH)
            stage_w(l, j)

        stages = dict(
            A=stage_a, B=stage_b, C=stage_c, D=stage_d, E=stage_e, G=stage_g, H=stage_h, I=stage_i, J=stage_j,
            K=stage_k, L=stage_l, M=stage_m, Q=stage_q, W=stage_w_both, V=stage_v, X=stage_x, S=stage_s,
        )
        for stage, *key in ORDER:
            stages[stage](*key)
            wait_sent(WAIT_LATER)
        wait_sent(0)
        for copy in out_copies:
            copy.wait()

    @pl.when(c == 0)
    def _():
        program(0)

    @pl.when(c == 1)
    def _():
        program(1)


def solution(mesh):
    dma = pltpu.SemaphoreType.DMA

    def per_device(inputs, gate_weight, up_weight, down_weight, norm_gain, norm_shift):
        any_space = pl.BlockSpec(memory_space=pl.ANY)
        return pl.pallas_call(
            kernel,
            out_shape=jax.ShapeDtypeStruct((T, DB), BF),
            in_specs=[any_space] * 6,
            out_specs=any_space,
            scratch_shapes=[
                pltpu.VMEM((2, NC, TC, DQ), BF),
                pltpu.VMEM((2, NT, DQ, 2 * UT), BF),
                pltpu.VMEM((2, NJ, 2, UT, DQ), BF),
                pltpu.VMEM((2, NJ, 2, DB, UT), BF),
                pltpu.VMEM((2, 2, NJ, UT // 2, DB), BF),
                pltpu.VMEM((2, NC, NJ, 4, 2, ZH, 4 * UT), BF),
                pltpu.VMEM((2, NC, NJ, 2, ZH, 4 * UT), BF),
                pltpu.VMEM((2, NC, NJ, 2, ZH, 4 * UT), BF),
                pltpu.VMEM((2, NC, NJ, 2, ZH, 4 * UT), BF),
                pltpu.VMEM((2, NC, NT, TC, UT), BF),
                pltpu.VMEM((2, NC, 4, 2, YH, DQ), BF),
                pltpu.VMEM((2, NC, 2, YH, DQ), BF),
                pltpu.VMEM((2, NC, 2, YH, DQ), BF),
                pltpu.VMEM((2, NC, 2, YH, DQ), BF),
                pltpu.VMEM((2, NC, 4, R, DQ), BF),
                pltpu.VMEM((2, NC, 3, R, DQ), BF),
                pltpu.VMEM((2, NC, R, DQ), F32),
                pltpu.VMEM((2, NC, R, 128), F32),
                pltpu.VMEM((2, NC, 3, R, 128), F32),
                pltpu.VMEM((2, NC, 4, R, DB), BF),
                pltpu.VMEM((T, DB), BF),
                pltpu.VMEM((4, 4, 2, DB), F32),
                dma((N_SLOTS,)),
                dma((N_SENT,)),
                dma((19 + NC,)),
                pltpu.SemaphoreType.REGULAR,
            ],
            compiler_params=pltpu.CompilerParams(
                collective_id=0, has_side_effects=True, vmem_limit_bytes=63 * 1024 * 1024
            ),
        )(inputs, gate_weight, up_weight, down_weight.reshape(LAYERS, TILES, UT, DB), norm_gain, norm_shift)

    return jax.shard_map(
        per_device,
        mesh=mesh,
        in_specs=(P(None, "ra"), P(None, "ra", "cb"), P(None, "ra", "cb"), P(None, "cb", "ra"), P(None, "ra"), P(None, "ra")),
        out_specs=P(None, "ra"),
        check_vma=False,
    )
```

```python
import jax
import jax.numpy as jnp
from jax import lax
from jax.experimental import pallas as pl
from jax.experimental.pallas import tpu as pltpu
from jax.sharding import PartitionSpec as P

MESH = pl.DeviceIdType.MESH
BF = jnp.bfloat16
F32 = jnp.float32
RESIDUAL = 0.5
EPSILON = 1e-05

T, D, FF, LAYERS = 1536, 4096, 11264, 2
NC = 6
TC = T // NC
ZB = TC // 4
ZH = ZB // 2
YB = TC // 4
YH = YB // 2
R = TC // 16
DB = D // 16
DQ = D // 4
UT = 128
NJ = 3
NT = 2 * NJ
TILES = FF // 8 // UT
SHARED = 4 * NJ - TILES

GROUPS = {(l, k): [(0, 1), (1, 2), (2, 3)] if l == 0 else [(0, 1), (1, 3)] for l in range(LAYERS) for k in range(NC)}

SLOTS = {}


def slots(*names):
    for name in names:
        SLOTS.setdefault(name, len(SLOTS))


for k in range(NC):
    for g in range(max(len(GROUPS[l, k]) for l in range(LAYERS))):
        slots(("za", k, g), ("zc", k, g), ("h0", k, g))
    slots(*((m, k) for m in ("h1", "ya", "yc", "xr", "st", "xq", "xg", "y0", "y1", "y2")))
for l in range(LAYERS):
    for j in range(NJ + 1):
        slots(("wr", l, j), ("w", l, j))
slots(("gain",), *(("dd", k) for k in range(NC)))
N_SLOTS = len(SLOTS)
N_SENT = 40
WAIT_LATER = 30

SUM_AXIS, UNIT_AXIS = "zx", "xz"
DIRECT = (4, 5)
ORDER = [
    ("X", 0, 0), ("W", 0, 0), ("W", 1, 2), ("W", 1, 1), ("X", 0, 3), ("S", 0, 0), ("X", 0, 1), ("V", 0, 0),
    ("S", 0, 3), ("X", 0, 2), ("S", 0, 1), ("K", -1, 0), ("W", 0, 1), ("K", -1, 3), ("S", 0, 2), ("W", 1, 0),
    ("K", -1, 1), ("V", 0, 1), ("X", 0, 5), ("L", -1, 0), ("L", -1, 3), ("L", -1, 1), ("W", 0, 2), ("V", 1, 0),
    ("K", -1, 2), ("A", 0, 0, 0), ("A", 0, 3, 0), ("A", 0, 3, 1), ("A", 0, 0, 1), ("L", -1, 2), ("V", 0, 2),
    ("S", 0, 5), ("A", 0, 1, 1), ("B", 0, 3, 0), ("B", 0, 0, 0), ("A", 0, 1, 0), ("X", 0, 4), ("B", 0, 3, 1),
    ("W", 0, 3), ("A", 0, 2, 1), ("A", 0, 2, 0), ("A", 0, 2, 2), ("K", -1, 5), ("A", 0, 3, 2), ("B", 0, 2, 1),
    ("S", 0, 4), ("A", 0, 1, 2), ("B", 0, 2, 0), ("B", 0, 2, 2), ("C", 0, 3, 1), ("B", 0, 3, 2), ("C", 0, 3, 0),
    ("L", -1, 5), ("B", 0, 1, 1), ("C", 0, 2, 1), ("V", 0, 3), ("B", 0, 1, 2), ("C", 0, 2, 0), ("C", 0, 2, 2),
    ("B", 0, 1, 0), ("C", 0, 3, 2), ("A", 0, 0, 2), ("C", 0, 1, 1), ("D", 0, 2, 1), ("K", -1, 4), ("D", 0, 2, 0),
    ("D", 0, 2, 2), ("C", 0, 1, 2), ("D", 0, 3, 0), ("D", 0, 3, 1), ("C", 0, 1, 0), ("D", 0, 3, 2), ("A", 0, 5, 1),
    ("B", 0, 0, 1), ("B", 0, 0, 2), ("A", 0, 5, 0), ("L", -1, 4), ("D", 0, 1, 1), ("E", 0, 2), ("A", 0, 5, 2),
    ("D", 0, 1, 2), ("E", 0, 3), ("C", 0, 0, 0), ("D", 0, 1, 0), ("C", 0, 0, 1), ("A", 0, 4, 2), ("A", 0, 4, 1),
    ("G", 0, 2), ("B", 0, 5, 1), ("C", 0, 0, 2), ("A", 0, 4, 0), ("B", 0, 5, 2), ("G", 0, 3), ("E", 0, 1),
    ("B", 0, 5, 0), ("B", 0, 4, 2), ("B", 0, 4, 1), ("H", 0, 2), ("D", 0, 0, 2), ("D", 0, 0, 0), ("D", 0, 0, 1),
    ("B", 0, 4, 0), ("C", 0, 5, 1), ("C", 0, 5, 2), ("H", 0, 3), ("G", 0, 1), ("C", 0, 5, 0), ("C", 0, 4, 2),
    ("C", 0, 4, 1), ("I", 0, 2), ("E", 0, 0), ("C", 0, 4, 0), ("D", 0, 5, 2), ("D", 0, 5, 1), ("D", 0, 5, 0),
    ("I", 0, 3), ("D", 0, 4, 1), ("J", 0, 2), ("H", 0, 1), ("D", 0, 4, 2), ("D", 0, 4, 0), ("G", 0, 0), ("V", 1, 2),
    ("E", 0, 5), ("J", 0, 3), ("Q", 0, 2), ("E", 0, 4), ("I", 0, 1), ("Q", 0, 3), ("H", 0, 0), ("G", 0, 5),
    ("K", 0, 2), ("J", 0, 1), ("V", 1, 1), ("G", 0, 4), ("K", 0, 3), ("H", 0, 5), ("I", 0, 0), ("Q", 0, 1),
    ("L", 0, 2), ("H", 0, 4), ("L", 0, 3), ("J", 0, 0), ("I", 0, 5), ("K", 0, 1), ("A", 1, 2, 0), ("A", 1, 2, 1),
    ("I", 0, 4), ("Q", 0, 0), ("J", 0, 5), ("A", 1, 3, 1), ("L", 0, 1), ("J", 0, 4), ("B", 1, 2, 0), ("A", 1, 3, 0),
    ("B", 1, 2, 1), ("K", 0, 0), ("B", 1, 3, 1), ("Q", 0, 5), ("A", 1, 1, 1), ("Q", 0, 4), ("C", 1, 2, 0),
    ("L", 0, 0), ("W", 1, 3), ("A", 1, 1, 0), ("C", 1, 3, 1), ("B", 1, 3, 0), ("K", 0, 4), ("C", 1, 2, 1),
    ("B", 1, 1, 1), ("A", 1, 0, 1), ("D", 1, 3, 1), ("L", 0, 4), ("V", 1, 3), ("B", 1, 1, 0), ("C", 1, 3, 0),
    ("K", 0, 5), ("D", 1, 2, 0), ("A", 1, 0, 0), ("B", 1, 0, 1), ("D", 1, 2, 1), ("C", 1, 1, 0), ("C", 1, 1, 1),
    ("L", 0, 5), ("D", 1, 3, 0), ("A", 1, 4, 0), ("B", 1, 0, 0), ("A", 1, 4, 1), ("E", 1, 2), ("C", 1, 0, 1),
    ("E", 1, 3), ("D", 1, 1, 1), ("D", 1, 1, 0), ("B", 1, 4, 0), ("C", 1, 0, 0), ("A", 1, 5, 1), ("G", 1, 2),
    ("A", 1, 5, 0), ("G", 1, 3), ("B", 1, 4, 1), ("E", 1, 1), ("D", 1, 0, 0), ("B", 1, 5, 1), ("D", 1, 0, 1),
    ("H", 1, 2), ("B", 1, 5, 0), ("C", 1, 4, 0), ("H", 1, 3), ("C", 1, 4, 1), ("C", 1, 5, 1), ("G", 1, 1),
    ("E", 1, 0), ("C", 1, 5, 0), ("D", 1, 4, 0), ("D", 1, 4, 1), ("I", 1, 3), ("I", 1, 2), ("D", 1, 5, 1),
    ("D", 1, 5, 0), ("H", 1, 1), ("G", 1, 0), ("E", 1, 4), ("J", 1, 3), ("J", 1, 2), ("E", 1, 5), ("H", 1, 0),
    ("I", 1, 1), ("G", 1, 4), ("K", 1, 3), ("K", 1, 2), ("J", 1, 1), ("G", 1, 5), ("I", 1, 0), ("H", 1, 4),
    ("L", 1, 3), ("L", 1, 2), ("K", 1, 1), ("J", 1, 0), ("H", 1, 5), ("I", 1, 4), ("L", 1, 1), ("M", 1, 3),
    ("M", 1, 2), ("K", 1, 0), ("I", 1, 5), ("J", 1, 4), ("M", 1, 1), ("L", 1, 0), ("J", 1, 5), ("M", 1, 0),
]


def kernel(
    x_hbm, wg_hbm, wu_hbm, wd_hbm, gain_hbm, shift_hbm, out_hbm,
    xs, wgu, wd, rel, rel_d, part, ra, rb, rc, hid, down, ya, yb, yc, ys, xr, mixed, st, st_in, nb, ov, gains,
    recv, sent, local, go,
):
    ra_at, cb_at = lax.axis_index("ra"), lax.axis_index("cb")
    z, x = ra_at // 4, lax.rem(ra_at, 4)
    y, c = cb_at // 2, lax.rem(cb_at, 2)

    def turn(v, d):
        return lax.rem(v + d, 4)

    zp, zo, zm = turn(z, 1), turn(z, 2), turn(z, 3)
    yp, yo, ym = turn(y, 1), turn(y, 2), turn(y, 3)
    xp, xo, xm = turn(x, 1), turn(x, 2), turn(x, 3)

    def at_z(v):
        return (v * 4 + x, cb_at)

    def at_x(v):
        return (z * 4 + v, cb_at)

    def at_sum(l, v):
        return at_z(v) if SUM_AXIS[l] == "z" else at_x(v)

    def at_unit(l, v):
        return at_x(v) if UNIT_AXIS[l] == "x" else at_z(v)

    def at_unit_main(l, v):
        return (z * 4 + v, y * 2 + 1) if UNIT_AXIS[l] == "x" else (v * 4 + x, y * 2 + 1)

    sums = [(zp, zo, zm, z), (xp, xo, xm, x)]
    unit_at = [(xp, xo, xm, x), (zp, zo, zm, z)]

    def at_y(v):
        return (ra_at, v * 2 + c)

    other = (ra_at, y * 2 + (1 - c))

    peers = [at_z(zp), at_z(zo), at_z(zm), at_x(xp), at_x(xo), at_x(xm), at_y(yp), at_y(ym), other]
    peers += [(z * 4 + xp, y * 2 + (1 - c)), (z * 4 + xm, y * 2 + (1 - c))]
    peers += [(zp * 4 + x, y * 2 + (1 - c)), (zm * 4 + x, y * 2 + (1 - c))]
    barrier = pltpu.get_barrier_semaphore()
    for peer in peers:
        pl.semaphore_signal(barrier, inc=1, device_id=peer, device_id_type=MESH)
    pl.semaphore_wait(barrier, len(peers))

    def arrived(dst, name):
        pltpu.make_async_remote_copy(
            src_ref=dst, dst_ref=dst, send_sem=sent.at[0], recv_sem=recv.at[SLOTS[name]],
            device_id=other, device_id_type=MESH,
        ).wait_recv()

    def d_cols(v):
        return pl.ds(pl.multiple_of(v * DB, DB), DB)

    def tile_of(v):
        return jnp.minimum(v * NJ, TILES - NJ)

    def units(v, j):
        return pl.ds(pl.multiple_of((tile_of(v) + j) * UT, UT), UT)

    def gu_half(l, j, cc, owner, what):
        return wgu.at[l, 2 * j + cc, d_cols(owner), pl.ds(what * UT, UT)]

    def relay_ref(l, j, h):
        return rel.at[l, j, h] if j < NJ else rel_d.at[l, h]

    def w_half(l, j, cc, owner, h):
        if j < NJ:
            return gu_half(l, j, cc, owner, h)
        return wd.at[l, :, cc, pl.ds(h * 64, 64), d_cols(owner)]

    def w_whole(l, j, cc, owner):
        return wgu.at[l, 2 * j + cc, d_cols(owner), :] if j < NJ else wd.at[l, :, cc, :, d_cols(owner)]

    def program(core):
        waits = []
        local_waits = {}

        def send(src, dst, name, dev):
            pltpu.make_async_remote_copy(
                src_ref=src, dst_ref=dst, send_sem=sent.at[len(waits) % N_SENT], recv_sem=recv.at[SLOTS[name]],
                device_id=dev, device_id_type=MESH,
            ).start()

        def all_sent(like):
            waits.append(
                pltpu.make_async_remote_copy(
                    src_ref=like, dst_ref=like, send_sem=sent.at[len(waits) % N_SENT], recv_sem=recv.at[0],
                    device_id=other, device_id_type=MESH,
                ).wait_send
            )

        done = []

        def wait_sent(keep):
            while len(waits) - len(done) > keep:
                waits[len(done)]()
                done.append(True)

        def stage_w(l, j):
            up, opposite, back, me = unit_at[l]
            if j < NJ:
                sources = (wg_hbm, wu_hbm)
                send(wg_hbm.at[l, :, units(opposite, j)], rel.at[l, j, 0], ("wr", l, j), at_unit(l, up))
                send(wu_hbm.at[l, :, units(opposite, j)], rel.at[l, j, 1], ("wr", l, j), at_unit(l, back))
                for what, src in enumerate(sources):
                    for to in (up, back):
                        send(
                            src.at[l, :, units(to, j)], gu_half(l, j, core, me, what), ("w", l, j), at_unit_main(l, to)
                        )
                if core == 0:
                    for what, src in enumerate(sources):
                        send(src.at[l, :, units(me, j)], gu_half(l, j, core, me, what), ("w", l, j), other)
                else:
                    mine = []
                    for what, src in enumerate(sources):
                        copy = pltpu.make_async_copy(
                            src.at[l, :, units(me, j)], gu_half(l, j, core, me, what), local.at[l * 7 + j * 2 + what]
                        )
                        copy.start()
                        mine.append(copy.wait)
                    local_waits[l, j] = mine
                all_sent(wgu.at[l, 0:4 - core, 0:DB, :])
            else:
                def src(v, h=None):
                    if h is None:
                        return wd_hbm.at[l, pl.ds(tile_of(v), NJ)]
                    return wd_hbm.at[l, pl.ds(tile_of(v), NJ), pl.ds(h * 64, 64)]

                send(src(opposite, 0), rel_d.at[l, 0], ("wr", l, j), at_unit(l, up))
                send(src(opposite, 1), rel_d.at[l, 1], ("wr", l, j), at_unit(l, back))
                send(src(up), w_whole(l, j, core, me), ("w", l, j), at_unit_main(l, up))
                send(src(back), w_whole(l, j, core, me), ("w", l, j), at_unit_main(l, back))
                if core == 0:
                    send(src(me), w_whole(l, j, core, me), ("w", l, j), other)
                else:
                    copy = pltpu.make_async_copy(src(me), w_whole(l, j, core, me), local.at[l * 7 + 6])
                    copy.start()
                    local_waits[l, j] = [copy.wait]
                all_sent(wgu.at[l, 0:4 - core, 0:NJ * UT, :])

        def stage_v(l, j):
            up, _, back, _ = unit_at[l]
            arrived(rel.at[l, j] if j < NJ else rel_d.at[l], ("wr", l, j))
            for h, (to, owner) in enumerate(((up, back), (back, up))):
                send(relay_ref(l, j, h), w_half(l, j, core, owner, h), ("w", l, j), at_unit_main(l, to))
            all_sent(wgu.at[l, 0, 0:DB if j < NJ else NJ * UT, :])

        if core == 0:
            for i, (stage, *key) in enumerate([t for t in ORDER if t[0] in "WV"]):
                if stage == "W":
                    if i:
                        pl.semaphore_wait(go, 1)
                    stage_w(*key)
                else:
                    stage_v(*key)
            copies = []
            for k in range(NC):
                rows = pl.ds(k * TC, TC)
                arrived(ov.at[rows, :], ("dd", k))
                copies.append(pltpu.make_async_copy(ov.at[rows, :], out_hbm.at[rows, :], local.at[k]))
                copies[-1].start()
            wait_sent(0)
            for copy in copies:
                copy.wait()
            return

        def weights_ready(l, j):
            for wait in local_waits[l, j]:
                wait()
            arrived(wgu.at[l, 0:2, 0:7 * DB // 2, :] if j < NJ else wgu.at[l, 0:3, 0:7 * UT, :], ("w", l, j))

        def gathered(p, k, at, rows):
            if p < LAYERS:
                return xs.at[p, k, pl.ds(pl.multiple_of(at, rows), rows), :]
            return ov.at[pl.ds(pl.multiple_of(k * TC + at, rows), rows), :]

        def part_rows(v):
            return y * YB + v * R

        in_copies = {}
        out_copies = []
        y_block = pl.ds(pl.multiple_of(y * YB, YB), YB)

        def stage_x(l, k):
            def half(h):
                rows = pl.ds(pl.multiple_of(k * TC + y * YB + h * YH, YH), YH)
                return x_hbm.at[rows, :], xs.at[0, k, pl.ds(pl.multiple_of(y * YB + h * YH, YH), YH), d_cols(x)]

            for h, name in enumerate((("xq", k), ("xg", k))):
                send(*half(h), name, at_x(xp))
                send(*half(1 - h), name, at_x(xm))
            all_sent(ov.at[0:2 * YB, :])
            rows = pl.ds(pl.multiple_of(k * TC + y * YB, YB), YB)
            in_copies[k] = pltpu.make_async_copy(x_hbm.at[rows, :], xs.at[0, k, y_block, d_cols(x)], local.at[14 + k])
            in_copies[k].start()

        def stage_s(l, k):
            arrived(ov.at[0:YB, :], ("xq", k))
            for h, (owner, to) in enumerate(((xm, xp), (xp, xm))):
                ref = xs.at[0, k, pl.ds(pl.multiple_of(y * YB + h * YH, YH), YH), d_cols(owner)]
                send(ref, ref, ("xg", k), at_x(to))
            all_sent(ov.at[0:YB, :])

        gain_copies = []

        def gains_send():
            for i, (src, axis) in enumerate(((gain_hbm, 0), (shift_hbm, 0), (gain_hbm, 1), (shift_hbm, 1))):
                me = unit_at[axis][3]
                for d in (1, 3, 2):
                    send(src, gains.at[i, me], ("gain",), at_unit(axis, turn(me, d)))
                all_sent(gains.at[i, 0:3])
                copy = pltpu.make_async_copy(src, gains.at[i, me], local.at[14 + NC + i])
                copy.start()
                gain_copies.append(copy)

        seen = set()

        def stage_a(l, k, g):
            first, last = GROUPS[l, k][g]
            if ("x", l, k) not in seen:
                seen.add(("x", l, k))
                arrived(xs.at[l, k, 0:YB, :], ("y1", k))
                arrived(xs.at[l, k, 0:YB, :], ("y2", k))
            for j in range(first, last):
                if (l, j) not in seen:
                    weights_ready(l, j)
                    seen.add((l, j))

            def tiles(j, carry):
                rhs = jnp.concatenate([wgu[l, 2 * j], wgu[l, 2 * j + 1]], axis=1)
                value = jnp.dot(xs[l, k], rhs, preferred_element_type=F32).astype(BF)
                for o in range(4):
                    for h in (0, 1):
                        at = o * ZB + h * ZH
                        part[l, k, j, o, h] = value[at:at + ZH]
                return carry

            lax.fori_loop(first, last, tiles, 0)
            js = pl.ds(first, last - first)
            up, opposite, back, _ = sums[l]
            send(part.at[l, k, js, opposite, 0], ra.at[l, k, js, 0], ("za", k, g), at_sum(l, up))
            send(part.at[l, k, js, opposite, 1], ra.at[l, k, js, 1], ("za", k, g), at_sum(l, back))
            send(part.at[l, k, js, up, 1], rb.at[l, k, js, 0], ("zc", k, g), at_sum(l, up))
            send(part.at[l, k, js, back, 0], rb.at[l, k, js, 1], ("zc", k, g), at_sum(l, back))
            all_sent(part.at[l, k, js, 0:2])

        def stage_b(l, k, g):
            first, last = GROUPS[l, k][g]
            js = pl.ds(first, last - first)
            up, _, back, _ = sums[l]
            arrived(ra.at[l, k, js], ("za", k, g))
            for h, to in enumerate((up, back)):
                for j in range(first, last):
                    part[l, k, j, to, h] = (part[l, k, j, to, h].astype(F32) + ra[l, k, j, h].astype(F32)).astype(BF)
                send(part.at[l, k, js, to, h], rc.at[l, k, js, h], ("zc", k, g), at_sum(l, to))
            all_sent(part.at[l, k, js, 0])

        def hid_ref(l, k, g, o, h):
            first, last = GROUPS[l, k][g]
            rows = pl.ds(pl.multiple_of(o * ZB + h * ZH, ZH), ZH)
            return hid.at[l, k, pl.ds(2 * first, 2 * (last - first)), rows, :]

        def stage_c(l, k, g):
            first, last = GROUPS[l, k][g]
            js = pl.ds(first, last - first)
            up, _, back, me = sums[l]
            arrived(part.at[l, k, js, 0:2], ("zc", k, g))
            for h in (0, 1):
                for j in range(first, last):
                    total = (
                        part[l, k, j, me, h].astype(F32) + rc[l, k, j, h].astype(F32) + rb[l, k, j, 1 - h].astype(F32)
                    )
                    for n in (0, 1):
                        gate, lift = total[:, n * 256:n * 256 + UT], total[:, n * 256 + UT:(n + 1) * 256]
                        value = gate * jax.nn.sigmoid(gate) * lift
                        if j < SHARED:
                            value = jnp.where(unit_at[l][3] == 3, jnp.zeros_like(value), value)
                        hid[l, k, 2 * j + n, pl.ds(pl.multiple_of(me * ZB + h * ZH, ZH), ZH), :] = value.astype(BF)
                if h == 0:
                    ref = hid_ref(l, k, g, me, 0)
                    send(ref, ref, ("h0", k, g), at_sum(l, up))
            ref = hid_ref(l, k, g, me, 1)
            send(ref, ref, ("h0", k, g), at_sum(l, back))
            send(ref, ref, ("h1", k), at_sum(l, up))
            ref = hid_ref(l, k, g, me, 0)
            send(ref, ref, ("h1", k), at_sum(l, back))
            all_sent(hid.at[l, k, pl.ds(2 * first, 2 * (last - first)), 0:4 * ZH, :])

        def stage_d(l, k, g):
            first, last = GROUPS[l, k][g]
            up, _, back, _ = sums[l]
            arrived(hid.at[l, k, pl.ds(2 * first, 2 * (last - first)), 0:2 * ZH, :], ("h0", k, g))
            for h, (owner, to) in enumerate(((back, up), (up, back))):
                ref = hid_ref(l, k, g, owner, h)
                send(ref, ref, ("h1", k), at_sum(l, to))
            all_sent(hid.at[l, k, pl.ds(2 * first, 2 * (last - first)), 0:2 * ZH, :])

        def stage_e(l, k):
            arrived(hid.at[l, k, :, 0:4 * ZH, :], ("h1", k))
            if (l, NJ) not in seen:
                weights_ready(l, NJ)
                seen.add((l, NJ))

            def columns(n, carry):
                lhs = jnp.concatenate([hid[l, k, t] for t in range(NT)], axis=1)
                cols = pl.ds(pl.multiple_of(n * 512, 512), 512)
                rhs = wd[l, :, :, :, cols].reshape(NT * UT, 512)
                value = jnp.dot(lhs, rhs, preferred_element_type=F32).astype(BF)
                for yy in range(4):
                    for h in (0, 1):
                        at = yy * YB + h * YH
                        down[l, k, yy, h, :, cols] = value[at:at + YH]
                return carry

            lax.fori_loop(0, DQ // 512, columns, 0)
            send(down.at[l, k, yo, 0], ya.at[l, k, 0], ("ya", k), at_y(yp))
            send(down.at[l, k, yo, 1], ya.at[l, k, 1], ("ya", k), at_y(ym))
            send(down.at[l, k, yp, 1], yb.at[l, k, 0], ("yc", k), at_y(yp))
            send(down.at[l, k, ym, 0], yb.at[l, k, 1], ("yc", k), at_y(ym))
            all_sent(down.at[l, k, 0:2])

        def stage_g(l, k):
            arrived(ya.at[l, k], ("ya", k))
            for h, to in enumerate((yp, ym)):
                down[l, k, to, h] = (down[l, k, to, h].astype(F32) + ya[l, k, h].astype(F32)).astype(BF)
                send(down.at[l, k, to, h], yc.at[l, k, h], ("yc", k), at_y(to))
            all_sent(down.at[l, k, 0])

        def stage_h(l, k):
            arrived(down.at[l, k, 0:2], ("yc", k))
            for h in (0, 1):
                total = down[l, k, y, h].astype(F32) + yc[l, k, h].astype(F32) + yb[l, k, 1 - h].astype(F32)
                ys[l, k, 2 * h] = total[:R].astype(BF)
                ys[l, k, 2 * h + 1] = total[R:].astype(BF)
            me = unit_at[l][3]
            for d in (2, 1, 3):
                send(ys.at[l, k, turn(me, d)], xr.at[l, k, d - 1], ("xr", k), at_unit(l, turn(me, d)))
            all_sent(ys.at[l, k, 0:3])

        def stage_i(l, k):
            me = unit_at[l][3]
            rows = pl.ds(pl.multiple_of(part_rows(me), R), R)
            value = RESIDUAL * xs[l, k, rows, :].astype(F32) + ys[l, k, me].astype(F32)
            arrived(xr.at[l, k], ("xr", k))
            for d in (1, 3, 2):
                value = value + xr[l, k, d - 1].astype(F32)
            mixed[l, k] = value
            row_sum = jnp.sum(value, axis=1, keepdims=True)
            row_squares = jnp.sum(value * value, axis=1, keepdims=True)
            lane = lax.broadcasted_iota(jnp.int32, (R, 128), 1)
            st[l, k] = jnp.where(lane == 0, row_sum, jnp.where(lane == 1, row_squares, 0.0))
            for d in (2, 1, 3):
                send(st.at[l, k], st_in.at[l, k, d - 1], ("st", k), at_sum(l, turn(sums[l][3], d)))
            all_sent(st_in.at[l, k])

        def stage_j(l, k):
            me = unit_at[l][3]
            if ("gain",) not in seen:
                seen.add(("gain",))
                arrived(gains.at[0:3], ("gain",))
                for copy in gain_copies:
                    copy.wait()
            stats = st[l, k]
            arrived(st_in.at[l, k], ("st", k))
            for d in (1, 3, 2):
                stats = stats + st_in[l, k, d - 1]
            mean = stats[:, 0:1] / D
            var = stats[:, 1:2] / D - mean * mean
            scale = lax.rsqrt(var + EPSILON)
            for q in range(4):
                cols = slice(q * DB, (q + 1) * DB)
                normed = (mixed[l, k, :, cols] - mean) * scale
                nb[l, k, q] = (normed * gains[2 * l, q, l:l + 1, :] + gains[2 * l + 1, q, l:l + 1, :]).astype(BF)

            if l + 1 < LAYERS:
                dst = xs.at[1, k, pl.ds(pl.multiple_of(part_rows(me), R), R), d_cols(z)]
            else:
                dst = gathered(LAYERS, k, part_rows(me), R)
            dst[...] = nb[l, k, me]
            if l + 1 == LAYERS and k in DIRECT:
                for dz in (2, 1, 3, 0):
                    for dy in (2, 1, 3, 0):
                        for core in (1, 0):
                            if dz + dy == 0 and core == 1:
                                continue
                            at = (turn(z, dz) * 4 + x, turn(y, dy) * 2 + core)
                            send(nb.at[1, k, turn(z, dz)], dst, ("xg", k) if core else ("dd", k), at)
                all_sent(ov.at[0:31 * R, :])
                return
            for d in (2, 1, 3):
                name = ("xq", k) if l + 1 < LAYERS else ("xg", k)
                send(nb.at[l, k, turn(me, d)], dst, name, at_unit(l, turn(me, d)))
            all_sent(nb.at[l, k, 0:3])

        def stage_q(l, k):
            arrived(nb.at[0, k, 0:3], ("xq", k))
            ref = xs.at[1, k, y_block, d_cols(z)]
            for d in (2, 1, 3):
                send(ref, ref, ("xg", k), at_z(turn(z, d)))
            all_sent(ov.at[0:3 * YB, :])

        def stage_k(l, k):
            p = l + 1
            got = (ov.at[0:2 * YB, :], ov.at[0:3 * YB, :], nb.at[1, k, 0:3])[p]
            arrived(got, ("xg", k))
            if p == 0:
                in_copies[k].wait()
            for h in (0, 1):
                ref = gathered(p, k, y * YB + h * YH, YH)
                send(ref, ref, (("y0", "y1")[h], k), at_y(yp))
                ref = gathered(p, k, y * YB + (1 - h) * YH, YH)
                send(ref, ref, (("y0", "y1")[h], k), at_y(ym))
            if p == LAYERS:
                ref = gathered(p, k, y * YB, YB)
                send(ref, ref, ("dd", k), other)
                all_sent(ov.at[0:6 * YH, :])
            else:
                all_sent(xs.at[p, k, 0:4 * YH, :])

        def stage_l(l, k):
            p = l + 1
            halves = (lambda n: xs.at[p, k, 0:n * YH, :]) if p < LAYERS else (lambda n: ov.at[0:n * YH, :])
            arrived(halves(2), ("y0", k))
            for h, (owner, to) in enumerate(((ym, yp), (yp, ym))):
                ref = gathered(p, k, owner * YB + h * YH, YH)
                send(ref, ref, ("y2", k), at_y(to))
            if p == LAYERS:
                arrived(halves(2), ("y1", k))
                for owner in (ym, yp):
                    ref = gathered(p, k, owner * YB, YB)
                    send(ref, ref, ("dd", k), other)
                all_sent(ov.at[0:6 * YH, :])
            else:
                all_sent(xs.at[p, k, 0:2 * YH, :])

        def stage_m(l, k):
            p = l + 1
            arrived(ov.at[0:YB, :], ("y2", k))
            ref = gathered(p, k, yo * YB, YB)
            send(ref, ref, ("dd", k), other)
            all_sent(ov.at[0:YB, :])
            rows = pl.ds(k * TC, TC)
            out_copies.append(pltpu.make_async_copy(ov.at[rows, :], out_hbm.at[rows, :], local.at[14 + k]))
            out_copies[-1].start()

        def stage_w_both(l, j):
            if l + j == 0:
                stage_w(l, j)
                gains_send()
                return
            pl.semaphore_signal(go, inc=1, device_id=other, device_id_type=MESH)
            stage_w(l, j)

        stages = dict(
            A=stage_a, B=stage_b, C=stage_c, D=stage_d, E=stage_e, G=stage_g, H=stage_h, I=stage_i, J=stage_j,
            K=stage_k, L=stage_l, M=stage_m, Q=stage_q, W=stage_w_both, V=stage_v, X=stage_x, S=stage_s,
        )
        for stage, *key in ORDER:
            stages[stage](*key)
            wait_sent(WAIT_LATER)
        for k in DIRECT:
            rows = pl.ds(k * TC, TC)
            arrived(ov.at[0:15 * R, :], ("xg", k))
            out_copies.append(pltpu.make_async_copy(ov.at[rows, :], out_hbm.at[rows, :], local.at[14 + k]))
            out_copies[-1].start()
        wait_sent(0)
        for copy in out_copies:
            copy.wait()

    @pl.when(c == 0)
    def _():
        program(0)

    @pl.when(c == 1)
    def _():
        program(1)


def solution(mesh):
    dma = pltpu.SemaphoreType.DMA

    def per_device(inputs, gate_weight, up_weight, down_weight, norm_gain, norm_shift):
        any_space = pl.BlockSpec(memory_space=pl.ANY)
        return pl.pallas_call(
            kernel,
            out_shape=jax.ShapeDtypeStruct((T, DB), BF),
            in_specs=[any_space] * 6,
            out_specs=any_space,
            scratch_shapes=[
                pltpu.VMEM((2, NC, TC, DQ), BF),
                pltpu.VMEM((2, NT, DQ, 2 * UT), BF),
                pltpu.VMEM((2, NJ, 2, UT, DQ), BF),
                pltpu.VMEM((2, NJ, 2, DB, UT), BF),
                pltpu.VMEM((2, 2, NJ, UT // 2, DB), BF),
                pltpu.VMEM((2, NC, NJ, 4, 2, ZH, 4 * UT), BF),
                pltpu.VMEM((2, NC, NJ, 2, ZH, 4 * UT), BF),
                pltpu.VMEM((2, NC, NJ, 2, ZH, 4 * UT), BF),
                pltpu.VMEM((2, NC, NJ, 2, ZH, 4 * UT), BF),
                pltpu.VMEM((2, NC, NT, TC, UT), BF),
                pltpu.VMEM((2, NC, 4, 2, YH, DQ), BF),
                pltpu.VMEM((2, NC, 2, YH, DQ), BF),
                pltpu.VMEM((2, NC, 2, YH, DQ), BF),
                pltpu.VMEM((2, NC, 2, YH, DQ), BF),
                pltpu.VMEM((2, NC, 4, R, DQ), BF),
                pltpu.VMEM((2, NC, 3, R, DQ), BF),
                pltpu.VMEM((2, NC, R, DQ), F32),
                pltpu.VMEM((2, NC, R, 128), F32),
                pltpu.VMEM((2, NC, 3, R, 128), F32),
                pltpu.VMEM((2, NC, 4, R, DB), BF),
                pltpu.VMEM((T, DB), BF),
                pltpu.VMEM((4, 4, 2, DB), F32),
                dma((N_SLOTS,)),
                dma((N_SENT,)),
                dma((19 + NC,)),
                pltpu.SemaphoreType.REGULAR,
            ],
            compiler_params=pltpu.CompilerParams(
                collective_id=0, has_side_effects=True, vmem_limit_bytes=63 * 1024 * 1024
            ),
        )(inputs, gate_weight, up_weight, down_weight.reshape(LAYERS, TILES, UT, DB), norm_gain, norm_shift)

    return jax.shard_map(
        per_device,
        mesh=mesh,
        in_specs=(P(None, "ra"), P(None, "ra", "cb"), P(None, "ra", "cb"), P(None, "cb", "ra"), P(None, "ra"), P(None, "ra")),
        out_specs=P(None, "ra"),
        check_vma=False,
    )
```

```python
import jax
import jax.numpy as jnp
from jax import lax
from jax.experimental import pallas as pl
from jax.experimental.pallas import tpu as pltpu
from jax.sharding import PartitionSpec as P

MESH = pl.DeviceIdType.MESH
BF = jnp.bfloat16
F32 = jnp.float32
RESIDUAL = 0.5
EPSILON = 1e-05

T, D, FF, LAYERS = 1536, 4096, 11264, 2
NC = 6
TC = T // NC
ZB = TC // 4
ZH = ZB // 2
YB = TC // 4
YH = YB // 2
R = TC // 16
DB = D // 16
DQ = D // 4
UT = 128
NJ = 3
NT = 2 * NJ
TILES = FF // 8 // UT
SHARED = 4 * NJ - TILES

GROUPS = {(l, k): [(0, 1), (1, 2), (2, 3)] if l == 0 else [(0, 1), (1, 3)] for l in range(LAYERS) for k in range(NC)}

SLOTS = {}


def slots(*names):
    for name in names:
        SLOTS.setdefault(name, len(SLOTS))


for k in range(NC):
    for g in range(max(len(GROUPS[l, k]) for l in range(LAYERS))):
        slots(("za", k, g), ("zc", k, g), ("h0", k, g))
    slots(*((m, k) for m in ("h1", "ya", "yc", "xr", "st", "xq", "xg", "y0", "y1", "y2")))
for l in range(LAYERS):
    for j in range(NJ + 1):
        slots(("wr", l, j), ("w", l, j))
slots(("gain",), *(("dd", k) for k in range(NC)))
N_SLOTS = len(SLOTS)
N_SENT = 40
WAIT_LATER = 30

SUM_AXIS, UNIT_AXIS = "zx", "xz"
DIRECT = (4, 5)
ORDER = [
    ("X", 0, 0), ("W", 0, 0), ("W", 1, 2), ("S", 0, 0), ("W", 1, 0), ("X", 0, 3), ("X", 0, 5), ("X", 0, 1),
    ("V", 0, 0), ("K", -1, 0), ("X", 0, 2), ("V", 1, 2), ("S", 0, 3), ("S", 0, 5), ("S", 0, 1), ("W", 0, 1),
    ("L", -1, 0), ("K", -1, 3), ("W", 1, 1), ("K", -1, 1), ("V", 0, 1), ("A", 0, 0, 0), ("W", 0, 2), ("L", -1, 3),
    ("K", -1, 5), ("V", 1, 1), ("L", -1, 1), ("A", 0, 0, 1), ("A", 0, 3, 1), ("L", -1, 5), ("A", 0, 3, 0),
    ("V", 0, 2), ("B", 0, 0, 0), ("S", 0, 2), ("A", 0, 1, 0), ("X", 0, 4), ("A", 0, 1, 1), ("B", 0, 3, 1),
    ("B", 0, 0, 1), ("W", 0, 3), ("B", 0, 3, 0), ("A", 0, 5, 0), ("A", 0, 3, 2), ("S", 0, 4), ("K", -1, 2),
    ("A", 0, 0, 2), ("C", 0, 3, 1), ("A", 0, 1, 2), ("B", 0, 3, 2), ("C", 0, 3, 0), ("B", 0, 0, 2), ("L", -1, 2),
    ("C", 0, 0, 0), ("V", 0, 3), ("B", 0, 1, 1), ("D", 0, 3, 1), ("A", 0, 5, 1), ("C", 0, 3, 2), ("D", 0, 3, 0),
    ("C", 0, 0, 1), ("C", 0, 0, 2), ("B", 0, 1, 0), ("A", 0, 2, 1), ("K", -1, 4), ("D", 0, 3, 2), ("B", 0, 1, 2),
    ("D", 0, 0, 0), ("A", 0, 2, 0), ("D", 0, 0, 2), ("D", 0, 0, 1), ("A", 0, 2, 2), ("B", 0, 5, 1), ("A", 0, 5, 2),
    ("C", 0, 1, 0), ("L", -1, 4), ("B", 0, 2, 1), ("E", 0, 3), ("B", 0, 5, 0), ("C", 0, 1, 1), ("E", 0, 0),
    ("C", 0, 1, 2), ("B", 0, 2, 0), ("B", 0, 2, 2), ("B", 0, 5, 2), ("A", 0, 4, 1), ("D", 0, 1, 0), ("G", 0, 3),
    ("D", 0, 1, 1), ("D", 0, 1, 2), ("C", 0, 2, 1), ("C", 0, 5, 0), ("C", 0, 2, 0), ("G", 0, 0), ("C", 0, 2, 2),
    ("A", 0, 4, 2), ("C", 0, 5, 2), ("H", 0, 3), ("C", 0, 5, 1), ("A", 0, 4, 0), ("E", 0, 1), ("D", 0, 2, 2),
    ("D", 0, 2, 1), ("H", 0, 0), ("D", 0, 2, 0), ("B", 0, 4, 2), ("B", 0, 4, 1), ("I", 0, 3), ("D", 0, 5, 0),
    ("D", 0, 5, 2), ("D", 0, 5, 1), ("B", 0, 4, 0), ("G", 0, 1), ("E", 0, 2), ("I", 0, 0), ("J", 0, 3),
    ("C", 0, 4, 1), ("E", 0, 5), ("C", 0, 4, 2), ("C", 0, 4, 0), ("H", 0, 1), ("J", 0, 0), ("G", 0, 2), ("Q", 0, 3),
    ("D", 0, 4, 1), ("D", 0, 4, 2), ("D", 0, 4, 0), ("G", 0, 5), ("I", 0, 1), ("Q", 0, 0), ("H", 0, 2), ("K", 0, 3),
    ("V", 1, 0), ("E", 0, 4), ("J", 0, 1), ("H", 0, 5), ("L", 0, 3), ("I", 0, 2), ("K", 0, 0), ("G", 0, 4),
    ("Q", 0, 1), ("I", 0, 5), ("J", 0, 2), ("A", 1, 3, 0), ("A", 1, 3, 1), ("L", 0, 0), ("K", 0, 1), ("Q", 0, 2),
    ("J", 0, 5), ("H", 0, 4), ("B", 1, 3, 0), ("B", 1, 3, 1), ("A", 1, 0, 1), ("L", 0, 1), ("Q", 0, 5),
    ("A", 1, 0, 0), ("I", 0, 4), ("W", 1, 3), ("K", 0, 2), ("C", 1, 3, 0), ("C", 1, 3, 1), ("B", 1, 0, 1),
    ("A", 1, 1, 0), ("B", 1, 0, 0), ("J", 0, 4), ("L", 0, 2), ("A", 1, 1, 1), ("K", 0, 5), ("C", 1, 0, 1),
    ("B", 1, 1, 0), ("A", 1, 2, 0), ("C", 1, 0, 0), ("Q", 0, 4), ("B", 1, 1, 1), ("D", 1, 3, 1), ("L", 0, 5),
    ("V", 1, 3), ("A", 1, 2, 1), ("K", 0, 4), ("B", 1, 2, 0), ("D", 1, 3, 0), ("D", 1, 0, 0), ("D", 1, 0, 1),
    ("C", 1, 1, 0), ("C", 1, 1, 1), ("A", 1, 5, 1), ("A", 1, 5, 0), ("B", 1, 2, 1), ("L", 0, 4), ("E", 1, 3),
    ("E", 1, 0), ("D", 1, 1, 0), ("C", 1, 2, 0), ("D", 1, 1, 1), ("B", 1, 5, 1), ("A", 1, 4, 1), ("G", 1, 3),
    ("C", 1, 2, 1), ("A", 1, 4, 0), ("B", 1, 5, 0), ("D", 1, 2, 0), ("G", 1, 0), ("E", 1, 1), ("B", 1, 4, 1),
    ("H", 1, 3), ("D", 1, 2, 1), ("B", 1, 4, 0), ("C", 1, 5, 1), ("G", 1, 1), ("C", 1, 5, 0), ("H", 1, 0),
    ("C", 1, 4, 1), ("I", 1, 3), ("E", 1, 2), ("C", 1, 4, 0), ("D", 1, 5, 1), ("D", 1, 5, 0), ("H", 1, 1),
    ("I", 1, 0), ("D", 1, 4, 1), ("D", 1, 4, 0), ("J", 1, 3), ("G", 1, 2), ("E", 1, 5), ("J", 1, 0), ("I", 1, 1),
    ("E", 1, 4), ("H", 1, 2), ("G", 1, 5), ("K", 1, 3), ("K", 1, 0), ("J", 1, 1), ("G", 1, 4), ("I", 1, 2),
    ("H", 1, 5), ("L", 1, 3), ("L", 1, 0), ("K", 1, 1), ("J", 1, 2), ("H", 1, 4), ("M", 1, 3), ("I", 1, 5),
    ("L", 1, 1), ("M", 1, 0), ("K", 1, 2), ("I", 1, 4), ("J", 1, 5), ("M", 1, 1), ("L", 1, 2), ("J", 1, 4),
    ("M", 1, 2),
]


def kernel(
    x_hbm, wg_hbm, wu_hbm, wd_hbm, gain_hbm, shift_hbm, out_hbm,
    xs, wgu, wd, rel, rel_d, part, ra, rb, rc, hid, down, ya, yb, yc, ys, xr, mixed, st, st_in, nb, ov, gains,
    recv, sent, local, go,
):
    ra_at, cb_at = lax.axis_index("ra"), lax.axis_index("cb")
    z, x = ra_at // 4, lax.rem(ra_at, 4)
    y, c = cb_at // 2, lax.rem(cb_at, 2)

    def turn(v, d):
        return lax.rem(v + d, 4)

    zp, zo, zm = turn(z, 1), turn(z, 2), turn(z, 3)
    yp, yo, ym = turn(y, 1), turn(y, 2), turn(y, 3)
    xp, xo, xm = turn(x, 1), turn(x, 2), turn(x, 3)

    def at_z(v):
        return (v * 4 + x, cb_at)

    def at_x(v):
        return (z * 4 + v, cb_at)

    def at_sum(l, v):
        return at_z(v) if SUM_AXIS[l] == "z" else at_x(v)

    def at_unit(l, v):
        return at_x(v) if UNIT_AXIS[l] == "x" else at_z(v)

    def at_unit_main(l, v):
        return (z * 4 + v, y * 2 + 1) if UNIT_AXIS[l] == "x" else (v * 4 + x, y * 2 + 1)

    sums = [(zp, zo, zm, z), (xp, xo, xm, x)]
    unit_at = [(xp, xo, xm, x), (zp, zo, zm, z)]

    def at_y(v):
        return (ra_at, v * 2 + c)

    other = (ra_at, y * 2 + (1 - c))

    peers = [at_z(zp), at_z(zm), at_x(xp), at_x(xm), at_y(yp), at_y(ym), other]
    peers += [(z * 4 + xp, y * 2 + (1 - c)), (z * 4 + xm, y * 2 + (1 - c))]
    peers += [(zp * 4 + x, y * 2 + (1 - c)), (zm * 4 + x, y * 2 + (1 - c))]
    barrier = pltpu.get_barrier_semaphore()
    for peer in peers:
        pl.semaphore_signal(barrier, inc=1, device_id=peer, device_id_type=MESH)
    pl.semaphore_wait(barrier, len(peers))

    def arrived(dst, name):
        pltpu.make_async_remote_copy(
            src_ref=dst, dst_ref=dst, send_sem=sent.at[0], recv_sem=recv.at[SLOTS[name]],
            device_id=other, device_id_type=MESH,
        ).wait_recv()

    def d_cols(v):
        return pl.ds(pl.multiple_of(v * DB, DB), DB)

    def tile_of(v):
        return jnp.minimum(v * NJ, TILES - NJ)

    def units(v, j):
        return pl.ds(pl.multiple_of((tile_of(v) + j) * UT, UT), UT)

    def gu_half(l, j, cc, owner, what):
        return wgu.at[l, 2 * j + cc, d_cols(owner), pl.ds(what * UT, UT)]

    def relay_ref(l, j, h):
        return rel.at[l, j, h] if j < NJ else rel_d.at[l, h]

    def w_half(l, j, cc, owner, h):
        if j < NJ:
            return gu_half(l, j, cc, owner, h)
        return wd.at[l, :, cc, pl.ds(h * 64, 64), d_cols(owner)]

    def w_whole(l, j, cc, owner):
        return wgu.at[l, 2 * j + cc, d_cols(owner), :] if j < NJ else wd.at[l, :, cc, :, d_cols(owner)]

    def program(core):
        waits = []
        local_waits = {}

        def send(src, dst, name, dev):
            pltpu.make_async_remote_copy(
                src_ref=src, dst_ref=dst, send_sem=sent.at[len(waits) % N_SENT], recv_sem=recv.at[SLOTS[name]],
                device_id=dev, device_id_type=MESH,
            ).start()

        def all_sent(like):
            waits.append(
                pltpu.make_async_remote_copy(
                    src_ref=like, dst_ref=like, send_sem=sent.at[len(waits) % N_SENT], recv_sem=recv.at[0],
                    device_id=other, device_id_type=MESH,
                ).wait_send
            )

        done = []

        def wait_sent(keep):
            while len(waits) - len(done) > keep:
                waits[len(done)]()
                done.append(True)

        def stage_w(l, j):
            up, opposite, back, me = unit_at[l]
            if j < NJ:
                sources = (wg_hbm, wu_hbm)
                send(wg_hbm.at[l, :, units(opposite, j)], rel.at[l, j, 0], ("wr", l, j), at_unit(l, up))
                send(wu_hbm.at[l, :, units(opposite, j)], rel.at[l, j, 1], ("wr", l, j), at_unit(l, back))
                for what, src in enumerate(sources):
                    for to in (up, back):
                        send(
                            src.at[l, :, units(to, j)], gu_half(l, j, core, me, what), ("w", l, j), at_unit_main(l, to)
                        )
                if core == 0:
                    for what, src in enumerate(sources):
                        send(src.at[l, :, units(me, j)], gu_half(l, j, core, me, what), ("w", l, j), other)
                else:
                    mine = []
                    for what, src in enumerate(sources):
                        copy = pltpu.make_async_copy(
                            src.at[l, :, units(me, j)], gu_half(l, j, core, me, what), local.at[l * 7 + j * 2 + what]
                        )
                        copy.start()
                        mine.append(copy.wait)
                    local_waits[l, j] = mine
                all_sent(wgu.at[l, 0:4 - core, 0:DB, :])
            else:
                def src(v, h=None):
                    if h is None:
                        return wd_hbm.at[l, pl.ds(tile_of(v), NJ)]
                    return wd_hbm.at[l, pl.ds(tile_of(v), NJ), pl.ds(h * 64, 64)]

                send(src(opposite, 0), rel_d.at[l, 0], ("wr", l, j), at_unit(l, up))
                send(src(opposite, 1), rel_d.at[l, 1], ("wr", l, j), at_unit(l, back))
                send(src(up), w_whole(l, j, core, me), ("w", l, j), at_unit_main(l, up))
                send(src(back), w_whole(l, j, core, me), ("w", l, j), at_unit_main(l, back))
                if core == 0:
                    send(src(me), w_whole(l, j, core, me), ("w", l, j), other)
                else:
                    copy = pltpu.make_async_copy(src(me), w_whole(l, j, core, me), local.at[l * 7 + 6])
                    copy.start()
                    local_waits[l, j] = [copy.wait]
                all_sent(wgu.at[l, 0:4 - core, 0:NJ * UT, :])

        def stage_v(l, j):
            up, _, back, _ = unit_at[l]
            arrived(rel.at[l, j] if j < NJ else rel_d.at[l], ("wr", l, j))
            for h, (to, owner) in enumerate(((up, back), (back, up))):
                send(relay_ref(l, j, h), w_half(l, j, core, owner, h), ("w", l, j), at_unit_main(l, to))
            all_sent(wgu.at[l, 0, 0:DB if j < NJ else NJ * UT, :])

        if core == 0:
            for i, (stage, *key) in enumerate([t for t in ORDER if t[0] in "WV"]):
                if stage == "W":
                    if i:
                        pl.semaphore_wait(go, 1)
                    stage_w(*key)
                else:
                    stage_v(*key)
            copies = []
            for k in range(NC):
                rows = pl.ds(k * TC, TC)
                arrived(ov.at[rows, :], ("dd", k))
                copies.append(pltpu.make_async_copy(ov.at[rows, :], out_hbm.at[rows, :], local.at[k]))
                copies[-1].start()
            wait_sent(0)
            for copy in copies:
                copy.wait()
            return

        def weights_ready(l, j):
            for wait in local_waits[l, j]:
                wait()
            arrived(wgu.at[l, 0:2, 0:7 * DB // 2, :] if j < NJ else wgu.at[l, 0:3, 0:7 * UT, :], ("w", l, j))

        def gathered(p, k, at, rows):
            if p < LAYERS:
                return xs.at[p, k, pl.ds(pl.multiple_of(at, rows), rows), :]
            return ov.at[pl.ds(pl.multiple_of(k * TC + at, rows), rows), :]

        def part_rows(v):
            return y * YB + v * R

        in_copies = {}
        out_copies = []
        y_block = pl.ds(pl.multiple_of(y * YB, YB), YB)

        def stage_x(l, k):
            def half(h):
                rows = pl.ds(pl.multiple_of(k * TC + y * YB + h * YH, YH), YH)
                return x_hbm.at[rows, :], xs.at[0, k, pl.ds(pl.multiple_of(y * YB + h * YH, YH), YH), d_cols(x)]

            for h, name in enumerate((("xq", k), ("xg", k))):
                send(*half(h), name, at_x(xp))
                send(*half(1 - h), name, at_x(xm))
            all_sent(ov.at[0:2 * YB, :])
            rows = pl.ds(pl.multiple_of(k * TC + y * YB, YB), YB)
            in_copies[k] = pltpu.make_async_copy(x_hbm.at[rows, :], xs.at[0, k, y_block, d_cols(x)], local.at[14 + k])
            in_copies[k].start()

        def stage_s(l, k):
            arrived(ov.at[0:YB, :], ("xq", k))
            for h, (owner, to) in enumerate(((xm, xp), (xp, xm))):
                ref = xs.at[0, k, pl.ds(pl.multiple_of(y * YB + h * YH, YH), YH), d_cols(owner)]
                send(ref, ref, ("xg", k), at_x(to))
            all_sent(ov.at[0:YB, :])

        gain_copies = []

        def gains_send():
            for i, (src, axis) in enumerate(((gain_hbm, 0), (shift_hbm, 0), (gain_hbm, 1), (shift_hbm, 1))):
                me = unit_at[axis][3]
                for d in (1, 3, 2):
                    send(src, gains.at[i, me], ("gain",), at_unit(axis, turn(me, d)))
                all_sent(gains.at[i, 0:3])
                copy = pltpu.make_async_copy(src, gains.at[i, me], local.at[14 + NC + i])
                copy.start()
                gain_copies.append(copy)

        seen = set()

        def stage_a(l, k, g):
            first, last = GROUPS[l, k][g]
            if ("x", l, k) not in seen:
                seen.add(("x", l, k))
                arrived(xs.at[l, k, 0:YB, :], ("y1", k))
                arrived(xs.at[l, k, 0:YB, :], ("y2", k))
            for j in range(first, last):
                if (l, j) not in seen:
                    weights_ready(l, j)
                    seen.add((l, j))

            def tiles(j, carry):
                rhs = jnp.concatenate([wgu[l, 2 * j], wgu[l, 2 * j + 1]], axis=1)
                value = jnp.dot(xs[l, k], rhs, preferred_element_type=F32).astype(BF)
                for o in range(4):
                    for h in (0, 1):
                        at = o * ZB + h * ZH
                        part[l, k, j, o, h] = value[at:at + ZH]
                return carry

            lax.fori_loop(first, last, tiles, 0)
            js = pl.ds(first, last - first)
            up, opposite, back, _ = sums[l]
            send(part.at[l, k, js, opposite, 0], ra.at[l, k, js, 0], ("za", k, g), at_sum(l, up))
            send(part.at[l, k, js, opposite, 1], ra.at[l, k, js, 1], ("za", k, g), at_sum(l, back))
            send(part.at[l, k, js, up, 1], rb.at[l, k, js, 0], ("zc", k, g), at_sum(l, up))
            send(part.at[l, k, js, back, 0], rb.at[l, k, js, 1], ("zc", k, g), at_sum(l, back))
            all_sent(part.at[l, k, js, 0:2])

        def stage_b(l, k, g):
            first, last = GROUPS[l, k][g]
            js = pl.ds(first, last - first)
            up, _, back, _ = sums[l]
            arrived(ra.at[l, k, js], ("za", k, g))
            for h, to in enumerate((up, back)):
                for j in range(first, last):
                    part[l, k, j, to, h] = (part[l, k, j, to, h].astype(F32) + ra[l, k, j, h].astype(F32)).astype(BF)
                send(part.at[l, k, js, to, h], rc.at[l, k, js, h], ("zc", k, g), at_sum(l, to))
            all_sent(part.at[l, k, js, 0])

        def hid_ref(l, k, g, o, h):
            first, last = GROUPS[l, k][g]
            rows = pl.ds(pl.multiple_of(o * ZB + h * ZH, ZH), ZH)
            return hid.at[l, k, pl.ds(2 * first, 2 * (last - first)), rows, :]

        def stage_c(l, k, g):
            first, last = GROUPS[l, k][g]
            js = pl.ds(first, last - first)
            up, _, back, me = sums[l]
            arrived(part.at[l, k, js, 0:2], ("zc", k, g))
            for h in (0, 1):
                for j in range(first, last):
                    total = (
                        part[l, k, j, me, h].astype(F32) + rc[l, k, j, h].astype(F32) + rb[l, k, j, 1 - h].astype(F32)
                    )
                    for n in (0, 1):
                        gate, lift = total[:, n * 256:n * 256 + UT], total[:, n * 256 + UT:(n + 1) * 256]
                        value = gate * jax.nn.sigmoid(gate) * lift
                        if j < SHARED:
                            value = jnp.where(unit_at[l][3] == 3, jnp.zeros_like(value), value)
                        hid[l, k, 2 * j + n, pl.ds(pl.multiple_of(me * ZB + h * ZH, ZH), ZH), :] = value.astype(BF)
                if h == 0:
                    ref = hid_ref(l, k, g, me, 0)
                    send(ref, ref, ("h0", k, g), at_sum(l, up))
            ref = hid_ref(l, k, g, me, 1)
            send(ref, ref, ("h0", k, g), at_sum(l, back))
            send(ref, ref, ("h1", k), at_sum(l, up))
            ref = hid_ref(l, k, g, me, 0)
            send(ref, ref, ("h1", k), at_sum(l, back))
            all_sent(hid.at[l, k, pl.ds(2 * first, 2 * (last - first)), 0:4 * ZH, :])

        def stage_d(l, k, g):
            first, last = GROUPS[l, k][g]
            up, _, back, _ = sums[l]
            arrived(hid.at[l, k, pl.ds(2 * first, 2 * (last - first)), 0:2 * ZH, :], ("h0", k, g))
            for h, (owner, to) in enumerate(((back, up), (up, back))):
                ref = hid_ref(l, k, g, owner, h)
                send(ref, ref, ("h1", k), at_sum(l, to))
            all_sent(hid.at[l, k, pl.ds(2 * first, 2 * (last - first)), 0:2 * ZH, :])

        def stage_e(l, k):
            arrived(hid.at[l, k, :, 0:4 * ZH, :], ("h1", k))
            if (l, NJ) not in seen:
                weights_ready(l, NJ)
                seen.add((l, NJ))

            def columns(n, carry):
                lhs = jnp.concatenate([hid[l, k, t] for t in range(NT)], axis=1)
                cols = pl.ds(pl.multiple_of(n * 512, 512), 512)
                rhs = wd[l, :, :, :, cols].reshape(NT * UT, 512)
                value = jnp.dot(lhs, rhs, preferred_element_type=F32).astype(BF)
                for yy in range(4):
                    for h in (0, 1):
                        at = yy * YB + h * YH
                        down[l, k, yy, h, :, cols] = value[at:at + YH]
                return carry

            lax.fori_loop(0, DQ // 512, columns, 0)
            send(down.at[l, k, yo, 0], ya.at[l, k, 0], ("ya", k), at_y(yp))
            send(down.at[l, k, yo, 1], ya.at[l, k, 1], ("ya", k), at_y(ym))
            send(down.at[l, k, yp, 1], yb.at[l, k, 0], ("yc", k), at_y(yp))
            send(down.at[l, k, ym, 0], yb.at[l, k, 1], ("yc", k), at_y(ym))
            all_sent(down.at[l, k, 0:2])

        def stage_g(l, k):
            arrived(ya.at[l, k], ("ya", k))
            for h, to in enumerate((yp, ym)):
                down[l, k, to, h] = (down[l, k, to, h].astype(F32) + ya[l, k, h].astype(F32)).astype(BF)
                send(down.at[l, k, to, h], yc.at[l, k, h], ("yc", k), at_y(to))
            all_sent(down.at[l, k, 0])

        def stage_h(l, k):
            arrived(down.at[l, k, 0:2], ("yc", k))
            for h in (0, 1):
                total = down[l, k, y, h].astype(F32) + yc[l, k, h].astype(F32) + yb[l, k, 1 - h].astype(F32)
                ys[l, k, 2 * h] = total[:R].astype(BF)
                ys[l, k, 2 * h + 1] = total[R:].astype(BF)
            me = unit_at[l][3]
            for d in (2, 1, 3):
                send(ys.at[l, k, turn(me, d)], xr.at[l, k, d - 1], ("xr", k), at_unit(l, turn(me, d)))
            all_sent(ys.at[l, k, 0:3])

        def stage_i(l, k):
            me = unit_at[l][3]
            rows = pl.ds(pl.multiple_of(part_rows(me), R), R)
            value = RESIDUAL * xs[l, k, rows, :].astype(F32) + ys[l, k, me].astype(F32)
            arrived(xr.at[l, k], ("xr", k))
            for d in (1, 3, 2):
                value = value + xr[l, k, d - 1].astype(F32)
            mixed[l, k] = value
            row_sum = jnp.sum(value, axis=1, keepdims=True)
            row_squares = jnp.sum(value * value, axis=1, keepdims=True)
            lane = lax.broadcasted_iota(jnp.int32, (R, 128), 1)
            st[l, k] = jnp.where(lane == 0, row_sum, jnp.where(lane == 1, row_squares, 0.0))
            for d in (2, 1, 3):
                send(st.at[l, k], st_in.at[l, k, d - 1], ("st", k), at_sum(l, turn(sums[l][3], d)))
            all_sent(st_in.at[l, k])

        def stage_j(l, k):
            me = unit_at[l][3]
            if ("gain",) not in seen:
                seen.add(("gain",))
                arrived(gains.at[0:3], ("gain",))
                for copy in gain_copies:
                    copy.wait()
            stats = st[l, k]
            arrived(st_in.at[l, k], ("st", k))
            for d in (1, 3, 2):
                stats = stats + st_in[l, k, d - 1]
            mean = stats[:, 0:1] / D
            var = stats[:, 1:2] / D - mean * mean
            scale = lax.rsqrt(var + EPSILON)
            for q in range(4):
                cols = slice(q * DB, (q + 1) * DB)
                normed = (mixed[l, k, :, cols] - mean) * scale
                nb[l, k, q] = (normed * gains[2 * l, q, l:l + 1, :] + gains[2 * l + 1, q, l:l + 1, :]).astype(BF)

            if l + 1 < LAYERS:
                dst = xs.at[1, k, pl.ds(pl.multiple_of(part_rows(me), R), R), d_cols(z)]
            else:
                dst = gathered(LAYERS, k, part_rows(me), R)
            dst[...] = nb[l, k, me]
            if l + 1 == LAYERS and k in DIRECT:
                for dz in (2, 1, 3, 0):
                    for dy in (2, 1, 3, 0):
                        for core in (1, 0):
                            if dz + dy == 0 and core == 1:
                                continue
                            at = (turn(z, dz) * 4 + x, turn(y, dy) * 2 + core)
                            send(nb.at[1, k, turn(z, dz)], dst, ("xg", k) if core else ("dd", k), at)
                all_sent(ov.at[0:31 * R, :])
                return
            for d in (2, 1, 3):
                name = ("xq", k) if l + 1 < LAYERS else ("xg", k)
                send(nb.at[l, k, turn(me, d)], dst, name, at_unit(l, turn(me, d)))
            all_sent(nb.at[l, k, 0:3])

        def stage_q(l, k):
            arrived(nb.at[0, k, 0:3], ("xq", k))
            ref = xs.at[1, k, y_block, d_cols(z)]
            for d in (2, 1, 3):
                send(ref, ref, ("xg", k), at_z(turn(z, d)))
            all_sent(ov.at[0:3 * YB, :])

        def stage_k(l, k):
            p = l + 1
            got = (ov.at[0:2 * YB, :], ov.at[0:3 * YB, :], nb.at[1, k, 0:3])[p]
            arrived(got, ("xg", k))
            if p == 0:
                in_copies[k].wait()
            for h in (0, 1):
                ref = gathered(p, k, y * YB + h * YH, YH)
                send(ref, ref, (("y0", "y1")[h], k), at_y(yp))
                ref = gathered(p, k, y * YB + (1 - h) * YH, YH)
                send(ref, ref, (("y0", "y1")[h], k), at_y(ym))
            if p == LAYERS:
                ref = gathered(p, k, y * YB, YB)
                send(ref, ref, ("dd", k), other)
                all_sent(ov.at[0:6 * YH, :])
            else:
                all_sent(xs.at[p, k, 0:4 * YH, :])

        def stage_l(l, k):
            p = l + 1
            halves = (lambda n: xs.at[p, k, 0:n * YH, :]) if p < LAYERS else (lambda n: ov.at[0:n * YH, :])
            arrived(halves(2), ("y0", k))
            for h, (owner, to) in enumerate(((ym, yp), (yp, ym))):
                ref = gathered(p, k, owner * YB + h * YH, YH)
                send(ref, ref, ("y2", k), at_y(to))
            if p == LAYERS:
                arrived(halves(2), ("y1", k))
                for owner in (ym, yp):
                    ref = gathered(p, k, owner * YB, YB)
                    send(ref, ref, ("dd", k), other)
                all_sent(ov.at[0:6 * YH, :])
            else:
                all_sent(xs.at[p, k, 0:2 * YH, :])

        def stage_m(l, k):
            p = l + 1
            arrived(ov.at[0:YB, :], ("y2", k))
            ref = gathered(p, k, yo * YB, YB)
            send(ref, ref, ("dd", k), other)
            all_sent(ov.at[0:YB, :])
            rows = pl.ds(k * TC, TC)
            out_copies.append(pltpu.make_async_copy(ov.at[rows, :], out_hbm.at[rows, :], local.at[14 + k]))
            out_copies[-1].start()

        def stage_w_both(l, j):
            if l + j == 0:
                stage_w(l, j)
                return
            pl.semaphore_signal(go, inc=1, device_id=other, device_id_type=MESH)
            stage_w(l, j)

        stages = dict(
            A=stage_a, B=stage_b, C=stage_c, D=stage_d, E=stage_e, G=stage_g, H=stage_h, I=stage_i, J=stage_j,
            K=stage_k, L=stage_l, M=stage_m, Q=stage_q, W=stage_w_both, V=stage_v, X=stage_x, S=stage_s,
        )
        for stage, *key in ORDER:
            stages[stage](*key)
            if stage == "C" and not gain_copies:
                gains_send()
            wait_sent(WAIT_LATER)
        for k in DIRECT:
            rows = pl.ds(k * TC, TC)
            arrived(ov.at[0:15 * R, :], ("xg", k))
            out_copies.append(pltpu.make_async_copy(ov.at[rows, :], out_hbm.at[rows, :], local.at[14 + k]))
            out_copies[-1].start()
        wait_sent(0)
        for copy in out_copies:
            copy.wait()

    @pl.when(c == 0)
    def _():
        program(0)

    @pl.when(c == 1)
    def _():
        program(1)


def solution(mesh):
    dma = pltpu.SemaphoreType.DMA

    def per_device(inputs, gate_weight, up_weight, down_weight, norm_gain, norm_shift):
        any_space = pl.BlockSpec(memory_space=pl.ANY)
        return pl.pallas_call(
            kernel,
            out_shape=jax.ShapeDtypeStruct((T, DB), BF),
            in_specs=[any_space] * 6,
            out_specs=any_space,
            scratch_shapes=[
                pltpu.VMEM((2, NC, TC, DQ), BF),
                pltpu.VMEM((2, NT, DQ, 2 * UT), BF),
                pltpu.VMEM((2, NJ, 2, UT, DQ), BF),
                pltpu.VMEM((2, NJ, 2, DB, UT), BF),
                pltpu.VMEM((2, 2, NJ, UT // 2, DB), BF),
                pltpu.VMEM((2, NC, NJ, 4, 2, ZH, 4 * UT), BF),
                pltpu.VMEM((2, NC, NJ, 2, ZH, 4 * UT), BF),
                pltpu.VMEM((2, NC, NJ, 2, ZH, 4 * UT), BF),
                pltpu.VMEM((2, NC, NJ, 2, ZH, 4 * UT), BF),
                pltpu.VMEM((2, NC, NT, TC, UT), BF),
                pltpu.VMEM((2, NC, 4, 2, YH, DQ), BF),
                pltpu.VMEM((2, NC, 2, YH, DQ), BF),
                pltpu.VMEM((2, NC, 2, YH, DQ), BF),
                pltpu.VMEM((2, NC, 2, YH, DQ), BF),
                pltpu.VMEM((2, NC, 4, R, DQ), BF),
                pltpu.VMEM((2, NC, 3, R, DQ), BF),
                pltpu.VMEM((2, NC, R, DQ), F32),
                pltpu.VMEM((2, NC, R, 128), F32),
                pltpu.VMEM((2, NC, 3, R, 128), F32),
                pltpu.VMEM((2, NC, 4, R, DB), BF),
                pltpu.VMEM((T, DB), BF),
                pltpu.VMEM((4, 4, 2, DB), F32),
                dma((N_SLOTS,)),
                dma((N_SENT,)),
                dma((19 + NC,)),
                pltpu.SemaphoreType.REGULAR,
            ],
            compiler_params=pltpu.CompilerParams(
                collective_id=0, has_side_effects=True, vmem_limit_bytes=63 * 1024 * 1024
            ),
        )(inputs, gate_weight, up_weight, down_weight.reshape(LAYERS, TILES, UT, DB), norm_gain, norm_shift)

    return jax.shard_map(
        per_device,
        mesh=mesh,
        in_specs=(P(None, "ra"), P(None, "ra", "cb"), P(None, "ra", "cb"), P(None, "cb", "ra"), P(None, "ra"), P(None, "ra")),
        out_specs=P(None, "ra"),
        check_vma=False,
    )
```

```python
import jax
import jax.numpy as jnp
from jax import lax
from jax.experimental import pallas as pl
from jax.experimental.pallas import tpu as pltpu
from jax.sharding import PartitionSpec as P

MESH = pl.DeviceIdType.MESH
BF = jnp.bfloat16
F32 = jnp.float32
RESIDUAL = 0.5
EPSILON = 1e-05

T, D, FF, LAYERS = 1536, 4096, 11264, 2
NC = 6
TC = T // NC
ZB = TC // 4
ZH = ZB // 2
YB = TC // 4
YH = YB // 2
R = TC // 16
DB = D // 16
DQ = D // 4
UT = 128
NJ = 3
NT = 2 * NJ
TILES = FF // 8 // UT
SHARED = 4 * NJ - TILES

GROUPS = {(l, k): [(0, 1), (1, 2), (2, 3)] if l == 0 else [(0, 1), (1, 3)] for l in range(LAYERS) for k in range(NC)}

SLOTS = {}


def slots(*names):
    for name in names:
        SLOTS.setdefault(name, len(SLOTS))


for k in range(NC):
    for g in range(max(len(GROUPS[l, k]) for l in range(LAYERS))):
        slots(("za", k, g), ("zc", k, g), ("h0", k, g))
    slots(*((m, k) for m in ("h1", "ya", "yc", "xr", "st", "xq", "xg", "y0", "y1", "y2")))
for l in range(LAYERS):
    for j in range(NJ + 1):
        slots(("wr", l, j), ("w", l, j))
slots(("gain",), *(("dd", k) for k in range(NC)))
N_SLOTS = len(SLOTS)
N_SENT = 40
WAIT_LATER = 30

SUM_AXIS, UNIT_AXIS = "zx", "xz"
DIRECT = (4, 5)
ORDER = [
    ("X", 0, 0), ("W", 0, 0), ("W", 1, 2), ("W", 1, 1), ("X", 0, 3), ("S", 0, 0), ("X", 0, 1), ("V", 0, 0),
    ("S", 0, 3), ("X", 0, 2), ("S", 0, 1), ("K", -1, 0), ("W", 0, 1), ("K", -1, 3), ("S", 0, 2), ("W", 1, 0),
    ("K", -1, 1), ("V", 0, 1), ("X", 0, 5), ("L", -1, 0), ("L", -1, 3), ("L", -1, 1), ("W", 0, 2), ("V", 1, 0),
    ("K", -1, 2), ("A", 0, 0, 0), ("A", 0, 3, 0), ("A", 0, 3, 1), ("A", 0, 0, 1), ("L", -1, 2), ("V", 0, 2),
    ("S", 0, 5), ("A", 0, 1, 1), ("B", 0, 3, 0), ("B", 0, 0, 0), ("A", 0, 1, 0), ("X", 0, 4), ("B", 0, 3, 1),
    ("W", 0, 3), ("A", 0, 2, 1), ("A", 0, 2, 0), ("A", 0, 2, 2), ("K", -1, 5), ("A", 0, 3, 2), ("B", 0, 2, 1),
    ("S", 0, 4), ("A", 0, 1, 2), ("B", 0, 2, 0), ("B", 0, 2, 2), ("C", 0, 3, 1), ("B", 0, 3, 2), ("C", 0, 3, 0),
    ("L", -1, 5), ("B", 0, 1, 1), ("C", 0, 2, 1), ("V", 0, 3), ("B", 0, 1, 2), ("C", 0, 2, 0), ("C", 0, 2, 2),
    ("B", 0, 1, 0), ("C", 0, 3, 2), ("A", 0, 0, 2), ("C", 0, 1, 1), ("D", 0, 2, 1), ("K", -1, 4), ("D", 0, 2, 0),
    ("D", 0, 2, 2), ("C", 0, 1, 2), ("D", 0, 3, 0), ("D", 0, 3, 1), ("C", 0, 1, 0), ("D", 0, 3, 2), ("A", 0, 5, 1),
    ("B", 0, 0, 1), ("B", 0, 0, 2), ("A", 0, 5, 0), ("L", -1, 4), ("D", 0, 1, 1), ("E", 0, 2), ("A", 0, 5, 2),
    ("D", 0, 1, 2), ("E", 0, 3), ("C", 0, 0, 0), ("D", 0, 1, 0), ("C", 0, 0, 1), ("A", 0, 4, 2), ("A", 0, 4, 1),
    ("G", 0, 2), ("B", 0, 5, 1), ("C", 0, 0, 2), ("A", 0, 4, 0), ("B", 0, 5, 2), ("G", 0, 3), ("E", 0, 1),
    ("B", 0, 5, 0), ("B", 0, 4, 2), ("B", 0, 4, 1), ("H", 0, 2), ("D", 0, 0, 2), ("D", 0, 0, 0), ("D", 0, 0, 1),
    ("B", 0, 4, 0), ("C", 0, 5, 1), ("C", 0, 5, 2), ("H", 0, 3), ("G", 0, 1), ("C", 0, 5, 0), ("C", 0, 4, 2),
    ("C", 0, 4, 1), ("I", 0, 2), ("E", 0, 0), ("C", 0, 4, 0), ("D", 0, 5, 2), ("D", 0, 5, 1), ("D", 0, 5, 0),
    ("I", 0, 3), ("D", 0, 4, 1), ("J", 0, 2), ("H", 0, 1), ("D", 0, 4, 2), ("D", 0, 4, 0), ("G", 0, 0), ("V", 1, 2),
    ("E", 0, 5), ("J", 0, 3), ("Q", 0, 2), ("E", 0, 4), ("I", 0, 1), ("Q", 0, 3), ("H", 0, 0), ("G", 0, 5),
    ("K", 0, 2), ("J", 0, 1), ("V", 1, 1), ("G", 0, 4), ("K", 0, 3), ("H", 0, 5), ("I", 0, 0), ("Q", 0, 1),
    ("L", 0, 2), ("H", 0, 4), ("L", 0, 3), ("J", 0, 0), ("I", 0, 5), ("K", 0, 1), ("A", 1, 2, 0), ("A", 1, 2, 1),
    ("I", 0, 4), ("Q", 0, 0), ("J", 0, 5), ("A", 1, 3, 1), ("L", 0, 1), ("J", 0, 4), ("B", 1, 2, 0), ("A", 1, 3, 0),
    ("B", 1, 2, 1), ("K", 0, 0), ("B", 1, 3, 1), ("Q", 0, 5), ("A", 1, 1, 1), ("Q", 0, 4), ("C", 1, 2, 0),
    ("L", 0, 0), ("W", 1, 3), ("A", 1, 1, 0), ("C", 1, 3, 1), ("B", 1, 3, 0), ("K", 0, 4), ("C", 1, 2, 1),
    ("B", 1, 1, 1), ("A", 1, 0, 1), ("D", 1, 3, 1), ("L", 0, 4), ("V", 1, 3), ("B", 1, 1, 0), ("C", 1, 3, 0),
    ("K", 0, 5), ("D", 1, 2, 0), ("A", 1, 0, 0), ("B", 1, 0, 1), ("D", 1, 2, 1), ("C", 1, 1, 0), ("C", 1, 1, 1),
    ("L", 0, 5), ("D", 1, 3, 0), ("A", 1, 4, 0), ("B", 1, 0, 0), ("A", 1, 4, 1), ("E", 1, 2), ("C", 1, 0, 1),
    ("E", 1, 3), ("D", 1, 1, 1), ("D", 1, 1, 0), ("B", 1, 4, 0), ("C", 1, 0, 0), ("A", 1, 5, 1), ("G", 1, 2),
    ("A", 1, 5, 0), ("G", 1, 3), ("B", 1, 4, 1), ("E", 1, 1), ("D", 1, 0, 0), ("B", 1, 5, 1), ("D", 1, 0, 1),
    ("H", 1, 2), ("B", 1, 5, 0), ("C", 1, 4, 0), ("H", 1, 3), ("C", 1, 4, 1), ("C", 1, 5, 1), ("G", 1, 1),
    ("E", 1, 0), ("C", 1, 5, 0), ("D", 1, 4, 0), ("D", 1, 4, 1), ("I", 1, 3), ("I", 1, 2), ("D", 1, 5, 1),
    ("D", 1, 5, 0), ("H", 1, 1), ("G", 1, 0), ("E", 1, 4), ("J", 1, 3), ("J", 1, 2), ("E", 1, 5), ("H", 1, 0),
    ("I", 1, 1), ("G", 1, 4), ("K", 1, 3), ("K", 1, 2), ("J", 1, 1), ("G", 1, 5), ("I", 1, 0), ("H", 1, 4),
    ("L", 1, 3), ("L", 1, 2), ("K", 1, 1), ("J", 1, 0), ("H", 1, 5), ("I", 1, 4), ("L", 1, 1), ("M", 1, 3),
    ("M", 1, 2), ("K", 1, 0), ("I", 1, 5), ("J", 1, 4), ("M", 1, 1), ("L", 1, 0), ("J", 1, 5), ("M", 1, 0),
]


def kernel(
    x_hbm, wg_hbm, wu_hbm, wd_hbm, gain_hbm, shift_hbm, out_hbm,
    xs, wgu, wd, rel, rel_d, part, ra, rb, rc, hid, down, ya, yb, yc, ys, xr, mixed, st, st_in, nb, ov, gains,
    recv, sent, local, go,
):
    ra_at, cb_at = lax.axis_index("ra"), lax.axis_index("cb")
    z, x = ra_at // 4, lax.rem(ra_at, 4)
    y, c = cb_at // 2, lax.rem(cb_at, 2)

    def turn(v, d):
        return lax.rem(v + d, 4)

    zp, zo, zm = turn(z, 1), turn(z, 2), turn(z, 3)
    yp, yo, ym = turn(y, 1), turn(y, 2), turn(y, 3)
    xp, xo, xm = turn(x, 1), turn(x, 2), turn(x, 3)

    def at_z(v):
        return (v * 4 + x, cb_at)

    def at_x(v):
        return (z * 4 + v, cb_at)

    def at_sum(l, v):
        return at_z(v) if SUM_AXIS[l] == "z" else at_x(v)

    def at_unit(l, v):
        return at_x(v) if UNIT_AXIS[l] == "x" else at_z(v)

    def at_unit_main(l, v):
        return (z * 4 + v, y * 2 + 1) if UNIT_AXIS[l] == "x" else (v * 4 + x, y * 2 + 1)

    sums = [(zp, zo, zm, z), (xp, xo, xm, x)]
    unit_at = [(xp, xo, xm, x), (zp, zo, zm, z)]

    def at_y(v):
        return (ra_at, v * 2 + c)

    other = (ra_at, y * 2 + (1 - c))

    peers = [at_z(zp), at_z(zm), at_x(xp), at_x(xm), at_y(yp), at_y(ym), other]
    peers += [(z * 4 + xp, y * 2 + (1 - c)), (z * 4 + xm, y * 2 + (1 - c))]
    peers += [(zp * 4 + x, y * 2 + (1 - c)), (zm * 4 + x, y * 2 + (1 - c))]
    barrier = pltpu.get_barrier_semaphore()
    for peer in peers:
        pl.semaphore_signal(barrier, inc=1, device_id=peer, device_id_type=MESH)
    pl.semaphore_wait(barrier, len(peers))

    def arrived(dst, name):
        pltpu.make_async_remote_copy(
            src_ref=dst, dst_ref=dst, send_sem=sent.at[0], recv_sem=recv.at[SLOTS[name]],
            device_id=other, device_id_type=MESH,
        ).wait_recv()

    def d_cols(v):
        return pl.ds(pl.multiple_of(v * DB, DB), DB)

    def tile_of(v):
        return jnp.minimum(v * NJ, TILES - NJ)

    def units(v, j):
        return pl.ds(pl.multiple_of((tile_of(v) + j) * UT, UT), UT)

    def gu_half(l, j, cc, owner, what):
        return wgu.at[l, 2 * j + cc, d_cols(owner), pl.ds(what * UT, UT)]

    def relay_ref(l, j, h):
        return rel.at[l, j, h] if j < NJ else rel_d.at[l, h]

    def w_half(l, j, cc, owner, h):
        if j < NJ:
            return gu_half(l, j, cc, owner, h)
        return wd.at[l, :, cc, pl.ds(h * 64, 64), d_cols(owner)]

    def w_whole(l, j, cc, owner):
        return wgu.at[l, 2 * j + cc, d_cols(owner), :] if j < NJ else wd.at[l, :, cc, :, d_cols(owner)]

    def program(core):
        waits = []
        local_waits = {}

        def send(src, dst, name, dev):
            pltpu.make_async_remote_copy(
                src_ref=src, dst_ref=dst, send_sem=sent.at[len(waits) % N_SENT], recv_sem=recv.at[SLOTS[name]],
                device_id=dev, device_id_type=MESH,
            ).start()

        def all_sent(like):
            waits.append(
                pltpu.make_async_remote_copy(
                    src_ref=like, dst_ref=like, send_sem=sent.at[len(waits) % N_SENT], recv_sem=recv.at[0],
                    device_id=other, device_id_type=MESH,
                ).wait_send
            )

        done = []

        def wait_sent(keep):
            while len(waits) - len(done) > keep:
                waits[len(done)]()
                done.append(True)

        def stage_w(l, j):
            up, opposite, back, me = unit_at[l]
            if j < NJ:
                sources = (wg_hbm, wu_hbm)
                send(wg_hbm.at[l, :, units(opposite, j)], rel.at[l, j, 0], ("wr", l, j), at_unit(l, up))
                send(wu_hbm.at[l, :, units(opposite, j)], rel.at[l, j, 1], ("wr", l, j), at_unit(l, back))
                for what, src in enumerate(sources):
                    for to in (up, back):
                        send(
                            src.at[l, :, units(to, j)], gu_half(l, j, core, me, what), ("w", l, j), at_unit_main(l, to)
                        )
                if core == 0:
                    for what, src in enumerate(sources):
                        send(src.at[l, :, units(me, j)], gu_half(l, j, core, me, what), ("w", l, j), other)
                else:
                    mine = []
                    for what, src in enumerate(sources):
                        copy = pltpu.make_async_copy(
                            src.at[l, :, units(me, j)], gu_half(l, j, core, me, what), local.at[l * 7 + j * 2 + what]
                        )
                        copy.start()
                        mine.append(copy.wait)
                    local_waits[l, j] = mine
                all_sent(wgu.at[l, 0:4 - core, 0:DB, :])
            else:
                def src(v, h=None):
                    if h is None:
                        return wd_hbm.at[l, pl.ds(tile_of(v), NJ)]
                    return wd_hbm.at[l, pl.ds(tile_of(v), NJ), pl.ds(h * 64, 64)]

                send(src(opposite, 0), rel_d.at[l, 0], ("wr", l, j), at_unit(l, up))
                send(src(opposite, 1), rel_d.at[l, 1], ("wr", l, j), at_unit(l, back))
                send(src(up), w_whole(l, j, core, me), ("w", l, j), at_unit_main(l, up))
                send(src(back), w_whole(l, j, core, me), ("w", l, j), at_unit_main(l, back))
                if core == 0:
                    send(src(me), w_whole(l, j, core, me), ("w", l, j), other)
                else:
                    copy = pltpu.make_async_copy(src(me), w_whole(l, j, core, me), local.at[l * 7 + 6])
                    copy.start()
                    local_waits[l, j] = [copy.wait]
                all_sent(wgu.at[l, 0:4 - core, 0:NJ * UT, :])

        def stage_v(l, j):
            up, _, back, _ = unit_at[l]
            arrived(rel.at[l, j] if j < NJ else rel_d.at[l], ("wr", l, j))
            for h, (to, owner) in enumerate(((up, back), (back, up))):
                send(relay_ref(l, j, h), w_half(l, j, core, owner, h), ("w", l, j), at_unit_main(l, to))
            all_sent(wgu.at[l, 0, 0:DB if j < NJ else NJ * UT, :])

        if core == 0:
            for i, (stage, *key) in enumerate([t for t in ORDER if t[0] in "WV"]):
                if stage == "W":
                    if i:
                        pl.semaphore_wait(go, 1)
                    stage_w(*key)
                else:
                    stage_v(*key)
            copies = []
            for k in range(NC):
                rows = pl.ds(k * TC, TC)
                arrived(ov.at[rows, :], ("dd", k))
                copies.append(pltpu.make_async_copy(ov.at[rows, :], out_hbm.at[rows, :], local.at[k]))
                copies[-1].start()
            wait_sent(0)
            for copy in copies:
                copy.wait()
            return

        def weights_ready(l, j):
            for wait in local_waits[l, j]:
                wait()
            arrived(wgu.at[l, 0:2, 0:7 * DB // 2, :] if j < NJ else wgu.at[l, 0:3, 0:7 * UT, :], ("w", l, j))

        def gathered(p, k, at, rows):
            if p < LAYERS:
                return xs.at[p, k, pl.ds(pl.multiple_of(at, rows), rows), :]
            return ov.at[pl.ds(pl.multiple_of(k * TC + at, rows), rows), :]

        def part_rows(v):
            return y * YB + v * R

        in_copies = {}
        out_copies = []
        y_block = pl.ds(pl.multiple_of(y * YB, YB), YB)

        def stage_x(l, k):
            def half(h):
                rows = pl.ds(pl.multiple_of(k * TC + y * YB + h * YH, YH), YH)
                return x_hbm.at[rows, :], xs.at[0, k, pl.ds(pl.multiple_of(y * YB + h * YH, YH), YH), d_cols(x)]

            for h, name in enumerate((("xq", k), ("xg", k))):
                send(*half(h), name, at_x(xp))
                send(*half(1 - h), name, at_x(xm))
            all_sent(ov.at[0:2 * YB, :])
            rows = pl.ds(pl.multiple_of(k * TC + y * YB, YB), YB)
            in_copies[k] = pltpu.make_async_copy(x_hbm.at[rows, :], xs.at[0, k, y_block, d_cols(x)], local.at[14 + k])
            in_copies[k].start()

        def stage_s(l, k):
            arrived(ov.at[0:YB, :], ("xq", k))
            for h, (owner, to) in enumerate(((xm, xp), (xp, xm))):
                ref = xs.at[0, k, pl.ds(pl.multiple_of(y * YB + h * YH, YH), YH), d_cols(owner)]
                send(ref, ref, ("xg", k), at_x(to))
            all_sent(ov.at[0:YB, :])

        gain_copies = []

        def gains_send():
            for i, (src, axis) in enumerate(((gain_hbm, 0), (shift_hbm, 0), (gain_hbm, 1), (shift_hbm, 1))):
                me = unit_at[axis][3]
                for d in (1, 3, 2):
                    send(src, gains.at[i, me], ("gain",), at_unit(axis, turn(me, d)))
                all_sent(gains.at[i, 0:3])
                copy = pltpu.make_async_copy(src, gains.at[i, me], local.at[14 + NC + i])
                copy.start()
                gain_copies.append(copy)

        seen = set()

        def stage_a(l, k, g):
            first, last = GROUPS[l, k][g]
            if ("x", l, k) not in seen:
                seen.add(("x", l, k))
                arrived(xs.at[l, k, 0:YB, :], ("y1", k))
                arrived(xs.at[l, k, 0:YB, :], ("y2", k))
            for j in range(first, last):
                if (l, j) not in seen:
                    weights_ready(l, j)
                    seen.add((l, j))

            def tiles(j, carry):
                rhs = jnp.concatenate([wgu[l, 2 * j], wgu[l, 2 * j + 1]], axis=1)
                value = jnp.dot(xs[l, k], rhs, preferred_element_type=F32).astype(BF)
                for o in range(4):
                    for h in (0, 1):
                        at = o * ZB + h * ZH
                        part[l, k, j, o, h] = value[at:at + ZH]
                return carry

            lax.fori_loop(first, last, tiles, 0)
            js = pl.ds(first, last - first)
            up, opposite, back, _ = sums[l]
            send(part.at[l, k, js, opposite, 0], ra.at[l, k, js, 0], ("za", k, g), at_sum(l, up))
            send(part.at[l, k, js, opposite, 1], ra.at[l, k, js, 1], ("za", k, g), at_sum(l, back))
            send(part.at[l, k, js, up, 1], rb.at[l, k, js, 0], ("zc", k, g), at_sum(l, up))
            send(part.at[l, k, js, back, 0], rb.at[l, k, js, 1], ("zc", k, g), at_sum(l, back))
            all_sent(part.at[l, k, js, 0:2])

        def stage_b(l, k, g):
            first, last = GROUPS[l, k][g]
            js = pl.ds(first, last - first)
            up, _, back, _ = sums[l]
            arrived(ra.at[l, k, js], ("za", k, g))
            for h, to in enumerate((up, back)):
                for j in range(first, last):
                    part[l, k, j, to, h] = (part[l, k, j, to, h].astype(F32) + ra[l, k, j, h].astype(F32)).astype(BF)
                send(part.at[l, k, js, to, h], rc.at[l, k, js, h], ("zc", k, g), at_sum(l, to))
            all_sent(part.at[l, k, js, 0])

        def hid_ref(l, k, g, o, h):
            first, last = GROUPS[l, k][g]
            rows = pl.ds(pl.multiple_of(o * ZB + h * ZH, ZH), ZH)
            return hid.at[l, k, pl.ds(2 * first, 2 * (last - first)), rows, :]

        def stage_c(l, k, g):
            first, last = GROUPS[l, k][g]
            js = pl.ds(first, last - first)
            up, _, back, me = sums[l]
            arrived(part.at[l, k, js, 0:2], ("zc", k, g))
            for h in (0, 1):
                for j in range(first, last):
                    total = (
                        part[l, k, j, me, h].astype(F32) + rc[l, k, j, h].astype(F32) + rb[l, k, j, 1 - h].astype(F32)
                    )
                    for n in (0, 1):
                        gate, lift = total[:, n * 256:n * 256 + UT], total[:, n * 256 + UT:(n + 1) * 256]
                        value = gate * jax.nn.sigmoid(gate) * lift
                        if j < SHARED:
                            value = jnp.where(unit_at[l][3] == 3, jnp.zeros_like(value), value)
                        hid[l, k, 2 * j + n, pl.ds(pl.multiple_of(me * ZB + h * ZH, ZH), ZH), :] = value.astype(BF)
                if h == 0:
                    ref = hid_ref(l, k, g, me, 0)
                    send(ref, ref, ("h0", k, g), at_sum(l, up))
            ref = hid_ref(l, k, g, me, 1)
            send(ref, ref, ("h0", k, g), at_sum(l, back))
            send(ref, ref, ("h1", k), at_sum(l, up))
            ref = hid_ref(l, k, g, me, 0)
            send(ref, ref, ("h1", k), at_sum(l, back))
            all_sent(hid.at[l, k, pl.ds(2 * first, 2 * (last - first)), 0:4 * ZH, :])

        def stage_d(l, k, g):
            first, last = GROUPS[l, k][g]
            up, _, back, _ = sums[l]
            arrived(hid.at[l, k, pl.ds(2 * first, 2 * (last - first)), 0:2 * ZH, :], ("h0", k, g))
            for h, (owner, to) in enumerate(((back, up), (up, back))):
                ref = hid_ref(l, k, g, owner, h)
                send(ref, ref, ("h1", k), at_sum(l, to))
            all_sent(hid.at[l, k, pl.ds(2 * first, 2 * (last - first)), 0:2 * ZH, :])

        def stage_e(l, k):
            arrived(hid.at[l, k, :, 0:4 * ZH, :], ("h1", k))
            if (l, NJ) not in seen:
                weights_ready(l, NJ)
                seen.add((l, NJ))

            def columns(n, carry):
                lhs = jnp.concatenate([hid[l, k, t] for t in range(NT)], axis=1)
                cols = pl.ds(pl.multiple_of(n * 512, 512), 512)
                rhs = wd[l, :, :, :, cols].reshape(NT * UT, 512)
                value = jnp.dot(lhs, rhs, preferred_element_type=F32).astype(BF)
                for yy in range(4):
                    for h in (0, 1):
                        at = yy * YB + h * YH
                        down[l, k, yy, h, :, cols] = value[at:at + YH]
                return carry

            lax.fori_loop(0, DQ // 512, columns, 0)
            send(down.at[l, k, yo, 0], ya.at[l, k, 0], ("ya", k), at_y(yp))
            send(down.at[l, k, yo, 1], ya.at[l, k, 1], ("ya", k), at_y(ym))
            send(down.at[l, k, yp, 1], yb.at[l, k, 0], ("yc", k), at_y(yp))
            send(down.at[l, k, ym, 0], yb.at[l, k, 1], ("yc", k), at_y(ym))
            all_sent(down.at[l, k, 0:2])

        def stage_g(l, k):
            arrived(ya.at[l, k], ("ya", k))
            for h, to in enumerate((yp, ym)):
                down[l, k, to, h] = (down[l, k, to, h].astype(F32) + ya[l, k, h].astype(F32)).astype(BF)
                send(down.at[l, k, to, h], yc.at[l, k, h], ("yc", k), at_y(to))
            all_sent(down.at[l, k, 0])

        def stage_h(l, k):
            arrived(down.at[l, k, 0:2], ("yc", k))
            for h in (0, 1):
                total = down[l, k, y, h].astype(F32) + yc[l, k, h].astype(F32) + yb[l, k, 1 - h].astype(F32)
                ys[l, k, 2 * h] = total[:R].astype(BF)
                ys[l, k, 2 * h + 1] = total[R:].astype(BF)
            me = unit_at[l][3]
            for d in (2, 1, 3):
                send(ys.at[l, k, turn(me, d)], xr.at[l, k, d - 1], ("xr", k), at_unit(l, turn(me, d)))
            all_sent(ys.at[l, k, 0:3])

        def stage_i(l, k):
            me = unit_at[l][3]
            rows = pl.ds(pl.multiple_of(part_rows(me), R), R)
            value = RESIDUAL * xs[l, k, rows, :].astype(F32) + ys[l, k, me].astype(F32)
            arrived(xr.at[l, k], ("xr", k))
            for d in (1, 3, 2):
                value = value + xr[l, k, d - 1].astype(F32)
            mixed[l, k] = value
            row_sum = jnp.sum(value, axis=1, keepdims=True)
            row_squares = jnp.sum(value * value, axis=1, keepdims=True)
            lane = lax.broadcasted_iota(jnp.int32, (R, 128), 1)
            st[l, k] = jnp.where(lane == 0, row_sum, jnp.where(lane == 1, row_squares, 0.0))
            for d in (2, 1, 3):
                send(st.at[l, k], st_in.at[l, k, d - 1], ("st", k), at_sum(l, turn(sums[l][3], d)))
            all_sent(st_in.at[l, k])

        def stage_j(l, k):
            me = unit_at[l][3]
            if ("gain",) not in seen:
                seen.add(("gain",))
                arrived(gains.at[0:3], ("gain",))
                for copy in gain_copies:
                    copy.wait()
            stats = st[l, k]
            arrived(st_in.at[l, k], ("st", k))
            for d in (1, 3, 2):
                stats = stats + st_in[l, k, d - 1]
            mean = stats[:, 0:1] / D
            var = stats[:, 1:2] / D - mean * mean
            scale = lax.rsqrt(var + EPSILON)
            for q in range(4):
                cols = slice(q * DB, (q + 1) * DB)
                normed = (mixed[l, k, :, cols] - mean) * scale
                nb[l, k, q] = (normed * gains[2 * l, q, l:l + 1, :] + gains[2 * l + 1, q, l:l + 1, :]).astype(BF)

            if l + 1 < LAYERS:
                dst = xs.at[1, k, pl.ds(pl.multiple_of(part_rows(me), R), R), d_cols(z)]
            else:
                dst = gathered(LAYERS, k, part_rows(me), R)
            dst[...] = nb[l, k, me]
            if l + 1 == LAYERS and k in DIRECT:
                for dz in (2, 1, 3, 0):
                    for dy in (2, 1, 3, 0):
                        for core in (1, 0):
                            if dz + dy == 0 and core == 1:
                                continue
                            at = (turn(z, dz) * 4 + x, turn(y, dy) * 2 + core)
                            send(nb.at[1, k, turn(z, dz)], dst, ("xg", k) if core else ("dd", k), at)
                all_sent(ov.at[0:31 * R, :])
                return
            for d in (2, 1, 3):
                name = ("xq", k) if l + 1 < LAYERS else ("xg", k)
                send(nb.at[l, k, turn(me, d)], dst, name, at_unit(l, turn(me, d)))
            all_sent(nb.at[l, k, 0:3])

        def stage_q(l, k):
            arrived(nb.at[0, k, 0:3], ("xq", k))
            ref = xs.at[1, k, y_block, d_cols(z)]
            for d in (2, 1, 3):
                send(ref, ref, ("xg", k), at_z(turn(z, d)))
            all_sent(ov.at[0:3 * YB, :])

        def stage_k(l, k):
            p = l + 1
            got = (ov.at[0:2 * YB, :], ov.at[0:3 * YB, :], nb.at[1, k, 0:3])[p]
            arrived(got, ("xg", k))
            if p == 0:
                in_copies[k].wait()
            for h in (0, 1):
                ref = gathered(p, k, y * YB + h * YH, YH)
                send(ref, ref, (("y0", "y1")[h], k), at_y(yp))
                ref = gathered(p, k, y * YB + (1 - h) * YH, YH)
                send(ref, ref, (("y0", "y1")[h], k), at_y(ym))
            if p == LAYERS:
                ref = gathered(p, k, y * YB, YB)
                send(ref, ref, ("dd", k), other)
                all_sent(ov.at[0:6 * YH, :])
            else:
                all_sent(xs.at[p, k, 0:4 * YH, :])

        def stage_l(l, k):
            p = l + 1
            halves = (lambda n: xs.at[p, k, 0:n * YH, :]) if p < LAYERS else (lambda n: ov.at[0:n * YH, :])
            arrived(halves(2), ("y0", k))
            for h, (owner, to) in enumerate(((ym, yp), (yp, ym))):
                ref = gathered(p, k, owner * YB + h * YH, YH)
                send(ref, ref, ("y2", k), at_y(to))
            if p == LAYERS:
                arrived(halves(2), ("y1", k))
                for owner in (ym, yp):
                    ref = gathered(p, k, owner * YB, YB)
                    send(ref, ref, ("dd", k), other)
                all_sent(ov.at[0:6 * YH, :])
            else:
                all_sent(xs.at[p, k, 0:2 * YH, :])

        def stage_m(l, k):
            p = l + 1
            arrived(ov.at[0:YB, :], ("y2", k))
            ref = gathered(p, k, yo * YB, YB)
            send(ref, ref, ("dd", k), other)
            all_sent(ov.at[0:YB, :])
            rows = pl.ds(k * TC, TC)
            out_copies.append(pltpu.make_async_copy(ov.at[rows, :], out_hbm.at[rows, :], local.at[14 + k]))
            out_copies[-1].start()

        def stage_w_both(l, j):
            if l + j == 0:
                stage_w(l, j)
                return
            pl.semaphore_signal(go, inc=1, device_id=other, device_id_type=MESH)
            stage_w(l, j)

        stages = dict(
            A=stage_a, B=stage_b, C=stage_c, D=stage_d, E=stage_e, G=stage_g, H=stage_h, I=stage_i, J=stage_j,
            K=stage_k, L=stage_l, M=stage_m, Q=stage_q, W=stage_w_both, V=stage_v, X=stage_x, S=stage_s,
        )
        for stage, *key in ORDER:
            stages[stage](*key)
            if stage == "C" and not gain_copies:
                gains_send()
            wait_sent(WAIT_LATER)
        for k in DIRECT:
            rows = pl.ds(k * TC, TC)
            arrived(ov.at[0:15 * R, :], ("xg", k))
            out_copies.append(pltpu.make_async_copy(ov.at[rows, :], out_hbm.at[rows, :], local.at[14 + k]))
            out_copies[-1].start()
        wait_sent(0)
        for copy in out_copies:
            copy.wait()

    @pl.when(c == 0)
    def _():
        program(0)

    @pl.when(c == 1)
    def _():
        program(1)


def solution(mesh):
    dma = pltpu.SemaphoreType.DMA

    def per_device(inputs, gate_weight, up_weight, down_weight, norm_gain, norm_shift):
        any_space = pl.BlockSpec(memory_space=pl.ANY)
        return pl.pallas_call(
            kernel,
            out_shape=jax.ShapeDtypeStruct((T, DB), BF),
            in_specs=[any_space] * 6,
            out_specs=any_space,
            scratch_shapes=[
                pltpu.VMEM((2, NC, TC, DQ), BF),
                pltpu.VMEM((2, NT, DQ, 2 * UT), BF),
                pltpu.VMEM((2, NJ, 2, UT, DQ), BF),
                pltpu.VMEM((2, NJ, 2, DB, UT), BF),
                pltpu.VMEM((2, 2, NJ, UT // 2, DB), BF),
                pltpu.VMEM((2, NC, NJ, 4, 2, ZH, 4 * UT), BF),
                pltpu.VMEM((2, NC, NJ, 2, ZH, 4 * UT), BF),
                pltpu.VMEM((2, NC, NJ, 2, ZH, 4 * UT), BF),
                pltpu.VMEM((2, NC, NJ, 2, ZH, 4 * UT), BF),
                pltpu.VMEM((2, NC, NT, TC, UT), BF),
                pltpu.VMEM((2, NC, 4, 2, YH, DQ), BF),
                pltpu.VMEM((2, NC, 2, YH, DQ), BF),
                pltpu.VMEM((2, NC, 2, YH, DQ), BF),
                pltpu.VMEM((2, NC, 2, YH, DQ), BF),
                pltpu.VMEM((2, NC, 4, R, DQ), BF),
                pltpu.VMEM((2, NC, 3, R, DQ), BF),
                pltpu.VMEM((2, NC, R, DQ), F32),
                pltpu.VMEM((2, NC, R, 128), F32),
                pltpu.VMEM((2, NC, 3, R, 128), F32),
                pltpu.VMEM((2, NC, 4, R, DB), BF),
                pltpu.VMEM((T, DB), BF),
                pltpu.VMEM((4, 4, 2, DB), F32),
                dma((N_SLOTS,)),
                dma((N_SENT,)),
                dma((19 + NC,)),
                pltpu.SemaphoreType.REGULAR,
            ],
            compiler_params=pltpu.CompilerParams(
                collective_id=0, has_side_effects=True, vmem_limit_bytes=63 * 1024 * 1024
            ),
        )(inputs, gate_weight, up_weight, down_weight.reshape(LAYERS, TILES, UT, DB), norm_gain, norm_shift)

    return jax.shard_map(
        per_device,
        mesh=mesh,
        in_specs=(P(None, "ra"), P(None, "ra", "cb"), P(None, "ra", "cb"), P(None, "cb", "ra"), P(None, "ra"), P(None, "ra")),
        out_specs=P(None, "ra"),
        check_vma=False,
    )
```
